32 devices in a mesh: sp: 16 (over z, y, x), tp: 2 (over core).
Axes of the slice: x: 2, y: 2, z: 4, core: 2. Of those that a mesh axis runs over, the one named last changes fastest.
Arguments:
- hidden_in: bfloat16 [8192, 2048], P('sp'), may hold values from -64 to 64
- pre_gain: float32 [2048], replicated, may hold values from 0.1 to 1.9
- query_proj: bfloat16 [2048, 2048], P(None, 'tp'), may hold values from -2 to 2
- key_proj: bfloat16 [2048, 2048], P('sp', 'tp'), may hold values from -2 to 2
- value_proj: bfloat16 [2048, 2048], P('sp', 'tp'), may hold values from -0.125 to 0.125
- out_proj: bfloat16 [2048, 2048], P('tp'), may hold values from -0.125 to 0.125
- post_gain: float32 [2048], replicated, may hold values from 0.1 to 1.9
Outputs:
- layer_out: bfloat16 [8192, 2048], P(('sp', 'tp'))
- log_weight: float32 [32, 8192], P('tp', 'sp')
The draws below stay inside these ranges and needn't reach their ends.
All inputs are finite; a program needn't handle non-finite values.
Results may differ from the reference program's by a relative error of at most 0.018.
The reference program's roundings to bfloat16 on the way count: a program that leaves them out, or rounds other values in their place, can miss the bound.
Values may be sent and summed in bfloat16 or wider, within the bound.
A program may use at most 128 MiB of HBM per device.

```python
import jax
import jax.numpy as jnp
from jax import lax

D = 2048
HEADS = 32
HEAD_DIM = 64
SPAN = 128
TOKENS = 8192
N_TP = 2


def draw_hidden_in(key, part):
    noise_part = jax.random.normal(jax.random.fold_in(key, 3), (TOKENS, D), jnp.float32)
    return jnp.clip(noise_part, -64.0, 64.0).astype(jnp.bfloat16)


def shared_pair(key):
    fan_scale = D ** (-0.5)
    query_part = jax.random.normal(jax.random.fold_in(key, 22), (D, HEADS * HEAD_DIM), jnp.float32) * fan_scale
    key_part = jax.random.normal(jax.random.fold_in(key, 23), (D, HEADS * HEAD_DIM), jnp.float32) * fan_scale
    return (jnp.clip(query_part, -2.0, 2.0), jnp.clip(key_part, -2.0, 2.0))


def draw_query_proj(key, part):
    return shared_pair(key)[0].astype(jnp.bfloat16)


def draw_key_proj(key, part):
    return shared_pair(key)[1].astype(jnp.bfloat16)


def steps_of(key, dims, split, least, high):
    factor_of = 1.0
    for dim, parts in split:
        steps = jax.random.uniform(jax.random.fold_in(jax.random.fold_in(key, 6), dim), (parts,), jnp.float32, least / len(split), high / len(split))
        factor_of = factor_of * jnp.repeat(jnp.exp(steps), dims[dim] // parts).reshape((-1,) + (1,) * (len(dims) - 1 - dim))
    return factor_of


def noise(key, shape, deviation, most, shards=(), held_as=jnp.bfloat16):
    values = jax.random.normal(key, shape, jnp.float32) * deviation
    if len(shards) > 0:
        values = steps_of(key, shape, shards, -0.22, 0.18) * values
    return jnp.clip(values, min=-most, max=most).astype(held_as)


def setup_inputs(seed: int = 0) -> dict:
    splits = jax.random.split(jax.random.key(seed), 8)
    return {
        "hidden_in": draw_hidden_in(jax.random.fold_in(splits[7], 71), 0),
        "pre_gain": jnp.clip(1.0 + 0.18 * jax.random.normal(splits[1], (D,), jnp.float32), 0.1, 1.9),
        "query_proj": draw_query_proj(jax.random.fold_in(splits[7], 71), 0),
        "key_proj": draw_key_proj(jax.random.fold_in(splits[7], 71), 0),
        "value_proj": noise(splits[4], (D, HEADS * HEAD_DIM), D ** -0.5, 0.125, ((0, 16), (1, 2))),
        "out_proj": noise(splits[5], (HEADS * HEAD_DIM, D), (HEADS * HEAD_DIM) ** -0.5, 0.125, ((0, 2),)),
        "post_gain": jnp.clip(1.0 + 0.18 * jax.random.normal(splits[6], (D,), jnp.float32), 0.1, 1.9),
    }


EPS = 1e-06
ROPE_BASE = 10000.0
DILATIONS = (1, 4, 16)

def rotate(vectors, positions):
    half_dim = vectors.shape[-1] // 2
    frequency = ROPE_BASE ** (-(jnp.arange(half_dim, dtype=jnp.float32) * 2.0 / vectors.shape[-1]))
    angles = positions[:, None] * frequency[None, :]
    cos_part = jnp.cos(angles)[:, None, :]
    sin_part = jnp.sin(angles)[:, None, :]
    front_half = vectors[..., :half_dim]
    back_half = vectors[..., half_dim:]
    return jnp.concatenate([front_half * cos_part - back_half * sin_part, back_half * cos_part + front_half * sin_part], axis=-1)

def rms_scale(matrix, gain):
    return matrix * lax.rsqrt(lax.optimization_barrier(jnp.mean(matrix * matrix, axis=-1, keepdims=True)) + EPS) * gain

def residue_attention(queries, key_rows, values, dilation):
    seq_len, head_count, head_depth = queries.shape
    blocks = seq_len // (dilation * SPAN)
    block_shape = (blocks, SPAN, dilation, head_count, head_depth)
    query_blocks = queries.reshape(block_shape).astype(jnp.float32)
    key_blocks = key_rows.reshape(block_shape).astype(jnp.float32)
    value_blocks = values.reshape(block_shape).astype(jnp.float32)
    zero_block = jnp.zeros((1,) + block_shape[1:], jnp.float32)
    key_pairs = jnp.concatenate([jnp.concatenate([zero_block, key_blocks[:-1]], axis=0), key_blocks], axis=1)
    value_pairs = jnp.concatenate([jnp.concatenate([zero_block, value_blocks[:-1]], axis=0), value_blocks], axis=1)
    scores = jnp.einsum('bqrhe,bkrhe->brhqk', query_blocks, key_pairs) * head_depth ** (-0.5)
    query_idx = jnp.arange(SPAN, dtype=jnp.int32)[:, None]
    key_idx = jnp.arange(2 * SPAN, dtype=jnp.int32)[None, :]
    distance = query_idx + SPAN - key_idx
    in_band = (distance >= 0) & (distance <= SPAN)
    key_pos = (jnp.arange(blocks, dtype=jnp.int32)[:, None, None, None, None] * SPAN + jnp.arange(2 * SPAN, dtype=jnp.int32)[None, None, None, None, :] - SPAN) * dilation + jnp.arange(dilation, dtype=jnp.int32)[None, :, None, None, None]
    valid = in_band[None, None, None] & (key_pos >= 0)
    scores = jnp.where(valid, scores, -jnp.inf)
    row_max = lax.optimization_barrier(jnp.max(scores, axis=-1, keepdims=True))
    exp_scores = jnp.exp(scores - row_max)
    denominator = lax.optimization_barrier(jnp.sum(exp_scores, axis=-1, keepdims=True))
    levels = (row_max + jnp.log(denominator))[..., 0]
    shares = lax.optimization_barrier((exp_scores / denominator).astype(jnp.bfloat16))
    outcome = jnp.einsum('brhqk,bkrhe->bqrhe', shares.astype(jnp.float32), value_pairs)
    outcome = outcome.reshape(seq_len, head_count, head_depth)
    levels = levels.transpose(2, 0, 3, 1).reshape(head_count, seq_len)
    return (outcome, levels)

def blend(group_outs, group_levels):
    levels = jnp.stack(group_levels)
    row_max = lax.optimization_barrier(jnp.max(levels, axis=0))
    log_weight = row_max + jnp.log(lax.optimization_barrier(jnp.sum(jnp.exp(levels - row_max[None]), axis=0)))
    shares = jnp.exp(levels - log_weight[None])
    blended = lax.optimization_barrier(jnp.sum(shares.transpose(0, 2, 1)[..., None] * jnp.stack(group_outs), axis=0))
    return (blended, log_weight)

def reference(hidden_in, pre_gain, query_proj, key_proj, value_proj, out_proj, post_gain):
    normed = rms_scale(hidden_in.astype(jnp.float32), pre_gain).astype(jnp.bfloat16)
    positions = jnp.arange(TOKENS, dtype=jnp.int32).astype(jnp.float32)
    group_width = HEADS // N_TP * HEAD_DIM

    def split_cols(matrix):
        return matrix.reshape(D, N_TP, group_width).transpose(1, 0, 2)

    def one_group(summed, weights):
        w_query, w_key, w_value, w_out = weights
        queries = rotate(jnp.dot(normed, w_query, preferred_element_type=jnp.float32).reshape(TOKENS, -1, HEAD_DIM), positions).astype(jnp.bfloat16)
        key_rows = rotate(jnp.dot(normed, w_key, preferred_element_type=jnp.float32).reshape(TOKENS, -1, HEAD_DIM), positions).astype(jnp.bfloat16)
        values = jnp.dot(normed, w_value, preferred_element_type=jnp.float32).astype(jnp.bfloat16).reshape(TOKENS, -1, HEAD_DIM)
        group_outs = []
        group_levels = []
        for dilation in DILATIONS:
            outcome, levels = residue_attention(queries, key_rows, values, dilation)
            group_outs.append(outcome)
            group_levels.append(levels)
        blended, log_weight = blend(group_outs, group_levels)
        attended = blended.astype(jnp.bfloat16).reshape(TOKENS, group_width)
        partial_value = lax.optimization_barrier(jnp.dot(attended, w_out, preferred_element_type=jnp.float32).astype(jnp.bfloat16))
        return (summed + partial_value.astype(jnp.float32), log_weight)
    summed, log_weight = lax.scan(one_group, jnp.zeros((TOKENS, D), jnp.float32), (split_cols(query_proj), split_cols(key_proj), split_cols(value_proj), out_proj.reshape(N_TP, group_width, D)))
    layer_out = rms_scale(summed, post_gain).astype(jnp.bfloat16)
    return (layer_out, log_weight.reshape(HEADS, TOKENS))
```

```python
import functools

import jax
import jax.numpy as jnp
from jax import lax
from jax.experimental import pallas as pl
from jax.experimental.pallas import tpu as pltpu
from jax.sharding import PartitionSpec as P

HEAD_DIM = 64
SPAN = 128
EPS = 1e-06
ROPE_BASE = 10000.0
WIDE = 16
LANES = 128
MESH = pl.DeviceIdType.MESH
ANY = pl.BlockSpec(memory_space=pl.ANY)
NEG = -1e30


def greet(peers):
    barrier = pltpu.get_barrier_semaphore()
    for peer in peers:
        pl.semaphore_signal(barrier, inc=1, device_id=peer, device_id_type=MESH)
    pl.semaphore_wait(barrier, len(peers))


def remote(src, dst, send, recv, peer):
    return pltpu.make_async_remote_copy(
        src_ref=src, dst_ref=dst, send_sem=send, recv_sem=recv, device_id=peer, device_id_type=MESH
    )


def group_of(mesh, width):
    for size in (4, 2):
        if mesh.shape["sp"] % size == 0 and width % (size * LANES) == 0:
            return size
    return 1


def flip(c, mask):
    out = c
    if mask & 1:
        out = out + 1 - 2 * lax.rem(c, 2)
    if mask & 2:
        out = out + 2 - 4 * lax.rem(lax.div(c, 2), 2)
    return out


def layer_kernel(
    n_sp, n_tp, group, behind,
    hid_ref, gain_ref, freq_ref, wq_ref, wk_ref, wv_ref,
    att_ref, lw_ref,
    hid, nrm, wq, wk, wv, cos_t, sin_t, scr,
    qn_all, kw_all, vw_all, qr_all, kx_all, vx_all,
    acc1, m1, l1, acc4, m4, l4, acc16, m16, l16, b1, b4, b16,
    local, near_s, near_r, line_s, line_r, dir_s, dir_r, across_s, across_r, twin_s, twin_r,
    early_s, early_r, late_s, late_r,
):
    f32, bf16 = jnp.float32, jnp.bfloat16
    s = lax.axis_index("sp")
    t = lax.axis_index("tp")
    rows, depth = hid_ref.shape
    all_rows = rows * group
    w_rows = wk_ref.shape[0]
    part = wq.shape[1]
    pairs = part // LANES
    steps = all_rows // WIDE
    few = rows // WIDE
    quarter = rows // 4
    count = n_sp // group
    c = lax.rem(s, group)
    base = s - c
    g = lax.div(s, group)
    half = lax.rem(t, 2)
    sibling = (s, t + 1 - 2 * half)
    masks = list(range(1, group))
    peer = {k: base + flip(c, k) for k in masks}
    up = lax.rem(s + group, n_sp)
    down = lax.rem(s + n_sp - group, n_sp)
    after = [lax.rem(s + b * group, n_sp) for b in range(1, behind + 1)]
    before = [lax.rem(s + n_sp - b * group, n_sp) for b in range(1, behind + 1)]
    start_row = pl.multiple_of(c * rows, rows)

    kept = [pltpu.make_async_copy(hid_ref, hid.at[pl.ds(start_row, rows)], local.at[0])]
    own_cols = pl.ds(pl.multiple_of(c * part, LANES), part)
    own_rows = pl.ds(pl.multiple_of(s * w_rows, w_rows), w_rows)
    kept.append(pltpu.make_async_copy(wq_ref.at[:, own_cols], wq, local.at[1]))
    for j, (src, dst) in enumerate(((wk_ref, wk), (wv_ref, wv))):
        kept.append(pltpu.make_async_copy(src.at[:, own_cols], dst.at[own_rows], local.at[2 + j]))
    for copy in kept:
        copy.start()

    known = [(peer[k], t) for k in masks] + [(x, t) for x in after + before] + [sibling]
    greet(known)

    def near(k, j):
        src, dst = ((wk_ref, wk), (wv_ref, wv))[j]
        cols = pl.ds(pl.multiple_of(flip(c, k) * part, LANES), part)
        return remote(src.at[:, cols], dst.at[own_rows], near_s.at[j, k - 1], near_r.at[j, k - 1], (peer[k], t))

    def line(way, j, d):
        ref = (wk, wv)[j]
        to, off = ((up, g - d), (down, g + d))[way]
        off = jnp.clip(off, 0, count - 1)
        slot = ref.at[pl.ds(pl.multiple_of(off * group * w_rows, group * w_rows), group * w_rows)]
        return remote(slot, slot, line_s.at[way, j, d], line_r.at[way, j, d + 1], (to, t))

    def line_in(way, j, d):
        ref = (wk, wv)[j]
        off = jnp.clip((g - d, g + d)[way], 0, count - 1)
        slot = ref.at[pl.ds(pl.multiple_of(off * group * w_rows, group * w_rows), group * w_rows)]
        return remote(slot, slot, line_s.at[way, j, d - 1], line_r.at[way, j, d], ((up, down)[way], t))

    def has_in(way, d):
        return g >= d if way == 0 else g + d < count

    def has_out(way, d):
        if way == 0:
            return (g >= d) & (g + 1 < count)
        return (g + d < count) & (g >= 1)

    def pass_on(j, d):
        for way in range(2):
            if not (isinstance(d, int) and d == 0):
                @pl.when(has_in(way, d))
                def _(way=way):
                    line_in(way, j, d).wait_recv()

            if not (isinstance(d, int) and d == count - 1):
                @pl.when(has_out(way, d))
                def _(way=way):
                    line(way, j, d).start()

    def passed(j, d):
        for way in range(2):
            @pl.when(has_out(way, d))
            def _(way=way):
                line(way, j, d).wait_send()

    def piece(block, side, q):
        return hid.at[pl.ds(pl.multiple_of(block * rows + side * (2 * quarter) + q * quarter, quarter), quarter)]

    def direct(k, q):
        src = hid_ref.at[pl.ds(pl.multiple_of(half * (2 * quarter) + q * quarter, quarter), quarter)]
        return remote(src, piece(c, half, q), dir_s.at[k - 1, q], dir_r.at[k - 1, q], (peer[k], t))

    def across(i):
        k, other = ((1, 2), (2, 1))[i]
        slot = piece(flip(c, k), half, i)
        return remote(slot, slot, across_s.at[i], across_r.at[i], (peer[other], t))

    def twin(k, q):
        slot = piece(flip(c, k), half, q)
        return remote(slot, slot, twin_s.at[k - 1, q], twin_r.at[k - 1, q], sibling)

    for j in range(2):
        for k in masks:
            near(k, j).start()
    firsts = {4: [(1, 0), (2, 1)], 2: [(1, 0)], 1: []}[group]
    seconds = {4: [(1, 1), (2, 0)], 2: [(1, 1)], 1: []}[group]
    thirds = {4: [(3, 0), (3, 1)], 2: [], 1: []}[group]
    for k, q in firsts + seconds:
        direct(k, q).start()

    def block_of(k):
        return flip(c, k) * rows

    def norm(k):
        def body(i, _):
            at = pl.ds(pl.multiple_of(block_of(k) + i * quarter, quarter), quarter)
            x = hid[at, :].astype(f32)
            scale = lax.rsqrt(jnp.mean(x * x, axis=-1, keepdims=True) + EPS)
            nrm[at, :] = (x * scale * gain_ref[...]).astype(bf16)
            return 0

        lax.fori_loop(0, 4, body, 0)

    front = lax.rem(lax.broadcasted_iota(jnp.int32, (rows, LANES), 1), HEAD_DIM) < HEAD_DIM // 2

    def project(k, j):
        row = pl.multiple_of(block_of(k), rows)
        here = pl.ds(row, rows)
        out = jnp.dot(nrm[here, :], (wq, wk, wv)[j][...], preferred_element_type=f32)
        nat = (qn_all, kw_all, vw_all)[j]
        res = (qr_all, kx_all, vx_all)[j]
        skip = 0 if j == 0 else SPAN
        skip_res = 0 if j == 0 else behind * steps
        step = pl.multiple_of(lax.div(row, WIDE), few)
        for i in range(pairs):
            u = out[:, i * LANES:(i + 1) * LANES]
            if j < 2:
                swapped = jnp.where(
                    front,
                    pltpu.roll(u, LANES - HEAD_DIM // 2, 1),
                    pltpu.roll(u, HEAD_DIM // 2, 1),
                )
                u = u * cos_t[here, :] + swapped * sin_t[here, :]
            if j == 0:
                u = u * HEAD_DIM ** (-0.5)
            nat[i, pl.ds(row + skip, rows), :] = u.astype(bf16)
            scr[i] = u
        for i in range(pairs):
            for r in range(WIDE):
                res[i, r, pl.ds(step + skip_res, few), :] = scr[i, pl.ds(r, few, stride=WIDE), :].astype(bf16)

    for j in range(2):
        for k in masks:
            near(k, j).wait_recv()
        kept[2 + j].wait()
        pass_on(j, 0)

    half_dim = HEAD_DIM // 2
    lo = lax.broadcasted_iota(jnp.int32, (LANES, LANES), 0).astype(f32) * freq_ref[...]
    cos_lo, sin_lo = jnp.cos(lo), jnp.sin(lo)
    lane = lax.rem(lax.broadcasted_iota(jnp.int32, (1, LANES), 1), HEAD_DIM)
    sign = jnp.where(lane < half_dim, -1.0, 1.0)

    def fill(i, _):
        hi = (base * rows + i * LANES).astype(f32) * freq_ref[...]
        cos_hi, sin_hi = jnp.cos(hi), jnp.sin(hi)
        at = pl.ds(pl.multiple_of(i * LANES, LANES), LANES)
        cos_t[at, :] = cos_lo * cos_hi - sin_lo * sin_hi
        sin_t[at, :] = (sin_lo * cos_hi + cos_lo * sin_hi) * sign
        return 0

    lax.fori_loop(0, all_rows // LANES, fill, 0)

    @pl.when(g < behind)
    def _():
        for pair in range(pairs):
            for ref in (kw_all, vw_all):
                @pl.when(g < 1)
                def _(ref=ref, pair=pair):
                    ref[pair, pl.ds(0, SPAN), :] = jnp.zeros((SPAN, LANES), bf16)
            for ref in (kx_all, vx_all):
                for b in range(1, behind + 1):
                    @pl.when(g < b)
                    def _(ref=ref, pair=pair, b=b):
                        ref[pair, :, pl.ds((behind - b) * steps, steps), :] = jnp.zeros((WIDE, steps, LANES), bf16)

    kept[0].wait()
    norm(0)
    kept[1].wait()
    project(0, 0)

    for k, q in firsts:
        direct(k, q).wait_recv()
        if group == 4:
            across(k - 1).start()
        twin(k, q).start()
    if count > 1:
        for j in range(2):
            pass_on(j, 1)
    for k, q in seconds:
        direct(k, q).wait_recv()
        twin(k, q).start()
    if count > 2:
        for j in range(2):
            pass_on(j, 2)
    for k in masks[:2]:
        for q in range(2):
            twin(k, q).wait_recv()
        norm(k)
        project(k, 0)
    if group == 4:
        for k, q in thirds:
            across(q).wait_recv()
            twin(k, q).start()
    if count > 3:
        for d in range(3, min(count, 4)):
            pass_on(0, d)
            pass_on(1, d)
    if count > 4:
        def further(d, _):
            pass_on(0, d)
            pass_on(1, d)
            return 0

        lax.fori_loop(4, count, further, 0)

    def early(pair, j):
        ref = (kw_all, vw_all)[j]
        return remote(
            ref.at[pair, pl.ds(all_rows, SPAN)], ref.at[pair, pl.ds(0, SPAN)],
            early_s.at[pair, j], early_r.at[pair, j], (after[0], t),
        )

    def late(pair, j, k, b):
        ref = (kx_all, vx_all)[j]
        at = pl.multiple_of(flip(c, k) * few, few)
        return remote(
            ref.at[pair, :, pl.ds(behind * steps + at, few)],
            ref.at[pair, :, pl.ds((behind - b) * steps + at, few)],
            late_s.at[pair, j, b - 1, k], late_r.at[pair, j, b - 1, k], (after[b - 1], t),
        )

    everything = [0] + masks

    def send_late(pair, j, k):
        for b in range(1, behind + 1):
            @pl.when(g + b < count)
            def _(b=b):
                late(pair, j, k, b).start()

    def send_early(pair, j):
        @pl.when(g + 1 < count)
        def _():
            early(pair, j).start()

    for k in everything[:3]:
        project(k, 1)
        if k > 0:
            send_late(0, 0, k - 1)
    if group == 4:
        for q in range(2):
            twin(3, q).wait_recv()
        norm(3)
        project(3, 0)
        project(3, 1)
        send_late(0, 0, 2)
    for i, k in enumerate(everything):
        project(k, 2)
        if i == 0:
            send_late(0, 0, everything[-1])
            send_early(0, 0)
        else:
            send_late(0, 1, k - 1)

    def put_bias(ref, near_by, first_of):
        shape = ref.shape[1:]
        a = lax.broadcasted_iota(jnp.int32, shape, 0)
        b = lax.broadcasted_iota(jnp.int32, shape, 1)
        distance, place = near_by(a, b)
        band = (distance >= 0) & (distance <= SPAN)
        ref[0] = jnp.where(band & (place + first_of >= 0), 0.0, NEG).astype(f32)
        ref[1] = jnp.where(band, 0.0, NEG).astype(f32)

    def plain(a, b):
        return a + SPAN - b, b - SPAN

    def woven(a, b):
        return 4 * (a % 32 + 32 - b % 64) + a // 32 - b // 64, b % 64 - 32

    put_bias(b1, plain, g * all_rows)
    put_bias(b16, plain, g * steps)
    put_bias(b4, woven, g * steps)

    send_late(0, 1, everything[-1])
    send_early(0, 1)
    for pair in range(1, pairs):
        for j in range(2):
            for k in everything:
                send_late(pair, j, k)
            send_early(pair, j)

    block = min(SPAN, steps)
    skip16 = behind * steps - SPAN

    def tile(q, k, v, bias):
        n = q.shape[0]
        low = lax.broadcasted_iota(jnp.int32, (n, LANES), 1) < HEAD_DIM
        low_q = low.astype(f32).astype(bf16)
        both = jnp.concatenate([q * low_q, q * (1 - low_q)], axis=0)
        sc = lax.dot_general(both, k, (((1,), (1,)), ((), ())), preferred_element_type=f32)
        sc = sc + jnp.concatenate([bias, bias], axis=0)
        m = jnp.max(sc, axis=-1, keepdims=True)
        e = jnp.exp(sc - m).astype(bf16)
        o = jnp.dot(e, jnp.concatenate([v, jnp.ones_like(v)], axis=1), preferred_element_type=f32)
        wide_m = jnp.broadcast_to(m, (2 * n, LANES))
        return (
            jnp.where(low, o[:n, :LANES], o[n:, :LANES]),
            jnp.where(low, wide_m[:n], wide_m[n:]),
            jnp.where(low, o[:n, LANES:], o[n:, LANES:]),
        )

    blocks16 = steps // block
    blocks4 = steps // 32

    for p in range(pairs):
        qn, kw, vw, qr, kx, vx = (ref.at[p] for ref in (qn_all, kw_all, vw_all, qr_all, kx_all, vx_all))

        def step16(idx, _):
            r = idx // blocks16
            i = idx % blocks16
            at = pl.multiple_of(i * block, block)
            keys = pl.ds(at + skip16, block + SPAN)
            got = tile(qr[r, pl.ds(at, block), :], kx[r, keys, :], vx[r, keys, :], b16[jnp.minimum(i, 1)])
            for ref, value in zip((acc16, m16, l16), got):
                ref[pl.ds(r + WIDE * at, block, stride=WIDE), :] = value
            return 0

        def step4(r, i):
            at = i * 32
            low = at + behind * steps - 32
            if not isinstance(i, int):
                at = pl.multiple_of(at, 32)
                low = pl.multiple_of(low, 32)
            keys = pl.ds(low, 64)
            got = tile(
                jnp.concatenate([qr[r + 4 * j, pl.ds(at, 32), :] for j in range(4)], axis=0),
                jnp.concatenate([kx[r + 4 * j, keys, :] for j in range(4)], axis=0),
                jnp.concatenate([vx[r + 4 * j, keys, :] for j in range(4)], axis=0),
                b4[0 if isinstance(i, int) else 1],
            )
            for ref, value in zip((acc4, m4, l4), got):
                for j in range(4):
                    ref[pl.ds(r + 4 * j + WIDE * at, 32, stride=WIDE), :] = value[j * 32:(j + 1) * 32]
            return 0

        def step1(i, _):
            at = pl.multiple_of(i * SPAN, SPAN)
            here = pl.ds(at, SPAN)
            keys = pl.ds(at, 2 * SPAN)
            got = tile(qn[here, :], kw[keys, :], vw[keys, :], b1[jnp.minimum(i, 1)])
            for ref, value in zip((acc1, m1, l1), got):
                ref[here, :] = value
            return 0

        def merge(i, _):
            here = pl.ds(pl.multiple_of(i * SPAN, SPAN), SPAN)
            tops = (m1[here, :], m4[here, :], m16[here, :])
            top = jnp.maximum(tops[0], jnp.maximum(tops[1], tops[2]))
            e1, e4, e16 = (jnp.exp(x - top) for x in tops)
            total = l1[here, :] * e1 + l4[here, :] * e4 + l16[here, :] * e16
            mixed = acc1[here, :] * e1 + acc4[here, :] * e4 + acc16[here, :] * e16
            att_ref[here, pl.ds(p * LANES, LANES)] = (mixed / total).astype(att_ref.dtype)
            turned = jnp.transpose(top + jnp.log(total))
            lw_ref[p, 0:1, here] = turned[0:1]
            lw_ref[p, 1:2, here] = turned[HEAD_DIM:HEAD_DIM + 1]
            return 0

        if blocks4 > 1:
            lax.fori_loop(
                0, 4 * (blocks4 - 1),
                lambda idx, _: step4(idx // (blocks4 - 1), idx % (blocks4 - 1) + 1), 0, unroll=2,
            )
        lax.fori_loop(1, all_rows // SPAN, step1, 0, unroll=2)
        for j in range(2):
            @pl.when(g >= 1)
            def _(j=j):
                early(p, j).wait_recv()
        step1(0, 0)
        for j in range(2):
            for b in range(1, behind + 1):
                @pl.when(g >= b)
                def _(j=j, b=b):
                    for k in everything:
                        late(p, j, k, b).wait_recv()
        lax.fori_loop(0, 4, lambda r, _: step4(r, 0), 0, unroll=2)
        lax.fori_loop(0, WIDE * blocks16, step16, 0, unroll=2)
        lax.fori_loop(0, all_rows // SPAN, merge, 0, unroll=2)

    for j in range(2):
        for k in masks:
            near(k, j).wait_send()
        for d in range(min(count - 1, 4)):
            passed(j, d)
        if count > 5:
            lax.fori_loop(4, count - 1, lambda d, _, j=j: (passed(j, d), 0)[1], 0)
    for k, q in firsts + seconds:
        direct(k, q).wait_send()
        twin(k, q).wait_send()
    if group == 4:
        for i in range(2):
            across(i).wait_send()
            twin(3, i).wait_send()
    for pair in range(pairs):
        for j in range(2):
            @pl.when(g + 1 < count)
            def _(pair=pair, j=j):
                early(pair, j).wait_send()

            for b in range(1, behind + 1):
                @pl.when(g + b < count)
                def _(pair=pair, j=j, b=b):
                    for k in everything:
                        late(pair, j, k, b).wait_send()


def layer(mesh, group, behind, hidden, gain, freq, wq, wk, wv):
    n_sp = mesh.shape["sp"]
    rows, depth = hidden.shape
    w_rows, width = wk.shape
    part = width // group
    pairs = part // LANES
    all_rows = rows * group
    steps = all_rows // WIDE
    block = min(SPAN, steps)
    count = n_sp // group
    f32, bf16 = jnp.float32, jnp.bfloat16
    dma = pltpu.SemaphoreType.DMA
    state = pltpu.VMEM((all_rows, LANES), f32)
    weight = pltpu.VMEM((depth, part), bf16)
    table = pltpu.VMEM((all_rows, LANES), f32)
    full = pltpu.VMEM((all_rows, depth), bf16)
    ring = pltpu.VMEM((pairs, SPAN + all_rows, LANES), bf16)
    woven = pltpu.VMEM((pairs, WIDE, (behind + 1) * steps, LANES), bf16)
    vmem = pl.BlockSpec(memory_space=pltpu.VMEM)
    near = max(group - 1, 1)
    return pl.pallas_call(
        functools.partial(layer_kernel, n_sp, mesh.shape["tp"], group, behind),
        out_shape=(
            jax.ShapeDtypeStruct((all_rows, part), bf16),
            jax.ShapeDtypeStruct((pairs, 2, all_rows), f32),
        ),
        in_specs=[ANY, vmem, vmem, ANY, ANY, ANY],
        out_specs=(vmem, vmem),
        scratch_shapes=[
            full, full, weight, weight, weight, table, table,
            pltpu.VMEM((pairs, rows, LANES), f32),
            pltpu.VMEM((pairs, all_rows, LANES), bf16), ring, ring,
            pltpu.VMEM((pairs, WIDE, steps, LANES), bf16), woven, woven,
            state, state, state, state, state, state, state, state, state,
            pltpu.VMEM((2, SPAN, 2 * SPAN), f32),
            pltpu.VMEM((2, SPAN, 2 * SPAN), f32),
            pltpu.VMEM((2, block, block + SPAN), f32),
            dma((4,)), dma((2, near)), dma((2, near)), dma((2, 2, count)), dma((2, 2, count)),
            dma((2, 2)), dma((2, 2)), dma((2,)), dma((2,)), dma((3, 2)), dma((3, 2)),
            dma((pairs, 2)), dma((pairs, 2)),
            dma((pairs, 2, behind, group)), dma((pairs, 2, behind, group)),
        ],
        compiler_params=pltpu.CompilerParams(
            vmem_limit_bytes=62 * 1024 * 1024, collective_id=0, has_side_effects=True
        ),
        name="layer_core",
    )(hidden, gain, freq, wq, wk, wv)


def return_kernel(group, rows, att_ref, lw_ref, att_out, lw_out, send, recv, local):
    s = lax.axis_index("sp")
    t = lax.axis_index("tp")
    part = att_ref.shape[1]
    c = lax.rem(s, group)
    base = s - c
    peers = [lax.rem(c + k, group) for k in range(1, group)]
    if group > 1:
        greet([(base + peer, t) for peer in peers])
    cols = pl.ds(pl.multiple_of(c * part, LANES), part)

    def pieces(peer):
        span = pl.ds(pl.multiple_of(peer * rows, rows), rows)
        return ((att_ref.at[span], att_out.at[:, cols]), (lw_ref.at[:, :, span], lw_out.at[c]))

    copies = []
    for k, peer in enumerate(peers):
        for j, (src, dst) in enumerate(pieces(peer)):
            copies.append(remote(src, dst, send.at[2 * k + j], recv.at[2 * k + j], (base + peer, t)))
    for j, (src, dst) in enumerate(pieces(c)):
        copies.append(pltpu.make_async_copy(src, dst, local.at[j]))
    for copy in copies:
        copy.start()
    for copy in copies:
        copy.wait()


def give_back(mesh, group, att, lw):
    rows = att.shape[0] // group
    part = att.shape[1]
    pairs = part // LANES
    dma = pltpu.SemaphoreType.DMA
    return pl.pallas_call(
        functools.partial(return_kernel, group, rows),
        out_shape=(
            jax.ShapeDtypeStruct((rows, part * group), att.dtype),
            jax.ShapeDtypeStruct((group, pairs, 2, rows), lw.dtype),
        ),
        in_specs=[ANY] * 2,
        out_specs=(ANY,) * 2,
        scratch_shapes=[dma((2 * group,)), dma((2 * group,)), dma((2,))],
        compiler_params=pltpu.CompilerParams(
            collective_id=2 if group > 1 else None, has_side_effects=True
        ),
        name="give_back",
    )(att, lw)


def swap_kernel(n_tp, part_ref, out_ref, send, recv):
    s = lax.axis_index("sp")
    t = lax.axis_index("tp")
    peers = [lax.rem(t + k, n_tp) for k in range(1, n_tp)]
    greet([(s, peer) for peer in peers])
    copies = [
        remote(part_ref.at[peer], out_ref.at[k], send.at[k], recv.at[k], (s, peer))
        for k, peer in enumerate(peers)
    ]
    for copy in copies:
        copy.start()
    for copy in copies:
        copy.wait()


def swap(mesh, partial):
    n_tp = mesh.shape["tp"]
    dma = pltpu.SemaphoreType.DMA
    return pl.pallas_call(
        functools.partial(swap_kernel, n_tp),
        out_shape=jax.ShapeDtypeStruct((n_tp - 1,) + partial.shape[1:], partial.dtype),
        in_specs=[ANY],
        out_specs=ANY,
        scratch_shapes=[dma((n_tp,)), dma((n_tp,))],
        compiler_params=pltpu.CompilerParams(collective_id=3, has_side_effects=True),
        name="swap_partials",
    )(partial)


def body(mesh, hidden_in, pre_gain, query_proj, key_proj, value_proj, out_proj, post_gain):
    rows, depth = hidden_in.shape
    width = query_proj.shape[1]
    n_tp = mesh.shape["tp"]
    group = group_of(mesh, width)
    t = lax.axis_index("tp")
    all_rows = rows * group
    behind = -(-(WIDE * SPAN) // all_rows)
    half_dim = HEAD_DIM // 2
    frequency = ROPE_BASE ** (-(jnp.arange(half_dim, dtype=jnp.float32) * 2.0 / HEAD_DIM))
    freq = jnp.concatenate([frequency] * (LANES // half_dim))[None, :]
    att, lw = layer(
        mesh, group, behind, hidden_in, pre_gain[None, :], freq, query_proj, key_proj, value_proj
    )
    attended, log_weight = give_back(mesh, group, att, lw)
    partial = jnp.dot(attended, out_proj, preferred_element_type=jnp.float32).astype(jnp.bfloat16)
    partial = partial.reshape(n_tp, rows // n_tp, depth)
    others = swap(mesh, partial)
    own = lax.dynamic_index_in_dim(partial, t, 0, keepdims=False)
    summed = own.astype(jnp.float32) + jnp.sum(others.astype(jnp.float32), axis=0)
    scale = lax.rsqrt(jnp.mean(summed * summed, axis=-1, keepdims=True) + EPS)
    layer_out = (summed * scale * post_gain).astype(jnp.bfloat16)
    return (layer_out, log_weight.reshape(width // HEAD_DIM, rows))


def solution(mesh):
    placed = (P("sp", None), P(), P(None, "tp"), P("sp", "tp"), P("sp", "tp"), P("tp", None), P())
    return jax.shard_map(
        functools.partial(body, mesh),
        mesh=mesh,
        in_specs=placed,
        out_specs=(P(("sp", "tp"), None), P("tp", "sp")),
        check_vma=False,
    )
```

```python
import functools

import jax
import jax.numpy as jnp
from jax import lax
from jax.experimental import pallas as pl
from jax.experimental.pallas import tpu as pltpu
from jax.sharding import PartitionSpec as P

HEAD_DIM = 64
SPAN = 128
EPS = 1e-06
ROPE_BASE = 10000.0
WIDE = 16
LANES = 128
MESH = pl.DeviceIdType.MESH
ANY = pl.BlockSpec(memory_space=pl.ANY)
NEG = -1e30


def remote(src, dst, send, recv, peer):
    return pltpu.make_async_remote_copy(
        src_ref=src, dst_ref=dst, send_sem=send, recv_sem=recv, device_id=peer, device_id_type=MESH
    )


def group_of(mesh, width):
    for size in (4, 2):
        if mesh.shape["sp"] % size == 0 and width % (size * LANES) == 0:
            return size
    return 1


def flip(c, mask):
    out = c
    if mask & 1:
        out = out + 1 - 2 * lax.rem(c, 2)
    if mask & 2:
        out = out + 2 - 4 * lax.rem(lax.div(c, 2), 2)
    return out


def layer_kernel(
    n_sp, n_tp, group, behind,
    hid_ref, gain_ref, freq_ref, wq_ref, wk_ref, wv_ref, wo_ref, post_ref,
    out_ref, lw_ref,
    raw, nrm, wq, wk, wv, wo, cos_t, sin_t, scr,
    qn_all, kw_all, vw_all, qr_all, kx_all, vx_all,
    acc1, m1, l1, acc4, m4, l4, acc16, m16, l16, b1, b4, b16,
    att, att_in, lw, lw_in, total, snd, rcv,
    local, near_s, near_r, line_s, line_r, dir_s, dir_r, across_s, across_r, twin_s, twin_r,
    early_s, early_r, late_s, late_r, back_s, back_r, swap_s, swap_r,
):
    f32, bf16 = jnp.float32, jnp.bfloat16
    s = lax.axis_index("sp")
    t = lax.axis_index("tp")
    rows, depth = hid_ref.shape
    all_rows = rows * group
    w_rows = wk_ref.shape[0]
    part = wq.shape[1]
    pairs = part // LANES
    steps = all_rows // WIDE
    few = rows // WIDE
    quarter = rows // 4
    count = n_sp // group
    c = lax.rem(s, group)
    base = s - c
    g = lax.div(s, group)
    half = lax.rem(t, 2)
    sibling = (s, t + 1 - 2 * half)
    masks = list(range(1, group))
    peer = {k: base + flip(c, k) for k in masks}
    up = lax.rem(s + group, n_sp)
    down = lax.rem(s + n_sp - group, n_sp)
    after = [lax.rem(s + b * group, n_sp) for b in range(1, behind + 1)]
    before = [lax.rem(s + n_sp - b * group, n_sp) for b in range(1, behind + 1)]
    start_row = pl.multiple_of(c * rows, rows)

    kept = [pltpu.make_async_copy(hid_ref, raw, local.at[0])]
    own_cols = pl.ds(pl.multiple_of(c * part, LANES), part)
    own_rows = pl.ds(pl.multiple_of(s * w_rows, w_rows), w_rows)
    kept.append(pltpu.make_async_copy(wq_ref.at[:, own_cols], wq, local.at[1]))
    for j, (src, dst) in enumerate(((wk_ref, wk), (wv_ref, wv))):
        kept.append(pltpu.make_async_copy(src.at[:, own_cols], dst.at[own_rows], local.at[2 + j]))
    for p in range(pairs):
        for i in range(group):
            kept.append(pltpu.make_async_copy(
                wo_ref.at[pl.ds(i * part + p * LANES, LANES)], wo.at[p, pl.ds(i * LANES, LANES)],
                local.at[4 + p * group + i],
            ))
    for copy in kept:
        copy.start()

    known = [(peer[k], t) for k in masks] + [(x, t) for x in after + before]
    known += [(s, lax.rem(t + k, n_tp)) for k in range(1, n_tp)]
    barrier = pltpu.get_barrier_semaphore()
    for other in known:
        pl.semaphore_signal(barrier, inc=1, device_id=other, device_id_type=MESH)

    half_dim = HEAD_DIM // 2
    lo = lax.broadcasted_iota(jnp.int32, (LANES, LANES), 0).astype(f32) * freq_ref[...]
    cos_lo, sin_lo = jnp.cos(lo), jnp.sin(lo)
    lane = lax.rem(lax.broadcasted_iota(jnp.int32, (1, LANES), 1), HEAD_DIM)
    sign = jnp.where(lane < half_dim, -1.0, 1.0)

    def fill(i, _):
        hi = (base * rows + i * LANES).astype(f32) * freq_ref[...]
        cos_hi, sin_hi = jnp.cos(hi), jnp.sin(hi)
        at = pl.ds(pl.multiple_of(i * LANES, LANES), LANES)
        cos_t[at, :] = cos_lo * cos_hi - sin_lo * sin_hi
        sin_t[at, :] = (sin_lo * cos_hi + cos_lo * sin_hi) * sign
        return 0

    lax.fori_loop(0, all_rows // LANES, fill, 0)

    @pl.when(g < behind)
    def _():
        for pair in range(pairs):
            for ref in (kw_all, vw_all):
                @pl.when(g < 1)
                def _(ref=ref, pair=pair):
                    ref[pair, pl.ds(0, SPAN), :] = jnp.zeros((SPAN, LANES), bf16)
            for ref in (kx_all, vx_all):
                for b in range(1, behind + 1):
                    @pl.when(g < b)
                    def _(ref=ref, pair=pair, b=b):
                        ref[pair, :, pl.ds((behind - b) * steps, steps), :] = jnp.zeros((WIDE, steps, LANES), bf16)

    pl.semaphore_wait(barrier, len(known))

    def near(k, j):
        src, dst = ((wk_ref, wk), (wv_ref, wv))[j]
        cols = pl.ds(pl.multiple_of(flip(c, k) * part, LANES), part)
        return remote(src.at[:, cols], dst.at[own_rows], near_s.at[j, k - 1], near_r.at[j, k - 1], (peer[k], t))

    def line(way, j, d):
        ref = (wk, wv)[j]
        to, off = ((up, g - d), (down, g + d))[way]
        off = jnp.clip(off, 0, count - 1)
        slot = ref.at[pl.ds(pl.multiple_of(off * group * w_rows, group * w_rows), group * w_rows)]
        return remote(slot, slot, line_s.at[way, j, d], line_r.at[way, j, d + 1], (to, t))

    def line_in(way, j, d):
        ref = (wk, wv)[j]
        off = jnp.clip((g - d, g + d)[way], 0, count - 1)
        slot = ref.at[pl.ds(pl.multiple_of(off * group * w_rows, group * w_rows), group * w_rows)]
        return remote(slot, slot, line_s.at[way, j, d - 1], line_r.at[way, j, d], ((up, down)[way], t))

    def has_in(way, d):
        return g >= d if way == 0 else g + d < count

    def has_out(way, d):
        if way == 0:
            return (g >= d) & (g + 1 < count)
        return (g + d < count) & (g >= 1)

    def pass_on(j, d):
        for way in range(2):
            if not (isinstance(d, int) and d == 0):
                @pl.when(has_in(way, d))
                def _(way=way):
                    line_in(way, j, d).wait_recv()

            if not (isinstance(d, int) and d == count - 1):
                @pl.when(has_out(way, d))
                def _(way=way):
                    line(way, j, d).start()

    def passed(j, d):
        for way in range(2):
            @pl.when(has_out(way, d))
            def _(way=way):
                line(way, j, d).wait_send()

    def piece(block, side, q):
        return nrm.at[pl.ds(pl.multiple_of(block * rows + side * (2 * quarter) + q * quarter, quarter), quarter)]

    def direct(k, q):
        slot = piece(c, half, q)
        return remote(slot, slot, dir_s.at[k - 1, q], dir_r.at[k - 1, q], (peer[k], t))

    def across(i):
        k, other = ((1, 2), (2, 1))[i]
        slot = piece(flip(c, k), half, i)
        return remote(slot, slot, across_s.at[i], across_r.at[i], (peer[other], t))

    def twin(k, q):
        slot = piece(flip(c, k), half, q)
        return remote(slot, slot, twin_s.at[k - 1, q], twin_r.at[k - 1, q], sibling)

    for j in range(2):
        for k in masks:
            near(k, j).start()
    firsts = {4: [(1, 0), (2, 1)], 2: [(1, 0)], 1: []}[group]
    seconds = {4: [(1, 1), (2, 0)], 2: [(1, 1)], 1: []}[group]
    thirds = {4: [(3, 0), (3, 1)], 2: [], 1: []}[group]
    def block_of(k):
        return flip(c, k) * rows

    kept[0].wait()

    def norm(i, _):
        x = raw[pl.ds(pl.multiple_of(i * quarter, quarter), quarter), :].astype(f32)
        scale = lax.rsqrt(jnp.mean(x * x, axis=-1, keepdims=True) + EPS)
        at = pl.ds(pl.multiple_of(start_row + i * quarter, quarter), quarter)
        nrm[at, :] = (x * scale * gain_ref[...]).astype(bf16)
        return 0

    lax.fori_loop(0, 4, norm, 0)

    def put_bias(ref, near_by, first_of):
        shape = ref.shape[1:]
        a = lax.broadcasted_iota(jnp.int32, shape, 0)
        b = lax.broadcasted_iota(jnp.int32, shape, 1)
        distance, place = near_by(a, b)
        band = (distance >= 0) & (distance <= SPAN)
        ref[0] = jnp.where(band & (place + first_of >= 0), 0.0, NEG).astype(f32)
        ref[1] = jnp.where(band, 0.0, NEG).astype(f32)

    def plain(a, b):
        return a + SPAN - b, b - SPAN

    def woven(a, b):
        return 4 * (a % 32 + 32 - b % 64) + a // 32 - b // 64, b % 64 - 32

    put_bias(b1, plain, g * all_rows)
    put_bias(b16, plain, g * steps)
    put_bias(b4, woven, g * steps)

    for k, q in firsts + seconds:
        direct(k, q).start()

    front = lax.rem(lax.broadcasted_iota(jnp.int32, (rows, LANES), 1), HEAD_DIM) < HEAD_DIM // 2

    def project(k, j):
        row = pl.multiple_of(block_of(k), rows)
        here = pl.ds(row, rows)
        out = jnp.dot(nrm[here, :], (wq, wk, wv)[j][...], preferred_element_type=f32)
        nat = (qn_all, kw_all, vw_all)[j]
        res = (qr_all, kx_all, vx_all)[j]
        skip = 0 if j == 0 else SPAN
        skip_res = 0 if j == 0 else behind * steps
        step = pl.multiple_of(lax.div(row, WIDE), few)
        for i in range(pairs):
            u = out[:, i * LANES:(i + 1) * LANES]
            if j < 2:
                swapped = jnp.where(
                    front,
                    pltpu.roll(u, LANES - HEAD_DIM // 2, 1),
                    pltpu.roll(u, HEAD_DIM // 2, 1),
                )
                u = u * cos_t[here, :] + swapped * sin_t[here, :]
            if j == 0:
                u = u * HEAD_DIM ** (-0.5)
            nat[i, pl.ds(row + skip, rows), :] = u.astype(bf16)
            scr[i] = u
        for i in range(pairs):
            for r in range(WIDE):
                res[i, 4 * (r % 4) + r // 4, pl.ds(step + skip_res, few), :] = scr[i, pl.ds(r, few, stride=WIDE), :].astype(bf16)

    for j in range(2):
        for k in masks:
            near(k, j).wait_recv()
        kept[2 + j].wait()
        pass_on(j, 0)

    kept[1].wait()
    project(0, 0)

    for k, q in firsts:
        direct(k, q).wait_recv()
        if group == 4:
            across(k - 1).start()
        twin(k, q).start()
    if count > 1:
        for j in range(2):
            pass_on(j, 1)
    for k, q in seconds:
        direct(k, q).wait_recv()
        twin(k, q).start()
    if count > 2:
        for j in range(2):
            pass_on(j, 2)
    for k in masks[:2]:
        for q in range(2):
            twin(k, q).wait_recv()
        project(k, 0)

    def far(j):
        if count > 3:
            pass_on(j, 3)
        if count > 4:
            lax.fori_loop(4, count, lambda d, _: (pass_on(j, d), 0)[1], 0)

    def early(pair, j):
        ref = (kw_all, vw_all)[j]
        return remote(
            ref.at[pair, pl.ds(all_rows, SPAN)], ref.at[pair, pl.ds(0, SPAN)],
            early_s.at[pair, j], early_r.at[pair, j], (after[0], t),
        )

    def late(pair, j, k, b):
        ref = (kx_all, vx_all)[j]
        at = pl.multiple_of(flip(c, k) * few, few)
        return remote(
            ref.at[pair, :, pl.ds(behind * steps + at, few)],
            ref.at[pair, :, pl.ds((behind - b) * steps + at, few)],
            late_s.at[pair, j, b - 1, k], late_r.at[pair, j, b - 1, k], (after[b - 1], t),
        )

    everything = [0] + masks

    def send_late(pair, j, k):
        for b in range(1, behind + 1):
            @pl.when(g + b < count)
            def _(b=b):
                late(pair, j, k, b).start()

    def send_early(pair, j):
        @pl.when(g + 1 < count)
        def _():
            early(pair, j).start()

    for j in range(2):
        far(j)
        for i, k in enumerate(everything[:3]):
            project(k, 1 + j)
            if i > 0:
                send_late(0, j, k - 1)
            elif j == 1:
                send_late(0, 0, everything[:3][-1])
    if group == 4:
        for k, q in thirds:
            across(q).wait_recv()
            twin(k, q).start()
        send_late(0, 1, 2)
        for q in range(2):
            twin(3, q).wait_recv()
        project(3, 1)
        project(3, 2)
        send_late(0, 0, 3)
        project(3, 0)
        send_late(0, 1, 3)
    else:
        send_late(0, 1, everything[-1])
    for j in range(2):
        send_early(0, j)

    def part_of(pair, j, u, b):
        ref = (kx_all, vx_all)[j]
        return remote(
            ref.at[pair, pl.ds(4 * u, 4), pl.ds(behind * steps, steps)],
            ref.at[pair, pl.ds(4 * u, 4), pl.ds((behind - b) * steps, steps)],
            late_s.at[pair, j, b - 1, u], late_r.at[pair, j, b - 1, u], (after[b - 1], t),
        )

    for pair in range(1, pairs):
        for j in range(2):
            send_early(pair, j)
        for u in range(4):
            for j in range(2):
                for b in range(1, behind + 1):
                    @pl.when(g + b < count)
                    def _(pair=pair, j=j, u=u, b=b):
                        part_of(pair, j, u, b).start()

    block = min(SPAN, steps)
    skip16 = behind * steps - SPAN

    def tile(q, k, v, bias):
        n = q.shape[0]
        low = lax.broadcasted_iota(jnp.int32, (n, LANES), 1) < HEAD_DIM
        low_q = low.astype(f32).astype(bf16)
        both = jnp.concatenate([q * low_q, q * (1 - low_q)], axis=0)
        sc = lax.dot_general(both, k, (((1,), (1,)), ((), ())), preferred_element_type=f32)
        sc = sc + jnp.concatenate([bias, bias], axis=0)
        m = jnp.max(sc, axis=-1, keepdims=True)
        e = jnp.exp(sc - m).astype(bf16)
        o = jnp.dot(e, jnp.concatenate([v, jnp.ones_like(v)], axis=1), preferred_element_type=f32)
        wide_m = jnp.broadcast_to(m, (2 * n, LANES))
        return (
            jnp.where(low, o[:n, :LANES], o[n:, :LANES]),
            jnp.where(low, wide_m[:n], wide_m[n:]),
            jnp.where(low, o[:n, LANES:], o[n:, LANES:]),
        )

    blocks16 = steps // block
    blocks4 = steps // 32

    def back(p, k):
        to = (peer[k], t)
        span = pl.ds(pl.multiple_of(flip(c, k) * rows, rows), rows)
        mine = pl.ds(pl.multiple_of(c * LANES, LANES), LANES)
        return (
            remote(att.at[p, span], att_in.at[p, :, mine], back_s.at[p, k - 1, 0], back_r.at[p, k - 1, 0], to),
            remote(lw.at[p, :, span], lw_in.at[c, p], back_s.at[p, k - 1, 1], back_r.at[p, k - 1, 1], to),
        )

    def mix_out(p):
        for copy in kept[4 + p * group:4 + (p + 1) * group]:
            copy.wait()
        for k in masks:
            for copy in back(p, k):
                copy.wait_recv()
        value = jnp.dot(att_in[p], wo[p], preferred_element_type=f32)
        total[...] = value if p == 0 else total[...] + value

    for p in range(pairs):
        qn, kw, vw, qr, kx, vx = (ref.at[p] for ref in (qn_all, kw_all, vw_all, qr_all, kx_all, vx_all))

        def step16(idx, _):
            slot = idx // blocks16
            i = idx % blocks16
            r = 4 * (slot % 4) + slot // 4
            at = pl.multiple_of(i * block, block)
            keys = pl.ds(at + skip16, block + SPAN)
            got = tile(
                qr[slot, pl.ds(at, block), :], kx[slot, keys, :], vx[slot, keys, :], b16[jnp.minimum(i, 1)]
            )
            for ref, value in zip((acc16, m16, l16), got):
                ref[pl.ds(r + WIDE * at, block, stride=WIDE), :] = value
            return 0

        def step4(r, i):
            at = i * 32
            low = at + behind * steps - 32
            if not isinstance(i, int):
                at = pl.multiple_of(at, 32)
                low = pl.multiple_of(low, 32)
            keys = pl.ds(low, 64)
            got = tile(
                jnp.concatenate([qr[4 * r + j, pl.ds(at, 32), :] for j in range(4)], axis=0),
                jnp.concatenate([kx[4 * r + j, keys, :] for j in range(4)], axis=0),
                jnp.concatenate([vx[4 * r + j, keys, :] for j in range(4)], axis=0),
                b4[0 if isinstance(i, int) else 1],
            )
            for ref, value in zip((acc4, m4, l4), got):
                for j in range(4):
                    ref[pl.ds(r + 4 * j + WIDE * at, 32, stride=WIDE), :] = value[j * 32:(j + 1) * 32]
            return 0

        def step1(i, _):
            at = pl.multiple_of(i * SPAN, SPAN)
            here = pl.ds(at, SPAN)
            keys = pl.ds(at, 2 * SPAN)
            got = tile(qn[here, :], kw[keys, :], vw[keys, :], b1[jnp.minimum(i, 1)])
            for ref, value in zip((acc1, m1, l1), got):
                ref[here, :] = value
            return 0

        def merge(i, _):
            here = pl.ds(pl.multiple_of(i * SPAN, SPAN), SPAN)
            tops = (m1[here, :], m4[here, :], m16[here, :])
            top = jnp.maximum(tops[0], jnp.maximum(tops[1], tops[2]))
            e1, e4, e16 = (jnp.exp(x - top) for x in tops)
            whole = l1[here, :] * e1 + l4[here, :] * e4 + l16[here, :] * e16
            mixed = acc1[here, :] * e1 + acc4[here, :] * e4 + acc16[here, :] * e16
            att[p, here, :] = (mixed / whole).astype(bf16)
            turned = jnp.transpose(top + jnp.log(whole))
            lw[p, 0:1, here] = turned[0:1]
            lw[p, 1:2, here] = turned[HEAD_DIM:HEAD_DIM + 1]
            return 0

        if blocks4 > 1:
            lax.fori_loop(
                0, 4 * (blocks4 - 1),
                lambda idx, _: step4(idx // (blocks4 - 1), idx % (blocks4 - 1) + 1), 0, unroll=2,
            )
        lax.fori_loop(1, all_rows // SPAN, step1, 0, unroll=2)
        for j in range(2):
            @pl.when(g >= 1)
            def _(j=j):
                early(p, j).wait_recv()
        step1(0, 0)
        if p > 0:
            mix_out(p - 1)
        if p == 0:
            for j in range(2):
                for b in range(1, behind + 1):
                    @pl.when(g >= b)
                    def _(j=j, b=b):
                        for k in everything:
                            late(0, j, k, b).wait_recv()
            lax.fori_loop(0, 4, lambda r, _: step4(r, 0), 0, unroll=2)
            lax.fori_loop(0, WIDE * blocks16, step16, 0, unroll=2)
        else:
            def chunk(u, _):
                for j in range(2):
                    for b in range(1, behind + 1):
                        @pl.when(g >= b)
                        def _(j=j, b=b):
                            part_of(p, j, u, b).wait_recv()
                step4(u, 0)
                lax.fori_loop(0, 4 * blocks16, lambda n, _: step16(4 * blocks16 * u + n, 0), 0, unroll=2)
                return 0

            lax.fori_loop(0, 4, chunk, 0)
        order = masks[::-1] + [0]
        tiles = rows // SPAN
        for i, k in enumerate(order):
            first = flip(c, k) * tiles
            lax.fori_loop(0, tiles, lambda n, _: merge(first + n, 0), 0, unroll=2)
            if i > 0:
                for copy in back(p, order[i - 1]):
                    copy.start()
        here = pl.ds(start_row, rows)
        mine = pl.ds(pl.multiple_of(c * LANES, LANES), LANES)
        att_in[p, :, mine] = att[p, here, :]
        lw_in[c, p] = lw[p, :, here]

    last = pairs - 1
    for copy in kept[4 + last * group:]:
        copy.wait()
    for k in masks:
        for copy in back(last, k):
            copy.wait_recv()
    share = rows // n_tp
    sub = share // 2

    def finish(owner, i):
        here = pl.ds(pl.multiple_of(owner * share + i * sub, sub), sub)
        value = jnp.dot(att_in[last, here, :], wo[last], preferred_element_type=f32)
        if last > 0:
            value = value + total[here, :]
        return value.astype(bf16)

    def swap(k, i):
        at = pl.ds(i * sub, sub)
        return remote(
            snd.at[k - 1, at], rcv.at[k - 1, at], swap_s.at[k - 1, i], swap_r.at[k - 1, i],
            (s, lax.rem(t + k, n_tp)),
        )

    waiting = []
    for k in range(1, n_tp):
        for i in range(2):
            snd[k - 1, pl.ds(i * sub, sub), :] = finish(lax.rem(t + k, n_tp), i)
            if waiting:
                waiting.pop().start()
            waiting.append(swap(k, i))
    for i in range(2):
        at = pl.ds(i * sub, sub)
        total[at, :] = finish(t, i).astype(f32)
        if waiting:
            waiting.pop().start()
    heads = 2 * pairs
    for i in range(group):
        for p in range(pairs):
            for h in range(2):
                row = i * heads + p * 2 + h
                lw_ref[row:row + 1, :] = lw_in[i, p, h:h + 1, :]
    for i in range(2):
        at = pl.ds(i * sub, sub)
        value = total[at, :]
        for k in range(1, n_tp):
            swap(k, i).wait_recv()
            value = value + rcv[k - 1, at, :].astype(f32)
        scale = lax.rsqrt(jnp.mean(value * value, axis=-1, keepdims=True) + EPS)
        out_ref[at, :] = (value * scale * post_ref[...]).astype(bf16)

    for k in range(1, n_tp):
        for i in range(2):
            swap(k, i).wait_send()
    for p in range(pairs):
        for k in masks:
            for copy in back(p, k):
                copy.wait_send()
    for j in range(2):
        for k in masks:
            near(k, j).wait_send()
        for d in range(min(count - 1, 4)):
            passed(j, d)
        if count > 5:
            lax.fori_loop(4, count - 1, lambda d, _, j=j: (passed(j, d), 0)[1], 0)
    for k, q in firsts + seconds:
        direct(k, q).wait_send()
        twin(k, q).wait_send()
    if group == 4:
        for i in range(2):
            across(i).wait_send()
            twin(3, i).wait_send()
    for pair in range(pairs):
        for j in range(2):
            @pl.when(g + 1 < count)
            def _(pair=pair, j=j):
                early(pair, j).wait_send()

            for b in range(1, behind + 1):
                @pl.when(g + b < count)
                def _(pair=pair, j=j, b=b):
                    if pair == 0:
                        for k in everything:
                            late(pair, j, k, b).wait_send()
                    else:
                        for u in range(4):
                            part_of(pair, j, u, b).wait_send()


def layer(mesh, group, behind, hidden, gain, freq, wq, wk, wv, wo, post):
    n_sp = mesh.shape["sp"]
    n_tp = mesh.shape["tp"]
    rows, depth = hidden.shape
    w_rows, width = wk.shape
    part = width // group
    pairs = part // LANES
    all_rows = rows * group
    steps = all_rows // WIDE
    block = min(SPAN, steps)
    count = n_sp // group
    share = rows // n_tp
    f32, bf16 = jnp.float32, jnp.bfloat16
    dma = pltpu.SemaphoreType.DMA
    state = pltpu.VMEM((all_rows, LANES), f32)
    weight = pltpu.VMEM((depth, part), bf16)
    table = pltpu.VMEM((all_rows, LANES), f32)
    ring = pltpu.VMEM((pairs, SPAN + all_rows, LANES), bf16)
    woven = pltpu.VMEM((pairs, WIDE, (behind + 1) * steps, LANES), bf16)
    pieces = pltpu.VMEM((n_tp - 1, share, depth), bf16)
    vmem = pl.BlockSpec(memory_space=pltpu.VMEM)
    near = max(group - 1, 1)
    return pl.pallas_call(
        functools.partial(layer_kernel, n_sp, n_tp, group, behind),
        out_shape=(
            jax.ShapeDtypeStruct((share, depth), bf16),
            jax.ShapeDtypeStruct((width // HEAD_DIM, rows), f32),
        ),
        in_specs=[ANY, vmem, vmem, ANY, ANY, ANY, ANY, vmem],
        out_specs=(vmem, vmem),
        scratch_shapes=[
            pltpu.VMEM((rows, depth), bf16), pltpu.VMEM((all_rows, depth), bf16),
            weight, weight, weight, pltpu.VMEM((pairs, group * LANES, depth), bf16), table, table,
            pltpu.VMEM((pairs, rows, LANES), f32),
            pltpu.VMEM((pairs, all_rows, LANES), bf16), ring, ring,
            pltpu.VMEM((pairs, WIDE, steps, LANES), bf16), woven, woven,
            state, state, state, state, state, state, state, state, state,
            pltpu.VMEM((2, SPAN, 2 * SPAN), f32),
            pltpu.VMEM((2, SPAN, 2 * SPAN), f32),
            pltpu.VMEM((2, block, block + SPAN), f32),
            pltpu.VMEM((pairs, all_rows, LANES), bf16), pltpu.VMEM((pairs, rows, group * LANES), bf16),
            pltpu.VMEM((pairs, 2, all_rows), f32), pltpu.VMEM((group, pairs, 2, rows), f32),
            pltpu.VMEM((rows, depth), f32), pieces, pieces,
            dma((4 + pairs * group,)),
            dma((2, near)), dma((2, near)), dma((2, 2, count)), dma((2, 2, count)),
            dma((2, 2)), dma((2, 2)), dma((2,)), dma((2,)), dma((3, 2)), dma((3, 2)),
            dma((pairs, 2)), dma((pairs, 2)),
            dma((pairs, 2, behind, 4)), dma((pairs, 2, behind, 4)),
            dma((pairs, near, 2)), dma((pairs, near, 2)), dma((n_tp - 1, 2)), dma((n_tp - 1, 2)),
        ],
        compiler_params=pltpu.CompilerParams(
            vmem_limit_bytes=63 * 1024 * 1024, collective_id=0, has_side_effects=True
        ),
        name="layer_core",
    )(hidden, gain, freq, wq, wk, wv, wo, post)


def body(mesh, hidden_in, pre_gain, query_proj, key_proj, value_proj, out_proj, post_gain):
    rows, depth = hidden_in.shape
    width = query_proj.shape[1]
    group = group_of(mesh, width)
    all_rows = rows * group
    behind = -(-(WIDE * SPAN) // all_rows)
    half_dim = HEAD_DIM // 2
    frequency = ROPE_BASE ** (-(jnp.arange(half_dim, dtype=jnp.float32) * 2.0 / HEAD_DIM))
    freq = jnp.concatenate([frequency] * (LANES // half_dim))[None, :]
    return layer(
        mesh, group, behind, hidden_in, pre_gain[None, :], freq,
        query_proj, key_proj, value_proj, out_proj, post_gain[None, :],
    )


def solution(mesh):
    placed = (P("sp", None), P(), P(None, "tp"), P("sp", "tp"), P("sp", "tp"), P("tp", None), P())
    return jax.shard_map(
        functools.partial(body, mesh),
        mesh=mesh,
        in_specs=placed,
        out_specs=(P(("sp", "tp"), None), P("tp", "sp")),
        check_vma=False,
    )
```

```python
import functools

import jax
import jax.numpy as jnp
from jax import lax
from jax.experimental import pallas as pl
from jax.experimental.pallas import tpu as pltpu
from jax.sharding import PartitionSpec as P

HEAD_DIM = 64
SPAN = 128
EPS = 1e-06
ROPE_BASE = 10000.0
WIDE = 16
LANES = 128
MESH = pl.DeviceIdType.MESH
ANY = pl.BlockSpec(memory_space=pl.ANY)
NEG = -1e30


def remote(src, dst, send, recv, peer):
    return pltpu.make_async_remote_copy(
        src_ref=src, dst_ref=dst, send_sem=send, recv_sem=recv, device_id=peer, device_id_type=MESH
    )


def group_of(mesh, width):
    for size in (4, 2):
        if mesh.shape["sp"] % size == 0 and width % (size * LANES) == 0:
            return size
    return 1


def flip(c, mask):
    out = c
    if mask & 1:
        out = out + 1 - 2 * lax.rem(c, 2)
    if mask & 2:
        out = out + 2 - 4 * lax.rem(lax.div(c, 2), 2)
    return out


def layer_kernel(
    n_sp, n_tp, group, behind,
    hid_ref, gain_ref, freq_ref, wq_ref, wk_ref, wv_ref, wo_ref, post_ref,
    out_ref, lw_ref,
    raw, nrm, wq, wk, wv, wo, cos_t, sin_t, scr,
    qn_all, kw_all, vw_all, qr_all, kx_all, vx_all,
    acc1, m1, l1, acc4, m4, l4, acc16, m16, l16, b1, b4, b16,
    att, att_in, lw, lw_in, total, snd, rcv,
    local, near_s, near_r, line_s, line_r, dir_s, dir_r, across_s, across_r, twin_s, twin_r,
    early_s, early_r, late_s, late_r, back_s, back_r, swap_s, swap_r,
):
    f32, bf16 = jnp.float32, jnp.bfloat16
    s = lax.axis_index("sp")
    t = lax.axis_index("tp")
    rows, depth = hid_ref.shape
    all_rows = rows * group
    w_rows = wk_ref.shape[0]
    part = wq.shape[1]
    pairs = part // LANES
    steps = all_rows // WIDE
    few = rows // WIDE
    quarter = rows // 4
    count = n_sp // group
    c = lax.rem(s, group)
    base = s - c
    g = lax.div(s, group)
    half = lax.rem(t, 2)
    sibling = (s, t + 1 - 2 * half)
    masks = list(range(1, group))
    peer = {k: base + flip(c, k) for k in masks}
    up = lax.rem(s + group, n_sp)
    down = lax.rem(s + n_sp - group, n_sp)
    after = [lax.rem(s + b * group, n_sp) for b in range(1, behind + 1)]
    before = [lax.rem(s + n_sp - b * group, n_sp) for b in range(1, behind + 1)]
    start_row = pl.multiple_of(c * rows, rows)

    kept = [pltpu.make_async_copy(hid_ref, raw, local.at[0])]
    own_cols = pl.ds(pl.multiple_of(c * part, LANES), part)
    own_rows = pl.ds(pl.multiple_of(s * w_rows, w_rows), w_rows)
    kept.append(pltpu.make_async_copy(wq_ref.at[:, own_cols], wq, local.at[1]))
    for j, (src, dst) in enumerate(((wk_ref, wk), (wv_ref, wv))):
        kept.append(pltpu.make_async_copy(src.at[:, own_cols], dst.at[own_rows], local.at[2 + j]))
    for p in range(pairs):
        for i in range(group):
            kept.append(pltpu.make_async_copy(
                wo_ref.at[pl.ds(i * part + p * LANES, LANES)], wo.at[p, pl.ds(i * LANES, LANES)],
                local.at[4 + p * group + i],
            ))
    for copy in kept:
        copy.start()

    known = [(peer[k], t) for k in masks] + [(x, t) for x in after + before]
    known += [(s, lax.rem(t + k, n_tp)) for k in range(1, n_tp)]
    barrier = pltpu.get_barrier_semaphore()
    for other in known:
        pl.semaphore_signal(barrier, inc=1, device_id=other, device_id_type=MESH)

    half_dim = HEAD_DIM // 2
    lo = lax.broadcasted_iota(jnp.int32, (LANES, LANES), 0).astype(f32) * freq_ref[...]
    cos_lo, sin_lo = jnp.cos(lo), jnp.sin(lo)
    lane = lax.rem(lax.broadcasted_iota(jnp.int32, (1, LANES), 1), HEAD_DIM)
    sign = jnp.where(lane < half_dim, -1.0, 1.0)

    def fill(i, _):
        hi = (base * rows + i * LANES).astype(f32) * freq_ref[...]
        cos_hi, sin_hi = jnp.cos(hi), jnp.sin(hi)
        at = pl.ds(pl.multiple_of(i * LANES, LANES), LANES)
        cos_t[at, :] = cos_lo * cos_hi - sin_lo * sin_hi
        sin_t[at, :] = (sin_lo * cos_hi + cos_lo * sin_hi) * sign
        return 0

    lax.fori_loop(0, all_rows // LANES, fill, 0)

    @pl.when(g < behind)
    def _():
        for pair in range(pairs):
            for ref in (kw_all, vw_all):
                @pl.when(g < 1)
                def _(ref=ref, pair=pair):
                    ref[pair, pl.ds(0, SPAN), :] = jnp.zeros((SPAN, LANES), bf16)
            for ref in (kx_all, vx_all):
                for b in range(1, behind + 1):
                    @pl.when(g < b)
                    def _(ref=ref, pair=pair, b=b):
                        ref[pair, :, pl.ds((behind - b) * steps, steps), :] = jnp.zeros((WIDE, steps, LANES), bf16)

    pl.semaphore_wait(barrier, len(known))

    def near(k, j):
        src, dst = ((wk_ref, wk), (wv_ref, wv))[j]
        cols = pl.ds(pl.multiple_of(flip(c, k) * part, LANES), part)
        return remote(src.at[:, cols], dst.at[own_rows], near_s.at[j, k - 1], near_r.at[j, k - 1], (peer[k], t))

    def line(way, j, d):
        ref = (wk, wv)[j]
        to, off = ((up, g - d), (down, g + d))[way]
        off = jnp.clip(off, 0, count - 1)
        slot = ref.at[pl.ds(pl.multiple_of(off * group * w_rows, group * w_rows), group * w_rows)]
        return remote(slot, slot, line_s.at[way, j, d], line_r.at[way, j, d + 1], (to, t))

    def line_in(way, j, d):
        ref = (wk, wv)[j]
        off = jnp.clip((g - d, g + d)[way], 0, count - 1)
        slot = ref.at[pl.ds(pl.multiple_of(off * group * w_rows, group * w_rows), group * w_rows)]
        return remote(slot, slot, line_s.at[way, j, d - 1], line_r.at[way, j, d], ((up, down)[way], t))

    def has_in(way, d):
        return g >= d if way == 0 else g + d < count

    def has_out(way, d):
        if way == 0:
            return (g >= d) & (g + 1 < count)
        return (g + d < count) & (g >= 1)

    def pass_on(j, d):
        for way in range(2):
            if not (isinstance(d, int) and d == 0):
                @pl.when(has_in(way, d))
                def _(way=way):
                    line_in(way, j, d).wait_recv()

            if not (isinstance(d, int) and d == count - 1):
                @pl.when(has_out(way, d))
                def _(way=way):
                    line(way, j, d).start()

    def passed(j, d):
        for way in range(2):
            @pl.when(has_out(way, d))
            def _(way=way):
                line(way, j, d).wait_send()

    def piece(block, side, q):
        return nrm.at[pl.ds(pl.multiple_of(block * rows + side * (2 * quarter) + q * quarter, quarter), quarter)]

    def direct(k, q):
        slot = piece(c, half, q)
        return remote(slot, slot, dir_s.at[k - 1, q], dir_r.at[k - 1, q], (peer[k], t))

    def across(i):
        k, other = ((1, 2), (2, 1))[i]
        slot = piece(flip(c, k), half, i)
        return remote(slot, slot, across_s.at[i], across_r.at[i], (peer[other], t))

    def twin(k, q):
        slot = piece(flip(c, k), half, q)
        return remote(slot, slot, twin_s.at[k - 1, q], twin_r.at[k - 1, q], sibling)

    for j in range(2):
        for k in masks:
            near(k, j).start()
    firsts = {4: [(1, 0), (2, 1)], 2: [(1, 0)], 1: []}[group]
    seconds = {4: [(1, 1), (2, 0)], 2: [(1, 1)], 1: []}[group]
    thirds = {4: [(3, 0), (3, 1)], 2: [], 1: []}[group]
    def block_of(k):
        return flip(c, k) * rows

    kept[0].wait()

    def norm(i, _):
        x = raw[pl.ds(pl.multiple_of(i * quarter, quarter), quarter), :].astype(f32)
        scale = lax.rsqrt(jnp.mean(x * x, axis=-1, keepdims=True) + EPS)
        at = pl.ds(pl.multiple_of(start_row + i * quarter, quarter), quarter)
        nrm[at, :] = (x * scale * gain_ref[...]).astype(bf16)
        return 0

    lax.fori_loop(0, 4, norm, 0)

    def put_bias(ref, near_by, first_of):
        shape = ref.shape[1:]
        a = lax.broadcasted_iota(jnp.int32, shape, 0)
        b = lax.broadcasted_iota(jnp.int32, shape, 1)
        distance, place = near_by(a, b)
        band = (distance >= 0) & (distance <= SPAN)
        ref[0] = jnp.where(band & (place + first_of >= 0), 0.0, NEG).astype(f32)
        ref[1] = jnp.where(band, 0.0, NEG).astype(f32)

    def plain(a, b):
        return a + SPAN - b, b - SPAN

    def woven(a, b):
        return 4 * (a % 32 + 32 - b % 64) + a // 32 - b // 64, b % 64 - 32

    put_bias(b1, plain, g * all_rows)
    a16 = lax.broadcasted_iota(jnp.int32, (few, few + SPAN), 0)
    k16 = lax.broadcasted_iota(jnp.int32, (few, few + SPAN), 1)
    for i in range(group):
        band = (a16 + SPAN >= k16) & (a16 <= k16)
        seen = g * steps + i * few + k16 >= SPAN
        b16[i] = jnp.where(band & seen, 0.0, NEG).astype(f32)
    put_bias(b4, woven, g * steps)

    for k, q in firsts + seconds:
        direct(k, q).start()

    front = lax.rem(lax.broadcasted_iota(jnp.int32, (rows, LANES), 1), HEAD_DIM) < HEAD_DIM // 2

    def project(k, j):
        row = pl.multiple_of(block_of(k), rows)
        here = pl.ds(row, rows)
        out = jnp.dot(nrm[here, :], (wq, wk, wv)[j][...], preferred_element_type=f32)
        nat = (qn_all, kw_all, vw_all)[j]
        res = (qr_all, kx_all, vx_all)[j]
        skip = 0 if j == 0 else SPAN
        skip_res = 0 if j == 0 else behind * steps
        step = pl.multiple_of(lax.div(row, WIDE), few)
        for i in range(pairs):
            u = out[:, i * LANES:(i + 1) * LANES]
            if j < 2:
                swapped = jnp.where(
                    front,
                    pltpu.roll(u, LANES - HEAD_DIM // 2, 1),
                    pltpu.roll(u, HEAD_DIM // 2, 1),
                )
                u = u * cos_t[here, :] + swapped * sin_t[here, :]
            if j == 0:
                u = u * HEAD_DIM ** (-0.5)
            nat[i, pl.ds(row + skip, rows), :] = u.astype(bf16)
            scr[i] = u
        for i in range(pairs):
            for r in range(WIDE):
                res[i, 4 * (r % 4) + r // 4, pl.ds(step + skip_res, few), :] = scr[i, pl.ds(r, few, stride=WIDE), :].astype(bf16)

    for j in range(2):
        for k in masks:
            near(k, j).wait_recv()
        kept[2 + j].wait()
        pass_on(j, 0)

    kept[1].wait()
    project(0, 0)

    for k, q in firsts:
        direct(k, q).wait_recv()
        if group == 4:
            across(k - 1).start()
        twin(k, q).start()
    if count > 1:
        for j in range(2):
            pass_on(j, 1)
    for k, q in seconds:
        direct(k, q).wait_recv()
        twin(k, q).start()
    if count > 2:
        for j in range(2):
            pass_on(j, 2)
    for k in masks[:2]:
        for q in range(2):
            twin(k, q).wait_recv()
        project(k, 0)

    def far(j):
        if count > 3:
            pass_on(j, 3)
        if count > 4:
            lax.fori_loop(4, count, lambda d, _: (pass_on(j, d), 0)[1], 0)

    def early(pair, j):
        ref = (kw_all, vw_all)[j]
        return remote(
            ref.at[pair, pl.ds(all_rows, SPAN)], ref.at[pair, pl.ds(0, SPAN)],
            early_s.at[pair, j], early_r.at[pair, j], (after[0], t),
        )

    def late(pair, j, block, b):
        ref = (kx_all, vx_all)[j]
        at = pl.multiple_of(block * few, few)
        return remote(
            ref.at[pair, :, pl.ds(behind * steps + at, few)],
            ref.at[pair, :, pl.ds((behind - b) * steps + at, few)],
            late_s.at[pair, j, b - 1, block], late_r.at[pair, j, b - 1, block], (after[b - 1], t),
        )

    everything = [0] + masks

    def send_late(pair, j, k):
        for b in range(1, behind + 1):
            @pl.when(g + b < count)
            def _(b=b):
                late(pair, j, flip(c, k), b).start()

    def send_early(pair, j):
        @pl.when(g + 1 < count)
        def _():
            early(pair, j).start()

    for j in range(2):
        far(j)
        for i, k in enumerate(everything[:3]):
            project(k, 1 + j)
            if i > 0:
                send_late(0, j, k - 1)
            elif j == 1:
                send_late(0, 0, everything[:3][-1])
    if group == 4:
        for k, q in thirds:
            across(q).wait_recv()
            twin(k, q).start()
        send_late(0, 1, 2)
        for q in range(2):
            twin(3, q).wait_recv()
        project(3, 1)
        project(3, 2)
        send_late(0, 0, 3)
        project(3, 0)
        send_late(0, 1, 3)
    else:
        send_late(0, 1, everything[-1])
    for j in range(2):
        send_early(0, j)

    for pair in range(1, pairs):
        for j in range(2):
            send_early(pair, j)
        for block in range(group)[::-1]:
            for b in range(1, behind + 1):
                @pl.when(g + b < count)
                def _(pair=pair, block=block, b=b):
                    for j in range(2):
                        late(pair, j, block, b).start()

    skip16 = behind * steps - SPAN

    def tile(q, k, v, bias):
        n = q.shape[0]
        low = lax.broadcasted_iota(jnp.int32, (n, LANES), 1) < HEAD_DIM
        low_q = low.astype(f32).astype(bf16)
        both = jnp.concatenate([q * low_q, q * (1 - low_q)], axis=0)
        sc = lax.dot_general(both, k, (((1,), (1,)), ((), ())), preferred_element_type=f32)
        sc = sc + jnp.concatenate([bias, bias], axis=0)
        m = jnp.max(sc, axis=-1, keepdims=True)
        e = jnp.exp(sc - m).astype(bf16)
        o = jnp.dot(e, jnp.concatenate([v, jnp.ones_like(v)], axis=1), preferred_element_type=f32)
        wide_m = jnp.broadcast_to(m, (2 * n, LANES))
        return (
            jnp.where(low, o[:n, :LANES], o[n:, :LANES]),
            jnp.where(low, wide_m[:n], wide_m[n:]),
            jnp.where(low, o[:n, LANES:], o[n:, LANES:]),
        )

    blocks4 = steps // 32

    def back(p, block):
        to = (base + block, t)
        span = pl.ds(block * rows, rows)
        mine = pl.ds(pl.multiple_of(c * LANES, LANES), LANES)
        return (
            remote(att.at[p, span], att_in.at[p, :, mine], back_s.at[p, block, 0], back_r.at[p, c, 0], to),
            remote(lw.at[p, :, span], lw_in.at[c, p], back_s.at[p, block, 1], back_r.at[p, c, 1], to),
        )

    def back_in(p, k):
        of = flip(c, k)
        theirs = pl.ds(pl.multiple_of(of * LANES, LANES), LANES)
        return (
            remote(
                att_in.at[p, :, theirs], att_in.at[p, :, theirs], back_s.at[p, 0, 0], back_r.at[p, of, 0], (peer[k], t)
            ),
            remote(lw_in.at[of, p], lw_in.at[of, p], back_s.at[p, 0, 1], back_r.at[p, of, 1], (peer[k], t)),
        )

    def mix_out(p):
        for copy in kept[4 + p * group:4 + (p + 1) * group]:
            copy.wait()
        for k in masks:
            for copy in back_in(p, k):
                copy.wait_recv()
        value = jnp.dot(att_in[p], wo[p], preferred_element_type=f32)
        total[...] = value if p == 0 else total[...] + value

    for p in range(pairs):
        qn, kw, vw, qr, kx, vx = (ref.at[p] for ref in (qn_all, kw_all, vw_all, qr_all, kx_all, vx_all))

        def step16(block, slot):
            r = 4 * (slot % 4) + slot // 4
            at = block * few
            keys = pl.ds(at + skip16, few + SPAN)
            got = tile(qr[slot, pl.ds(at, few), :], kx[slot, keys, :], vx[slot, keys, :], b16[block])
            for ref, value in zip((acc16, m16, l16), got):
                ref[pl.ds(r + WIDE * at, few, stride=WIDE), :] = value
            return 0

        def step4(r, i):
            at = i * 32
            low = at + behind * steps - 32
            if not isinstance(i, int):
                at = pl.multiple_of(at, 32)
                low = pl.multiple_of(low, 32)
            keys = pl.ds(low, 64)
            got = tile(
                jnp.concatenate([qr[4 * r + j, pl.ds(at, 32), :] for j in range(4)], axis=0),
                jnp.concatenate([kx[4 * r + j, keys, :] for j in range(4)], axis=0),
                jnp.concatenate([vx[4 * r + j, keys, :] for j in range(4)], axis=0),
                b4[0 if isinstance(i, int) else 1],
            )
            for ref, value in zip((acc4, m4, l4), got):
                for j in range(4):
                    ref[pl.ds(r + 4 * j + WIDE * at, 32, stride=WIDE), :] = value[j * 32:(j + 1) * 32]
            return 0

        def step1(i, _):
            at = pl.multiple_of(i * SPAN, SPAN)
            here = pl.ds(at, SPAN)
            keys = pl.ds(at, 2 * SPAN)
            got = tile(qn[here, :], kw[keys, :], vw[keys, :], b1[jnp.minimum(i, 1)])
            for ref, value in zip((acc1, m1, l1), got):
                ref[here, :] = value
            return 0

        def merge(i, _):
            here = pl.ds(pl.multiple_of(i * SPAN, SPAN), SPAN)
            tops = (m1[here, :], m4[here, :], m16[here, :])
            top = jnp.maximum(tops[0], jnp.maximum(tops[1], tops[2]))
            e1, e4, e16 = (jnp.exp(x - top) for x in tops)
            whole = l1[here, :] * e1 + l4[here, :] * e4 + l16[here, :] * e16
            mixed = acc1[here, :] * e1 + acc4[here, :] * e4 + acc16[here, :] * e16
            att[p, here, :] = (mixed / whole).astype(bf16)
            turned = jnp.transpose(top + jnp.log(whole))
            lw[p, 0:1, here] = turned[0:1]
            lw[p, 1:2, here] = turned[HEAD_DIM:HEAD_DIM + 1]
            return 0

        if blocks4 > 1:
            lax.fori_loop(
                0, 4 * (blocks4 - 1),
                lambda idx, _: step4(idx // (blocks4 - 1), idx % (blocks4 - 1) + 1), 0, unroll=4,
            )
        plains = all_rows // SPAN - 1
        lax.fori_loop(1, plains + 1, step1, 0, unroll=max(x for x in range(1, 6) if plains % x == 0))
        if p > 0:
            mix_out(p - 1)
        tiles = rows // SPAN
        for block in range(group)[::-1]:
            for b in range(1, behind + 1):
                for h in range(group):
                    age = (behind - b) * group + h
                    if age == block or (block == group - 1 and age > block):
                        @pl.when(g >= b)
                        def _(b=b, h=h):
                            for j in range(2):
                                late(p, j, h, b).wait_recv()
            if block == group - 1:
                lax.fori_loop(0, 4, lambda r, _: step4(r, 0), 0, unroll=4)
                for j in range(2):
                    @pl.when(g >= 1)
                    def _(j=j):
                        early(p, j).wait_recv()
                step1(0, 0)
            lax.fori_loop(0, WIDE, lambda n, _, block=block: step16(block, n), 0, unroll=4)
            lax.fori_loop(0, tiles, lambda n, _, block=block: merge(block * tiles + n, 0), 0, unroll=4)

            @pl.when(c != block)
            def _(block=block):
                for copy in back(p, block):
                    copy.start()

        here = pl.ds(start_row, rows)
        mine = pl.ds(pl.multiple_of(c * LANES, LANES), LANES)
        att_in[p, :, mine] = att[p, here, :]
        lw_in[c, p] = lw[p, :, here]

    last = pairs - 1
    for copy in kept[4 + last * group:]:
        copy.wait()
    for k in masks:
        for copy in back_in(last, k):
            copy.wait_recv()
    share = rows // n_tp
    sub = share // 2

    def finish(owner, i):
        here = pl.ds(pl.multiple_of(owner * share + i * sub, sub), sub)
        value = jnp.dot(att_in[last, here, :], wo[last], preferred_element_type=f32)
        if last > 0:
            value = value + total[here, :]
        return value.astype(bf16)

    def swap(k, i):
        at = pl.ds(i * sub, sub)
        return remote(
            snd.at[k - 1, at], rcv.at[k - 1, at], swap_s.at[k - 1, i], swap_r.at[k - 1, i],
            (s, lax.rem(t + k, n_tp)),
        )

    waiting = []
    for k in range(1, n_tp):
        for i in range(2):
            snd[k - 1, pl.ds(i * sub, sub), :] = finish(lax.rem(t + k, n_tp), i)
            if waiting:
                waiting.pop().start()
            waiting.append(swap(k, i))
    for i in range(2):
        at = pl.ds(i * sub, sub)
        total[at, :] = finish(t, i).astype(f32)
        if waiting:
            waiting.pop().start()
    heads = 2 * pairs
    for i in range(group):
        for p in range(pairs):
            for h in range(2):
                row = i * heads + p * 2 + h
                lw_ref[row:row + 1, :] = lw_in[i, p, h:h + 1, :]
    for i in range(2):
        at = pl.ds(i * sub, sub)
        value = total[at, :]
        for k in range(1, n_tp):
            swap(k, i).wait_recv()
            value = value + rcv[k - 1, at, :].astype(f32)
        scale = lax.rsqrt(jnp.mean(value * value, axis=-1, keepdims=True) + EPS)
        out_ref[at, :] = (value * scale * post_ref[...]).astype(bf16)

    for k in range(1, n_tp):
        for i in range(2):
            swap(k, i).wait_send()
    for p in range(pairs):
        for block in range(group):
            @pl.when(c != block)
            def _(p=p, block=block):
                for copy in back(p, block):
                    copy.wait_send()
    for j in range(2):
        for k in masks:
            near(k, j).wait_send()
        for d in range(min(count - 1, 4)):
            passed(j, d)
        if count > 5:
            lax.fori_loop(4, count - 1, lambda d, _, j=j: (passed(j, d), 0)[1], 0)
    for k, q in firsts + seconds:
        direct(k, q).wait_send()
        twin(k, q).wait_send()
    if group == 4:
        for i in range(2):
            across(i).wait_send()
            twin(3, i).wait_send()
    for pair in range(pairs):
        for j in range(2):
            @pl.when(g + 1 < count)
            def _(pair=pair, j=j):
                early(pair, j).wait_send()

            for b in range(1, behind + 1):
                @pl.when(g + b < count)
                def _(pair=pair, j=j, b=b):
                    for block in range(group):
                        late(pair, j, block, b).wait_send()


def layer(mesh, group, behind, hidden, gain, freq, wq, wk, wv, wo, post):
    n_sp = mesh.shape["sp"]
    n_tp = mesh.shape["tp"]
    rows, depth = hidden.shape
    w_rows, width = wk.shape
    part = width // group
    pairs = part // LANES
    all_rows = rows * group
    steps = all_rows // WIDE
    few = rows // WIDE
    count = n_sp // group
    share = rows // n_tp
    f32, bf16 = jnp.float32, jnp.bfloat16
    dma = pltpu.SemaphoreType.DMA
    state = pltpu.VMEM((all_rows, LANES), f32)
    weight = pltpu.VMEM((depth, part), bf16)
    table = pltpu.VMEM((all_rows, LANES), f32)
    ring = pltpu.VMEM((pairs, SPAN + all_rows, LANES), bf16)
    woven = pltpu.VMEM((pairs, WIDE, (behind + 1) * steps, LANES), bf16)
    pieces = pltpu.VMEM((n_tp - 1, share, depth), bf16)
    vmem = pl.BlockSpec(memory_space=pltpu.VMEM)
    near = max(group - 1, 1)
    return pl.pallas_call(
        functools.partial(layer_kernel, n_sp, n_tp, group, behind),
        out_shape=(
            jax.ShapeDtypeStruct((share, depth), bf16),
            jax.ShapeDtypeStruct((width // HEAD_DIM, rows), f32),
        ),
        in_specs=[ANY, vmem, vmem, ANY, ANY, ANY, ANY, vmem],
        out_specs=(vmem, vmem),
        scratch_shapes=[
            pltpu.VMEM((rows, depth), bf16), pltpu.VMEM((all_rows, depth), bf16),
            weight, weight, weight, pltpu.VMEM((pairs, group * LANES, depth), bf16), table, table,
            pltpu.VMEM((pairs, rows, LANES), f32),
            pltpu.VMEM((pairs, all_rows, LANES), bf16), ring, ring,
            pltpu.VMEM((pairs, WIDE, steps, LANES), bf16), woven, woven,
            state, state, state, state, state, state, state, state, state,
            pltpu.VMEM((2, SPAN, 2 * SPAN), f32),
            pltpu.VMEM((2, SPAN, 2 * SPAN), f32),
            pltpu.VMEM((group, few, few + SPAN), f32),
            pltpu.VMEM((pairs, all_rows, LANES), bf16), pltpu.VMEM((pairs, rows, group * LANES), bf16),
            pltpu.VMEM((pairs, 2, all_rows), f32), pltpu.VMEM((group, pairs, 2, rows), f32),
            pltpu.VMEM((rows, depth), f32), pieces, pieces,
            dma((4 + pairs * group,)),
            dma((2, near)), dma((2, near)), dma((2, 2, count)), dma((2, 2, count)),
            dma((2, 2)), dma((2, 2)), dma((2,)), dma((2,)), dma((3, 2)), dma((3, 2)),
            dma((pairs, 2)), dma((pairs, 2)),
            dma((pairs, 2, behind, group)), dma((pairs, 2, behind, group)),
            dma((pairs, group, 2)), dma((pairs, group, 2)), dma((n_tp - 1, 2)), dma((n_tp - 1, 2)),
        ],
        compiler_params=pltpu.CompilerParams(
            vmem_limit_bytes=63 * 1024 * 1024, collective_id=0, has_side_effects=True
        ),
        name="layer_core",
    )(hidden, gain, freq, wq, wk, wv, wo, post)


def body(mesh, hidden_in, pre_gain, query_proj, key_proj, value_proj, out_proj, post_gain):
    rows, depth = hidden_in.shape
    width = query_proj.shape[1]
    group = group_of(mesh, width)
    all_rows = rows * group
    behind = -(-(WIDE * SPAN) // all_rows)
    half_dim = HEAD_DIM // 2
    frequency = ROPE_BASE ** (-(jnp.arange(half_dim, dtype=jnp.float32) * 2.0 / HEAD_DIM))
    freq = jnp.concatenate([frequency] * (LANES // half_dim))[None, :]
    return layer(
        mesh, group, behind, hidden_in, pre_gain[None, :], freq,
        query_proj, key_proj, value_proj, out_proj, post_gain[None, :],
    )


def solution(mesh):
    placed = (P("sp", None), P(), P(None, "tp"), P("sp", "tp"), P("sp", "tp"), P("tp", None), P())
    return jax.shard_map(
        functools.partial(body, mesh),
        mesh=mesh,
        in_specs=placed,
        out_specs=(P(("sp", "tp"), None), P("tp", "sp")),
        check_vma=False,
    )
```

```python
import functools

import jax
import jax.numpy as jnp
from jax import lax
from jax.experimental import pallas as pl
from jax.experimental.pallas import tpu as pltpu
from jax.sharding import PartitionSpec as P

HEAD_DIM = 64
SPAN = 128
EPS = 1e-06
ROPE_BASE = 10000.0
WIDE = 16
LANES = 128
MESH = pl.DeviceIdType.MESH
ANY = pl.BlockSpec(memory_space=pl.ANY)
NEG = -1e30


def remote(src, dst, send, recv, peer):
    return pltpu.make_async_remote_copy(
        src_ref=src, dst_ref=dst, send_sem=send, recv_sem=recv, device_id=peer, device_id_type=MESH
    )


def group_of(mesh, width):
    for size in (4, 2):
        if mesh.shape["sp"] % size == 0 and width % (size * LANES) == 0:
            return size
    return 1


def flip(c, mask):
    out = c
    if mask & 1:
        out = out + 1 - 2 * lax.rem(c, 2)
    if mask & 2:
        out = out + 2 - 4 * lax.rem(lax.div(c, 2), 2)
    return out


def layer_kernel(
    n_sp, n_tp, group, behind,
    hid_ref, gain_ref, freq_ref, wq_ref, wk_ref, wv_ref, wo_ref, post_ref,
    out_ref, lw_ref,
    raw, nrm, wq, wk, wv, wo, cos_t, sin_t, scr,
    qn_all, kw_all, vw_all, qr_all, kx_all, vx_all,
    acc1, m1, l1, acc4, m4, l4, wide, b1, b4, b16,
    att, att_in, lw, lw_in, total, mix, keep, snd, rcv, final,
    local, near_s, near_r, line_s, line_r, dir_s, dir_r, across_s, across_r, twin_s, twin_r,
    early_s, early_r, late_s, late_r, back_s, back_r, level_s, level_r, swap_s, swap_r,
):
    f32, bf16 = jnp.float32, jnp.bfloat16
    s = lax.axis_index("sp")
    t = lax.axis_index("tp")
    rows, depth = hid_ref.shape
    all_rows = rows * group
    w_rows = wk_ref.shape[0]
    part = wq.shape[1]
    pairs = part // LANES
    steps = all_rows // WIDE
    few = rows // WIDE
    quarter = rows // 4
    count = n_sp // group
    c = lax.rem(s, group)
    base = s - c
    g = lax.div(s, group)
    half = lax.rem(t, 2)
    sibling = (s, t + 1 - 2 * half)
    masks = list(range(1, group))
    peer = {k: base + flip(c, k) for k in masks}
    up = lax.rem(s + group, n_sp)
    down = lax.rem(s + n_sp - group, n_sp)
    after = [lax.rem(s + b * group, n_sp) for b in range(1, behind + 1)]
    before = [lax.rem(s + n_sp - b * group, n_sp) for b in range(1, behind + 1)]
    start_row = pl.multiple_of(c * rows, rows)

    kept = [pltpu.make_async_copy(hid_ref, raw, local.at[0])]
    own_cols = pl.ds(pl.multiple_of(c * part, LANES), part)
    own_rows = pl.ds(pl.multiple_of(s * w_rows, w_rows), w_rows)
    kept.append(pltpu.make_async_copy(wq_ref.at[:, own_cols], wq, local.at[1]))
    for j, (src, dst) in enumerate(((wk_ref, wk), (wv_ref, wv))):
        kept.append(pltpu.make_async_copy(src.at[:, own_cols], dst.at[own_rows], local.at[2 + j]))
    for p in range(pairs):
        for i in range(group):
            kept.append(pltpu.make_async_copy(
                wo_ref.at[pl.ds(i * part + p * LANES, LANES)], wo.at[p, pl.ds(i * LANES, LANES)],
                local.at[4 + p * group + i],
            ))
    for copy in kept:
        copy.start()

    known = [(peer[k], t) for k in masks] + [(x, t) for x in after + before]
    known += [(s, lax.rem(t + k, n_tp)) for k in range(1, n_tp)]
    barrier = pltpu.get_barrier_semaphore()
    for other in known:
        pl.semaphore_signal(barrier, inc=1, device_id=other, device_id_type=MESH)

    half_dim = HEAD_DIM // 2
    lo = lax.broadcasted_iota(jnp.int32, (LANES, LANES), 0).astype(f32) * freq_ref[...]
    cos_lo, sin_lo = jnp.cos(lo), jnp.sin(lo)
    lane = lax.rem(lax.broadcasted_iota(jnp.int32, (1, LANES), 1), HEAD_DIM)
    sign = jnp.where(lane < half_dim, -1.0, 1.0)

    def fill(i, _):
        hi = (base * rows + i * LANES).astype(f32) * freq_ref[...]
        cos_hi, sin_hi = jnp.cos(hi), jnp.sin(hi)
        at = pl.ds(pl.multiple_of(i * LANES, LANES), LANES)
        cos_t[at, :] = cos_lo * cos_hi - sin_lo * sin_hi
        sin_t[at, :] = (sin_lo * cos_hi + cos_lo * sin_hi) * sign
        return 0

    lax.fori_loop(0, all_rows // LANES, fill, 0)

    @pl.when(g < behind)
    def _():
        for pair in range(pairs):
            for ref in (kw_all, vw_all):
                @pl.when(g < 1)
                def _(ref=ref, pair=pair):
                    ref[pair, pl.ds(0, SPAN), :] = jnp.zeros((SPAN, LANES), bf16)
            for ref in (kx_all, vx_all):
                for b in range(1, behind + 1):
                    @pl.when(g < b)
                    def _(ref=ref, pair=pair, b=b):
                        ref[pair, :, pl.ds((behind - b) * steps, steps), :] = jnp.zeros((WIDE, steps, LANES), bf16)

    pl.semaphore_wait(barrier, len(known))

    def near(k, j):
        src, dst = ((wk_ref, wk), (wv_ref, wv))[j]
        cols = pl.ds(pl.multiple_of(flip(c, k) * part, LANES), part)
        return remote(src.at[:, cols], dst.at[own_rows], near_s.at[j, k - 1], near_r.at[j, k - 1], (peer[k], t))

    def line(way, j, d):
        ref = (wk, wv)[j]
        to, off = ((up, g - d), (down, g + d))[way]
        off = jnp.clip(off, 0, count - 1)
        slot = ref.at[pl.ds(pl.multiple_of(off * group * w_rows, group * w_rows), group * w_rows)]
        return remote(slot, slot, line_s.at[way, j, d], line_r.at[way, j, d + 1], (to, t))

    def line_in(way, j, d):
        ref = (wk, wv)[j]
        off = jnp.clip((g - d, g + d)[way], 0, count - 1)
        slot = ref.at[pl.ds(pl.multiple_of(off * group * w_rows, group * w_rows), group * w_rows)]
        return remote(slot, slot, line_s.at[way, j, d - 1], line_r.at[way, j, d], ((up, down)[way], t))

    def has_in(way, d):
        return g >= d if way == 0 else g + d < count

    def has_out(way, d):
        if way == 0:
            return (g >= d) & (g + 1 < count)
        return (g + d < count) & (g >= 1)

    def pass_on(j, d):
        for way in range(2):
            if not (isinstance(d, int) and d == 0):
                @pl.when(has_in(way, d))
                def _(way=way):
                    line_in(way, j, d).wait_recv()

            if not (isinstance(d, int) and d == count - 1):
                @pl.when(has_out(way, d))
                def _(way=way):
                    line(way, j, d).start()

    def passed(j, d):
        for way in range(2):
            @pl.when(has_out(way, d))
            def _(way=way):
                line(way, j, d).wait_send()

    def piece(block, side, q):
        return nrm.at[pl.ds(pl.multiple_of(block * rows + side * (2 * quarter) + q * quarter, quarter), quarter)]

    def direct(k, q):
        slot = piece(c, half, q)
        return remote(slot, slot, dir_s.at[k - 1, q], dir_r.at[k - 1, q], (peer[k], t))

    def across(i):
        k, other = ((1, 2), (2, 1))[i]
        slot = piece(flip(c, k), half, i)
        return remote(slot, slot, across_s.at[i], across_r.at[i], (peer[other], t))

    def twin(k, q):
        slot = piece(flip(c, k), half, q)
        return remote(slot, slot, twin_s.at[k - 1, q], twin_r.at[k - 1, q], sibling)

    for j in range(2):
        for k in masks:
            near(k, j).start()
    firsts = {4: [(1, 0), (2, 1)], 2: [(1, 0)], 1: []}[group]
    seconds = {4: [(1, 1), (2, 0)], 2: [(1, 1)], 1: []}[group]
    thirds = {4: [(3, 0), (3, 1)], 2: [], 1: []}[group]
    def block_of(k):
        return flip(c, k) * rows

    kept[0].wait()

    def norm(i, _):
        x = raw[pl.ds(pl.multiple_of(i * quarter, quarter), quarter), :].astype(f32)
        scale = lax.rsqrt(jnp.mean(x * x, axis=-1, keepdims=True) + EPS)
        at = pl.ds(pl.multiple_of(start_row + i * quarter, quarter), quarter)
        nrm[at, :] = (x * scale * gain_ref[...]).astype(bf16)
        return 0

    lax.fori_loop(0, 4, norm, 0)

    def put_bias(ref, near_by, first_of):
        shape = ref.shape[1:]
        a = lax.broadcasted_iota(jnp.int32, shape, 0)
        b = lax.broadcasted_iota(jnp.int32, shape, 1)
        distance, place = near_by(a, b)
        band = (distance >= 0) & (distance <= SPAN)
        ref[0] = jnp.where(band & (place + first_of >= 0), 0.0, NEG).astype(f32)
        ref[1] = jnp.where(band, 0.0, NEG).astype(f32)

    def plain(a, b):
        return a + SPAN - b, b - SPAN

    def woven(a, b):
        return 4 * (a % 32 + 32 - b % 64) + a // 32 - b // 64, b % 64 - 32

    put_bias(b1, plain, g * all_rows)
    a16 = lax.broadcasted_iota(jnp.int32, b16.shape, 0)
    k16 = lax.broadcasted_iota(jnp.int32, b16.shape, 1)
    seen = (a16 + SPAN >= k16) & (a16 <= k16) & (g * steps + k16 >= SPAN)
    b16[...] = jnp.where(seen, 0.0, NEG).astype(f32)
    put_bias(b4, woven, g * steps)

    for k, q in firsts + seconds:
        direct(k, q).start()

    front = lax.rem(lax.broadcasted_iota(jnp.int32, (rows, LANES), 1), HEAD_DIM) < HEAD_DIM // 2

    def project(k, j):
        row = pl.multiple_of(block_of(k), rows)
        here = pl.ds(row, rows)
        out = jnp.dot(nrm[here, :], (wq, wk, wv)[j][...], preferred_element_type=f32)
        nat = (qn_all, kw_all, vw_all)[j]
        res = (qr_all, kx_all, vx_all)[j]
        skip = 0 if j == 0 else SPAN
        skip_res = 0 if j == 0 else behind * steps
        step = pl.multiple_of(lax.div(row, WIDE), few)
        for i in range(pairs):
            u = out[:, i * LANES:(i + 1) * LANES]
            if j < 2:
                swapped = jnp.where(
                    front,
                    pltpu.roll(u, LANES - HEAD_DIM // 2, 1),
                    pltpu.roll(u, HEAD_DIM // 2, 1),
                )
                u = u * cos_t[here, :] + swapped * sin_t[here, :]
            if j == 0:
                u = u * HEAD_DIM ** (-0.5)
            nat[i, pl.ds(row + skip, rows), :] = u.astype(bf16)
            scr[i] = u
        for i in range(pairs):
            for r in range(WIDE):
                res[i, 4 * (r % 4) + r // 4, pl.ds(step + skip_res, few), :] = scr[i, pl.ds(r, few, stride=WIDE), :].astype(bf16)

    for j in range(2):
        for k in masks:
            near(k, j).wait_recv()
        kept[2 + j].wait()
        pass_on(j, 0)

    kept[1].wait()
    project(0, 0)

    for k, q in firsts:
        direct(k, q).wait_recv()
        if group == 4:
            across(k - 1).start()
        twin(k, q).start()
    if count > 1:
        for j in range(2):
            pass_on(j, 1)
    for k, q in seconds:
        direct(k, q).wait_recv()
        twin(k, q).start()
    if count > 2:
        for j in range(2):
            pass_on(j, 2)
    for k in masks[:2]:
        for q in range(2):
            twin(k, q).wait_recv()
        project(k, 0)

    def far(j):
        if count > 3:
            pass_on(j, 3)
        if count > 4:
            lax.fori_loop(4, count, lambda d, _: (pass_on(j, d), 0)[1], 0)

    def early(pair, j):
        ref = (kw_all, vw_all)[j]
        return remote(
            ref.at[pair, pl.ds(all_rows, SPAN)], ref.at[pair, pl.ds(0, SPAN)],
            early_s.at[pair, j], early_r.at[pair, j], (after[0], t),
        )

    def late(pair, j, k, b):
        ref = (kx_all, vx_all)[j]
        at = pl.multiple_of(flip(c, k) * few, few)
        return remote(
            ref.at[pair, :, pl.ds(behind * steps + at, few)],
            ref.at[pair, :, pl.ds((behind - b) * steps + at, few)],
            late_s.at[pair, j, b - 1, k], late_r.at[pair, j, b - 1, k], (after[b - 1], t),
        )

    everything = [0] + masks

    def send_late(pair, j, k):
        for b in range(1, behind + 1):
            @pl.when(g + b < count)
            def _(b=b):
                late(pair, j, k, b).start()

    def send_early(pair, j):
        @pl.when(g + 1 < count)
        def _():
            early(pair, j).start()

    for j in range(2):
        far(j)
        for i, k in enumerate(everything[:3]):
            project(k, 1 + j)
            if i > 0:
                send_late(0, j, k - 1)
            elif j == 1:
                send_late(0, 0, everything[:3][-1])
    if group == 4:
        for k, q in thirds:
            across(q).wait_recv()
            twin(k, q).start()
        send_late(0, 1, 2)
        for q in range(2):
            twin(3, q).wait_recv()
        project(3, 1)
        project(3, 2)
        send_late(0, 0, 3)
        project(3, 0)
        send_late(0, 1, 3)
    else:
        send_late(0, 1, everything[-1])
    for j in range(2):
        send_early(0, j)

    def part_of(pair, j, u, b):
        ref = (kx_all, vx_all)[j]
        return remote(
            ref.at[pair, pl.ds(4 * u, 4), pl.ds(behind * steps, steps)],
            ref.at[pair, pl.ds(4 * u, 4), pl.ds((behind - b) * steps, steps)],
            late_s.at[pair, j, b - 1, u], late_r.at[pair, j, b - 1, u], (after[b - 1], t),
        )

    for pair in range(1, pairs):
        for j in range(2):
            send_early(pair, j)
        for u in range(4):
            for j in range(2):
                for b in range(1, behind + 1):
                    @pl.when(g + b < count)
                    def _(pair=pair, j=j, u=u, b=b):
                        part_of(pair, j, u, b).start()

    skip16 = behind * steps - SPAN

    def tile(q, k, v, bias):
        n = q.shape[0]
        low = lax.broadcasted_iota(jnp.int32, (n, LANES), 1) < HEAD_DIM
        low_q = low.astype(f32).astype(bf16)
        both = jnp.concatenate([q * low_q, q * (1 - low_q)], axis=0)
        sc = lax.dot_general(both, k, (((1,), (1,)), ((), ())), preferred_element_type=f32)
        sc = sc + jnp.concatenate([bias, bias], axis=0)
        m = jnp.max(sc, axis=-1, keepdims=True)
        e = jnp.exp(sc - m).astype(bf16)
        o = jnp.dot(e, jnp.concatenate([v, jnp.ones_like(v)], axis=1), preferred_element_type=f32)
        wide_m = jnp.broadcast_to(m, (2 * n, LANES))
        return (
            jnp.where(low, o[:n, :LANES], o[n:, :LANES]),
            jnp.where(low, wide_m[:n], wide_m[n:]),
            jnp.where(low, o[:n, LANES:], o[n:, LANES:]),
        )

    blocks4 = steps // 32

    mine = pl.ds(pl.multiple_of(c * LANES, LANES), LANES)
    own_steps = pl.ds(pl.multiple_of(c * few, few), few)

    def back(p, k, u):
        slots = pl.ds(4 * u, 4)
        span = pl.ds(pl.multiple_of(flip(c, k) * few, few), few)
        return remote(
            att.at[p, slots, span], att_in.at[p, slots, :, mine],
            back_s.at[p, k - 1, u], back_r.at[p, k - 1, u], (peer[k], t),
        )

    def level(p, k):
        span = pl.ds(pl.multiple_of(flip(c, k) * rows, rows), rows)
        return remote(lw.at[p, :, span], lw_in.at[c, p], level_s.at[p, k - 1], level_r.at[p, k - 1], (peer[k], t))

    def send_back(p, u):
        for k in masks[::-1]:
            back(p, k, u).start()
        slots = pl.ds(4 * u, 4)
        att_in[p, slots, :, mine] = att[p, slots, own_steps, :]

    def levels(p):
        def turn(i, _):
            here = pl.ds(pl.multiple_of(i * SPAN, SPAN), SPAN)
            turned = jnp.transpose(wide[here, :])
            lw[p, 0:1, here] = turned[0:1]
            lw[p, 1:2, here] = turned[HEAD_DIM:HEAD_DIM + 1]
            return 0

        lax.fori_loop(0, all_rows // SPAN, turn, 0, unroll=4)

    def send_levels(p):
        for k in masks:
            level(p, k).start()
        lw_in[c, p] = lw[p, :, pl.ds(start_row, rows)]

    def fetched(p):
        for copy in kept[4 + p * group:4 + (p + 1) * group]:
            copy.wait()

    def mix_out(p):
        fetched(p)
        for k in masks:
            for u in range(4):
                back(p, k, u).wait_recv()
        for u in range(4):
            rows_in = att_in[p, pl.ds(4 * u, 4)].reshape(4 * few, group * LANES)
            value = jnp.dot(rows_in, wo[p], preferred_element_type=f32)
            total[u] = value if p == 0 else total[u] + value

    last = pairs - 1
    thin = few // n_tp

    def swap(k, u):
        return remote(
            snd.at[k - 1, u], rcv.at[k - 1, u], swap_s.at[k - 1, u], swap_r.at[k - 1, u],
            (s, lax.rem(t + k, n_tp)),
        )

    def share_of(owner):
        if thin % 8 == 0:
            return mix[:, pl.ds(pl.multiple_of(owner * thin, thin), thin), :].astype(bf16)
        value = mix[:, 0:thin, :]
        for o in range(1, n_tp):
            value = jnp.where(owner == o, mix[:, o * thin:(o + 1) * thin, :], value)
        return value.astype(bf16)

    def close(u):
        for k in masks:
            back(last, k, u).wait_recv()
        rows_in = att_in[last, pl.ds(4 * u, 4)].reshape(4 * few, group * LANES)
        value = jnp.dot(rows_in, wo[last], preferred_element_type=f32)
        if last > 0:
            value = value + total[u]
        mix[...] = value.reshape(4, few, value.shape[1])
        for k in range(1, n_tp):
            snd[k - 1, u] = share_of(lax.rem(t + k, n_tp))
        keep[u] = share_of(t)
        for k in range(1, n_tp):
            swap(k, u).start()

    def settle(u):
        value = keep[u].astype(f32)
        for k in range(1, n_tp):
            swap(k, u).wait_recv()
            value = value + rcv[k - 1, u].astype(f32)
        scale = lax.rsqrt(jnp.mean(value * value, axis=-1, keepdims=True) + EPS)
        value = value * scale * post_ref[...]
        for j in range(4):
            for i in range(depth // LANES):
                final[i, pl.ds(u + 4 * j, thin, stride=WIDE), :] = value[j, :, i * LANES:(i + 1) * LANES]

    for p in range(pairs):
        qn, kw, vw, qr, kx, vx = (ref.at[p] for ref in (qn_all, kw_all, vw_all, qr_all, kx_all, vx_all))

        def step16(slot, _):
            r = 4 * (slot % 4) + slot // 4
            keys = pl.ds(skip16, steps + SPAN)
            o16, m16, l16 = tile(qr[slot], kx[slot, keys, :], vx[slot, keys, :], b16[...])
            apart = pl.ds(r, steps, stride=WIDE)
            here = pl.ds(pl.multiple_of(slot * steps, steps), steps)
            m_1, m_4 = m1[apart, :], m4[here, :]
            top = jnp.maximum(m16, jnp.maximum(m_1, m_4))
            e1, e4, e16 = jnp.exp(m_1 - top), jnp.exp(m_4 - top), jnp.exp(m16 - top)
            whole = l1[apart, :] * e1 + l4[here, :] * e4 + l16 * e16
            mixed = acc1[apart, :] * e1 + acc4[here, :] * e4 + o16 * e16
            att[p, slot] = (mixed / whole).astype(bf16)
            wide[apart, :] = top + jnp.log(whole)
            return 0

        def step4(r, i):
            at = i * 32
            low = at + behind * steps - 32
            if not isinstance(i, int):
                at = pl.multiple_of(at, 32)
                low = pl.multiple_of(low, 32)
            keys = pl.ds(low, 64)
            got = tile(
                jnp.concatenate([qr[4 * r + j, pl.ds(at, 32), :] for j in range(4)], axis=0),
                jnp.concatenate([kx[4 * r + j, keys, :] for j in range(4)], axis=0),
                jnp.concatenate([vx[4 * r + j, keys, :] for j in range(4)], axis=0),
                b4[0 if isinstance(i, int) else 1],
            )
            for ref, value in zip((acc4, m4, l4), got):
                for j in range(4):
                    ref[pl.ds(pl.multiple_of((4 * r + j) * steps + at, 32), 32), :] = value[j * 32:(j + 1) * 32]
            return 0

        def step1(i, _):
            at = pl.multiple_of(i * SPAN, SPAN)
            here = pl.ds(at, SPAN)
            keys = pl.ds(at, 2 * SPAN)
            got = tile(qn[here, :], kw[keys, :], vw[keys, :], b1[jnp.minimum(i, 1)])
            for ref, value in zip((acc1, m1, l1), got):
                ref[here, :] = value
            return 0

        if blocks4 > 1:
            lax.fori_loop(
                0, 4 * (blocks4 - 1),
                lambda idx, _: step4(idx // (blocks4 - 1), idx % (blocks4 - 1) + 1), 0, unroll=4,
            )
        plains = all_rows // SPAN - 1
        lax.fori_loop(1, plains + 1, step1, 0, unroll=max(x for x in range(1, 6) if plains % x == 0))
        for j in range(2):
            @pl.when(g >= 1)
            def _(j=j):
                early(p, j).wait_recv()
        step1(0, 0)
        if p > 0:
            mix_out(p - 1)
        if p == last:
            fetched(last)
        if p == 0:
            for j in range(2):
                for b in range(1, behind + 1):
                    @pl.when(g >= b)
                    def _(j=j, b=b):
                        for k in everything:
                            late(0, j, k, b).wait_recv()
        for u in range(4):
            if p > 0:
                for j in range(2):
                    for b in range(1, behind + 1):
                        @pl.when(g >= b)
                        def _(j=j, b=b, u=u):
                            part_of(p, j, u, b).wait_recv()
            step4(u, 0)
            lax.fori_loop(0, 4, lambda n, _, u=u: step16(4 * u + n, 0), 0, unroll=4)
            send_back(p, u)
            if p == last and u >= 1:
                close(u - 1)
            if p == last and u >= 2:
                settle(u - 2)
        levels(p)
        send_levels(p)

    close(3)
    settle(2)
    heads = 2 * pairs
    for p in range(pairs):
        for k in masks:
            level(p, k).wait_recv()
    for i in range(group):
        for p in range(pairs):
            for h in range(2):
                row = i * heads + p * 2 + h
                lw_ref[row:row + 1, :] = lw_in[i, p, h:h + 1, :]
    settle(3)
    for i in range(depth // LANES):
        out_ref[:, i * LANES:(i + 1) * LANES] = final[i].astype(bf16)

    for k in range(1, n_tp):
        for u in range(4):
            swap(k, u).wait_send()
    for p in range(pairs):
        for k in masks:
            level(p, k).wait_send()
            for u in range(4):
                back(p, k, u).wait_send()
    for j in range(2):
        for k in masks:
            near(k, j).wait_send()
        for d in range(min(count - 1, 4)):
            passed(j, d)
        if count > 5:
            lax.fori_loop(4, count - 1, lambda d, _, j=j: (passed(j, d), 0)[1], 0)
    for k, q in firsts + seconds:
        direct(k, q).wait_send()
        twin(k, q).wait_send()
    if group == 4:
        for i in range(2):
            across(i).wait_send()
            twin(3, i).wait_send()
    for pair in range(pairs):
        for j in range(2):
            @pl.when(g + 1 < count)
            def _(pair=pair, j=j):
                early(pair, j).wait_send()

            for b in range(1, behind + 1):
                @pl.when(g + b < count)
                def _(pair=pair, j=j, b=b):
                    if pair == 0:
                        for k in everything:
                            late(pair, j, k, b).wait_send()
                    else:
                        for u in range(4):
                            part_of(pair, j, u, b).wait_send()


def layer(mesh, group, behind, hidden, gain, freq, wq, wk, wv, wo, post):
    n_sp = mesh.shape["sp"]
    n_tp = mesh.shape["tp"]
    rows, depth = hidden.shape
    w_rows, width = wk.shape
    part = width // group
    pairs = part // LANES
    all_rows = rows * group
    steps = all_rows // WIDE
    few = rows // WIDE
    thin = few // n_tp
    count = n_sp // group
    share = rows // n_tp
    f32, bf16 = jnp.float32, jnp.bfloat16
    dma = pltpu.SemaphoreType.DMA
    state = pltpu.VMEM((all_rows, LANES), f32)
    weight = pltpu.VMEM((depth, part), bf16)
    table = pltpu.VMEM((all_rows, LANES), f32)
    ring = pltpu.VMEM((pairs, SPAN + all_rows, LANES), bf16)
    woven = pltpu.VMEM((pairs, WIDE, (behind + 1) * steps, LANES), bf16)
    pieces = pltpu.VMEM((n_tp - 1, 4, 4, thin, depth), bf16)
    vmem = pl.BlockSpec(memory_space=pltpu.VMEM)
    near = max(group - 1, 1)
    return pl.pallas_call(
        functools.partial(layer_kernel, n_sp, n_tp, group, behind),
        out_shape=(
            jax.ShapeDtypeStruct((share, depth), bf16),
            jax.ShapeDtypeStruct((width // HEAD_DIM, rows), f32),
        ),
        in_specs=[ANY, vmem, vmem, ANY, ANY, ANY, ANY, vmem],
        out_specs=(vmem, vmem),
        scratch_shapes=[
            pltpu.VMEM((rows, depth), bf16), pltpu.VMEM((all_rows, depth), bf16),
            weight, weight, weight, pltpu.VMEM((pairs, group * LANES, depth), bf16), table, table,
            pltpu.VMEM((pairs, rows, LANES), f32),
            pltpu.VMEM((pairs, all_rows, LANES), bf16), ring, ring,
            pltpu.VMEM((pairs, WIDE, steps, LANES), bf16), woven, woven,
            state, state, state, state, state, state, state,
            pltpu.VMEM((2, SPAN, 2 * SPAN), f32),
            pltpu.VMEM((2, SPAN, 2 * SPAN), f32),
            pltpu.VMEM((steps, steps + SPAN), f32),
            pltpu.VMEM((pairs, WIDE, steps, LANES), bf16), pltpu.VMEM((pairs, WIDE, few, group * LANES), bf16),
            pltpu.VMEM((pairs, 2, all_rows), f32), pltpu.VMEM((group, pairs, 2, rows), f32),
            pltpu.VMEM((4, 4 * few, depth), f32), pltpu.VMEM((4, few, depth), f32),
            pltpu.VMEM((4, 4, thin, depth), bf16), pieces, pieces,
            pltpu.VMEM((depth // LANES, share, LANES), f32),
            dma((4 + pairs * group,)),
            dma((2, near)), dma((2, near)), dma((2, 2, count)), dma((2, 2, count)),
            dma((2, 2)), dma((2, 2)), dma((2,)), dma((2,)), dma((3, 2)), dma((3, 2)),
            dma((pairs, 2)), dma((pairs, 2)),
            dma((pairs, 2, behind, 4)), dma((pairs, 2, behind, 4)),
            dma((pairs, near, 4)), dma((pairs, near, 4)), dma((pairs, near)), dma((pairs, near)),
            dma((n_tp - 1, 4)), dma((n_tp - 1, 4)),
        ],
        compiler_params=pltpu.CompilerParams(
            vmem_limit_bytes=63 * 1024 * 1024, collective_id=0, has_side_effects=True
        ),
        name="layer_core",
    )(hidden, gain, freq, wq, wk, wv, wo, post)


def body(mesh, hidden_in, pre_gain, query_proj, key_proj, value_proj, out_proj, post_gain):
    rows, depth = hidden_in.shape
    width = query_proj.shape[1]
    group = group_of(mesh, width)
    all_rows = rows * group
    behind = -(-(WIDE * SPAN) // all_rows)
    half_dim = HEAD_DIM // 2
    frequency = ROPE_BASE ** (-(jnp.arange(half_dim, dtype=jnp.float32) * 2.0 / HEAD_DIM))
    freq = jnp.concatenate([frequency] * (LANES // half_dim))[None, :]
    return layer(
        mesh, group, behind, hidden_in, pre_gain[None, :], freq,
        query_proj, key_proj, value_proj, out_proj, post_gain[None, :],
    )


def solution(mesh):
    placed = (P("sp", None), P(), P(None, "tp"), P("sp", "tp"), P("sp", "tp"), P("tp", None), P())
    return jax.shard_map(
        functools.partial(body, mesh),
        mesh=mesh,
        in_specs=placed,
        out_specs=(P(("sp", "tp"), None), P("tp", "sp")),
        check_vma=False,
    )
```

```python
import functools

import jax
import jax.numpy as jnp
from jax import lax
from jax.experimental import pallas as pl
from jax.experimental.pallas import tpu as pltpu
from jax.sharding import PartitionSpec as P

HEAD_DIM = 64
SPAN = 128
EPS = 1e-06
ROPE_BASE = 10000.0
WIDE = 16
LANES = 128
MESH = pl.DeviceIdType.MESH
ANY = pl.BlockSpec(memory_space=pl.ANY)
NEG = -1e30


def remote(src, dst, send, recv, peer):
    return pltpu.make_async_remote_copy(
        src_ref=src, dst_ref=dst, send_sem=send, recv_sem=recv, device_id=peer, device_id_type=MESH
    )


def group_of(mesh, width):
    for size in (4, 2):
        if mesh.shape["sp"] % size == 0 and width % (size * LANES) == 0:
            return size
    return 1


def flip(c, mask):
    out = c
    if mask & 1:
        out = out + 1 - 2 * lax.rem(c, 2)
    if mask & 2:
        out = out + 2 - 4 * lax.rem(lax.div(c, 2), 2)
    return out


def layer_kernel(
    n_sp, n_tp, group, behind,
    hid_ref, gain_ref, freq_ref, wq_ref, wk_ref, wv_ref, wo_ref, post_ref,
    out_ref, lw_ref,
    raw, nrm, ext, wq, wk, wv, wo, cos_t, sin_t, cos_e, sin_e, scr,
    qn_all, kw_all, vw_all, qr_all, kx_all, vx_all,
    acc1_all, m1_all, l1_all, acc4_all, m4_all, l4_all, wide, b1, b4, b16,
    att, att_in, lw, lw_in, total, mix, keep, snd, rcv, final,
    local, near_s, near_r, line_s, line_r, dir_s, dir_r, across_s, across_r, twin_s, twin_r,
    rise_s, rise_r, edir_s, edir_r, eacross_s, eacross_r, etwin_s, etwin_r,
    early_s, early_r, late_s, late_r, back_s, back_r, level_s, level_r, swap_s, swap_r,
):
    f32, bf16 = jnp.float32, jnp.bfloat16
    s = lax.axis_index("sp")
    t = lax.axis_index("tp")
    rows, depth = hid_ref.shape
    all_rows = rows * group
    w_rows = wk_ref.shape[0]
    part = wq.shape[1]
    pairs = part // LANES
    steps = all_rows // WIDE
    few = rows // WIDE
    quarter = rows // 4
    count = n_sp // group
    c = lax.rem(s, group)
    base = s - c
    g = lax.div(s, group)
    half = lax.rem(t, 2)
    sibling = (s, t + 1 - 2 * half)
    masks = list(range(1, group))
    peer = {k: base + flip(c, k) for k in masks}
    up = lax.rem(s + group, n_sp)
    down = lax.rem(s + n_sp - group, n_sp)
    after = [lax.rem(s + b * group, n_sp) for b in range(1, behind + 1)]
    before = [lax.rem(s + n_sp - b * group, n_sp) for b in range(1, behind + 1)]
    start_row = pl.multiple_of(c * rows, rows)
    mixed = behind == 1 and group == 4
    end_steps = steps - few if mixed else steps

    kept = [pltpu.make_async_copy(hid_ref, raw, local.at[0])]
    own_cols = pl.ds(pl.multiple_of(c * part, LANES), part)
    own_rows = pl.ds(pl.multiple_of(s * w_rows, w_rows), w_rows)
    kept.append(pltpu.make_async_copy(wq_ref.at[:, own_cols], wq, local.at[1]))
    for j, (src, dst) in enumerate(((wk_ref, wk), (wv_ref, wv))):
        kept.append(pltpu.make_async_copy(src.at[:, own_cols], dst.at[own_rows], local.at[2 + j]))
    for p in range(pairs):
        for i in range(group):
            kept.append(pltpu.make_async_copy(
                wo_ref.at[pl.ds(i * part + p * LANES, LANES)], wo.at[p, pl.ds(i * LANES, LANES)],
                local.at[4 + p * group + i],
            ))
    for copy in kept:
        copy.start()

    known = [(peer[k], t) for k in masks] + [(x, t) for x in after + before]
    known += [(s, lax.rem(t + k, n_tp)) for k in range(1, n_tp)]
    barrier = pltpu.get_barrier_semaphore()
    for other in known:
        pl.semaphore_signal(barrier, inc=1, device_id=other, device_id_type=MESH)

    half_dim = HEAD_DIM // 2
    lo = lax.broadcasted_iota(jnp.int32, (LANES, LANES), 0).astype(f32) * freq_ref[...]
    cos_lo, sin_lo = jnp.cos(lo), jnp.sin(lo)
    lane = lax.rem(lax.broadcasted_iota(jnp.int32, (1, LANES), 1), HEAD_DIM)
    sign = jnp.where(lane < half_dim, -1.0, 1.0)

    def fill(i, _):
        hi = (base * rows + i * LANES).astype(f32) * freq_ref[...]
        cos_hi, sin_hi = jnp.cos(hi), jnp.sin(hi)
        at = pl.ds(pl.multiple_of(i * LANES, LANES), LANES)
        cos_t[at, :] = cos_lo * cos_hi - sin_lo * sin_hi
        sin_t[at, :] = (sin_lo * cos_hi + cos_lo * sin_hi) * sign
        return 0

    lax.fori_loop(0, all_rows // LANES, fill, 0)

    def fill_ext(i, _):
        hi = (base * rows - rows + i * LANES).astype(f32) * freq_ref[...]
        cos_hi, sin_hi = jnp.cos(hi), jnp.sin(hi)
        at = pl.ds(pl.multiple_of(i * LANES, LANES), LANES)
        cos_e[at, :] = cos_lo * cos_hi - sin_lo * sin_hi
        sin_e[at, :] = (sin_lo * cos_hi + cos_lo * sin_hi) * sign
        return 0

    if mixed:
        lax.fori_loop(0, rows // LANES, fill_ext, 0)

    @pl.when(g < behind)
    def _():
        for pair in range(pairs):
            for ref in (kw_all, vw_all):
                @pl.when(g < 1)
                def _(ref=ref, pair=pair):
                    ref[pair, pl.ds(0, SPAN), :] = jnp.zeros((SPAN, LANES), bf16)
            for ref in (kx_all, vx_all):
                for b in range(1, behind + 1):
                    @pl.when(g < b)
                    def _(ref=ref, pair=pair, b=b):
                        ref[pair, :, pl.ds((behind - b) * steps, steps), :] = jnp.zeros((WIDE, steps, LANES), bf16)

    pl.semaphore_wait(barrier, len(known))

    def near(k, j):
        src, dst = ((wk_ref, wk), (wv_ref, wv))[j]
        cols = pl.ds(pl.multiple_of(flip(c, k) * part, LANES), part)
        return remote(src.at[:, cols], dst.at[own_rows], near_s.at[j, k - 1], near_r.at[j, k - 1], (peer[k], t))

    def line(way, j, d):
        ref = (wk, wv)[j]
        to, off = ((up, g - d), (down, g + d))[way]
        off = jnp.clip(off, 0, count - 1)
        slot = ref.at[pl.ds(pl.multiple_of(off * group * w_rows, group * w_rows), group * w_rows)]
        return remote(slot, slot, line_s.at[way, j, d], line_r.at[way, j, d + 1], (to, t))

    def line_in(way, j, d):
        ref = (wk, wv)[j]
        off = jnp.clip((g - d, g + d)[way], 0, count - 1)
        slot = ref.at[pl.ds(pl.multiple_of(off * group * w_rows, group * w_rows), group * w_rows)]
        return remote(slot, slot, line_s.at[way, j, d - 1], line_r.at[way, j, d], ((up, down)[way], t))

    def has_in(way, d):
        return g >= d if way == 0 else g + d < count

    def has_out(way, d):
        if way == 0:
            return (g >= d) & (g + 1 < count)
        return (g + d < count) & (g >= 1)

    def pass_on(j, d):
        for way in range(2):
            if not (isinstance(d, int) and d == 0):
                @pl.when(has_in(way, d))
                def _(way=way):
                    line_in(way, j, d).wait_recv()

            if not (isinstance(d, int) and d == count - 1):
                @pl.when(has_out(way, d))
                def _(way=way):
                    line(way, j, d).start()

    def passed(j, d):
        for way in range(2):
            @pl.when(has_out(way, d))
            def _(way=way):
                line(way, j, d).wait_send()

    def piece(block, side, q):
        return nrm.at[pl.ds(pl.multiple_of(block * rows + side * (2 * quarter) + q * quarter, quarter), quarter)]

    def direct(k, q):
        slot = piece(c, half, q)
        return remote(slot, slot, dir_s.at[k - 1, q], dir_r.at[k - 1, q], (peer[k], t))

    def across(i):
        k, other = ((1, 2), (2, 1))[i]
        slot = piece(flip(c, k), half, i)
        return remote(slot, slot, across_s.at[i], across_r.at[i], (peer[other], t))

    def twin(k, q):
        slot = piece(flip(c, k), half, q)
        return remote(slot, slot, twin_s.at[k - 1, q], twin_r.at[k - 1, q], sibling)

    bit = rows // 16

    def rise():
        at = pl.multiple_of(c * 4 * bit + half * 2 * bit, 2 * bit)
        src = nrm.at[pl.ds(pl.multiple_of(all_rows - rows + at, 2 * bit), 2 * bit)]
        return remote(src, ext.at[pl.ds(at, 2 * bit)], rise_s.at[0], rise_r.at[0], (up, t))

    def crumb(block, side, q, n=1):
        return ext.at[pl.ds(pl.multiple_of(block * 4 * bit + side * 2 * bit + q * bit, bit), n * bit)]

    def ext_direct(k, q):
        slot = crumb(c, half, q)
        return remote(slot, slot, edir_s.at[k - 1, q], edir_r.at[k - 1, q], (peer[k], t))

    def ext_across(i):
        k, other = ((1, 2), (2, 1))[i]
        slot = crumb(flip(c, k), half, i)
        return remote(slot, slot, eacross_s.at[i], eacross_r.at[i], (peer[other], t))

    def ext_twin(k, q):
        slot = crumb(flip(c, k), half, q, 2 if k == 0 else 1)
        return remote(slot, slot, etwin_s.at[k, q], etwin_r.at[k, q], sibling)

    def share_rise():
        rise().wait_recv()
        for k, q in firsts + seconds:
            ext_direct(k, q).start()
        ext_twin(0, 0).start()

    for j in range(2):
        for k in masks:
            near(k, j).start()
    firsts = {4: [(1, 0), (2, 1)], 2: [(1, 0)], 1: []}[group]
    seconds = {4: [(1, 1), (2, 0)], 2: [(1, 1)], 1: []}[group]
    thirds = {4: [(3, 0), (3, 1)], 2: [], 1: []}[group]
    def block_of(k):
        return flip(c, k) * rows

    kept[0].wait()

    def norm(i, _):
        x = raw[pl.ds(pl.multiple_of(i * quarter, quarter), quarter), :].astype(f32)
        scale = lax.rsqrt(jnp.mean(x * x, axis=-1, keepdims=True) + EPS)
        at = pl.ds(pl.multiple_of(start_row + i * quarter, quarter), quarter)
        nrm[at, :] = (x * scale * gain_ref[...]).astype(bf16)
        return 0

    lax.fori_loop(0, 4, norm, 0)

    def put_bias(ref, near_by, first_of):
        shape = ref.shape[1:]
        a = lax.broadcasted_iota(jnp.int32, shape, 0)
        b = lax.broadcasted_iota(jnp.int32, shape, 1)
        distance, place = near_by(a, b)
        band = (distance >= 0) & (distance <= SPAN)
        ref[0] = jnp.where(band & (place + first_of >= 0), 0.0, NEG).astype(f32)
        ref[1] = jnp.where(band, 0.0, NEG).astype(f32)

    def plain(a, b):
        return a + SPAN - b, b - SPAN

    def woven(a, b):
        return 4 * (a % 32 + 32 - b % 64) + a // 32 - b // 64, b % 64 - 32

    put_bias(b1, plain, g * all_rows)
    a16 = lax.broadcasted_iota(jnp.int32, b16.shape, 0)
    k16 = lax.broadcasted_iota(jnp.int32, b16.shape, 1)
    seen = (a16 + SPAN >= k16) & (a16 <= k16) & (g * steps + k16 >= SPAN)
    b16[...] = jnp.where(seen, 0.0, NEG).astype(f32)
    put_bias(b4, woven, g * steps)

    for k, q in firsts + seconds[:1]:
        direct(k, q).start()

    front = lax.rem(lax.broadcasted_iota(jnp.int32, (rows, LANES), 1), HEAD_DIM) < HEAD_DIM // 2

    def project(k, j):
        row = pl.multiple_of(block_of(k), rows)
        here = pl.ds(row, rows)
        out = jnp.dot(nrm[here, :], (wq, wk, wv)[j][...], preferred_element_type=f32)
        nat = (qn_all, kw_all, vw_all)[j]
        res = (qr_all, kx_all, vx_all)[j]
        skip = 0 if j == 0 else SPAN
        skip_res = 0 if j == 0 else behind * steps
        step = pl.multiple_of(lax.div(row, WIDE), few)
        for i in range(pairs):
            u = out[:, i * LANES:(i + 1) * LANES]
            if j < 2:
                swapped = jnp.where(
                    front,
                    pltpu.roll(u, LANES - HEAD_DIM // 2, 1),
                    pltpu.roll(u, HEAD_DIM // 2, 1),
                )
                u = u * cos_t[here, :] + swapped * sin_t[here, :]
            if j == 0:
                u = u * HEAD_DIM ** (-0.5)
            nat[i, pl.ds(row + skip, rows), :] = u.astype(bf16)
            scr[i] = u
        for i in range(pairs):
            for r in range(WIDE):
                res[i, 4 * (r % 4) + r // 4, pl.ds(step + skip_res, few), :] = scr[i, pl.ds(r, few, stride=WIDE), :].astype(bf16)

    def project_ext(j):
        out = jnp.dot(ext[...], (wq, wk, wv)[j][...], preferred_element_type=f32)
        nat = (qn_all, kw_all, vw_all)[j]
        res = (qr_all, kx_all, vx_all)[j]
        for i in range(pairs):
            u = out[:, i * LANES:(i + 1) * LANES]
            if j == 1:
                swapped = jnp.where(
                    front,
                    pltpu.roll(u, LANES - HEAD_DIM // 2, 1),
                    pltpu.roll(u, HEAD_DIM // 2, 1),
                )
                u = u * cos_e[...] + swapped * sin_e[...]
            nat[i, pl.ds(0, SPAN), :] = u[rows - SPAN:].astype(bf16)
            scr[i] = u
        for i in range(pairs):
            for r in range(WIDE):
                slot = 4 * (r % 4) + r // 4
                res[i, slot, pl.ds(end_steps, few), :] = scr[i, pl.ds(r, few, stride=WIDE), :].astype(bf16)

    for j in range(2):
        for k in masks:
            near(k, j).wait_recv()
        kept[2 + j].wait()
        pass_on(j, 0)

    kept[1].wait()
    project(0, 0)

    for k, q in firsts:
        direct(k, q).wait_recv()
        if group == 4:
            across(k - 1).start()
            if k == 1:
                direct(2, 0).start()
        twin(k, q).start()
    if count > 1:
        for j in range(2):
            pass_on(j, 1)
    for k, q in seconds[:1]:
        direct(k, q).wait_recv()
        twin(k, q).start()
    if count > 2:
        for j in range(2):
            pass_on(j, 2)
    for k in masks[:1]:
        for q in range(2):
            twin(k, q).wait_recv()
        project(k, 0)
    if group == 4:
        twin(2, 1).wait_recv()
        if mixed:
            @pl.when((c != 0) & (g + 1 < count))
            def _():
                rise().start()
        across(0).wait_recv()
        twin(3, 0).start()

    def far(j):
        if count > 3:
            pass_on(j, 3)
        if count > 4:
            lax.fori_loop(4, count, lambda d, _: (pass_on(j, d), 0)[1], 0)

    def early(pair, j):
        ref = (kw_all, vw_all)[j]
        return remote(
            ref.at[pair, pl.ds(all_rows, SPAN)], ref.at[pair, pl.ds(0, SPAN)],
            early_s.at[pair, j], early_r.at[pair, j], (after[0], t),
        )

    def late(pair, j, k, b):
        ref = (kx_all, vx_all)[j]
        at = pl.multiple_of(flip(c, k) * few, few)
        return remote(
            ref.at[pair, :, pl.ds(behind * steps + at, few)],
            ref.at[pair, :, pl.ds((behind - b) * steps + at, few)],
            late_s.at[pair, j, b - 1, k], late_r.at[pair, j, b - 1, k], (after[b - 1], t),
        )

    everything = [0] + masks

    def needed(k):
        return flip(c, k) != group - 1 if mixed else flip(c, k) >= 0

    def send_late(pair, j, k):
        for b in range(1, behind + 1):
            @pl.when((g + b < count) & needed(k))
            def _(b=b):
                late(pair, j, k, b).start()

    def send_early(pair, j):
        @pl.when(g + 1 < count)
        def _():
            early(pair, j).start()

    for j in range(2):
        far(j)
        if group == 4 and j == 0:
            twin(3, 0).wait_recv()
            if mixed:
                @pl.when((c == 0) & (g + 1 < count))
                def _():
                    rise().start()
        for i, k in enumerate(everything[:2]):
            project(k, 1 + j)
            if i > 0:
                send_late(0, j, k - 1)
            elif j == 1:
                send_late(0, 0, everything[:2][-1])
    if group == 4:
        direct(2, 0).wait_recv()
        twin(2, 0).start()
        across(1).wait_recv()
        twin(3, 1).start()
        send_late(0, 1, 1)
        twin(2, 0).wait_recv()
        project(2, 1)
        project(2, 2)
        if mixed:
            pl.when(g >= 1)(share_rise)
        send_late(0, 0, 2)
        twin(3, 1).wait_recv()
        project(3, 1)
        send_late(0, 1, 2)
        project(3, 2)
        send_late(0, 0, 3)
        project(2, 0)
        project(3, 0)
        send_late(0, 1, 3)
    else:
        send_late(0, 1, everything[-1])
    if not mixed:
        for j in range(2):
            send_early(0, j)

    def part_of(pair, j, u, b):
        ref = (kx_all, vx_all)[j]
        return remote(
            ref.at[pair, pl.ds(4 * u, 4), pl.ds(behind * steps, end_steps)],
            ref.at[pair, pl.ds(4 * u, 4), pl.ds((behind - b) * steps, end_steps)],
            late_s.at[pair, j, b - 1, u], late_r.at[pair, j, b - 1, u], (after[b - 1], t),
        )

    for pair in range(1, pairs):
        if not mixed:
            for j in range(2):
                send_early(pair, j)
        for u in range(4):
            for j in range(2):
                for b in range(1, behind + 1):
                    @pl.when(g + b < count)
                    def _(pair=pair, j=j, u=u, b=b):
                        part_of(pair, j, u, b).start()

    skip16 = behind * steps - SPAN

    def tile(q, k, v, bias):
        n = q.shape[0]
        low = lax.broadcasted_iota(jnp.int32, (n, LANES), 1) < HEAD_DIM
        low_q = low.astype(f32).astype(bf16)
        both = jnp.concatenate([q * low_q, q * (1 - low_q)], axis=0)
        sc = lax.dot_general(both, k, (((1,), (1,)), ((), ())), preferred_element_type=f32)
        sc = sc + jnp.concatenate([bias, bias], axis=0)
        m = jnp.max(sc, axis=-1, keepdims=True)
        e = jnp.exp(sc - m).astype(bf16)
        o = jnp.dot(e, jnp.concatenate([v, jnp.ones_like(v)], axis=1), preferred_element_type=f32)
        wide_m = jnp.broadcast_to(m, (2 * n, LANES))
        return (
            jnp.where(low, o[:n, :LANES], o[n:, :LANES]),
            jnp.where(low, wide_m[:n], wide_m[n:]),
            jnp.where(low, o[:n, LANES:], o[n:, LANES:]),
        )

    blocks4 = steps // 32

    mine = pl.ds(pl.multiple_of(c * LANES, LANES), LANES)
    own_steps = pl.ds(pl.multiple_of(c * few, few), few)

    def back(p, k, u):
        slots = pl.ds(4 * u, 4)
        span = pl.ds(pl.multiple_of(flip(c, k) * few, few), few)
        return remote(
            att.at[p, slots, span], att_in.at[p, slots, :, mine],
            back_s.at[p, k - 1, u], back_r.at[p, k - 1, u], (peer[k], t),
        )

    def level(p, k):
        span = pl.ds(pl.multiple_of(flip(c, k) * rows, rows), rows)
        return remote(lw.at[p, :, span], lw_in.at[c, p], level_s.at[p, k - 1], level_r.at[p, k - 1], (peer[k], t))

    def send_back(p, u):
        for k in masks[::-1]:
            back(p, k, u).start()
        slots = pl.ds(4 * u, 4)
        att_in[p, slots, :, mine] = att[p, slots, own_steps, :]

    def levels(p):
        def turn(i, _):
            here = pl.ds(pl.multiple_of(i * SPAN, SPAN), SPAN)
            turned = jnp.transpose(wide[here, :])
            lw[p, 0:1, here] = turned[0:1]
            lw[p, 1:2, here] = turned[HEAD_DIM:HEAD_DIM + 1]
            return 0

        lax.fori_loop(0, all_rows // SPAN, turn, 0, unroll=4)

    def send_levels(p):
        for k in masks:
            level(p, k).start()
        lw_in[c, p] = lw[p, :, pl.ds(start_row, rows)]

    def fetched(p):
        for copy in kept[4 + p * group:4 + (p + 1) * group]:
            copy.wait()

    def mix_out(p):
        fetched(p)
        for k in masks:
            for u in range(4):
                back(p, k, u).wait_recv()
        for u in range(4):
            rows_in = att_in[p, pl.ds(4 * u, 4)].reshape(4 * few, group * LANES)
            value = jnp.dot(rows_in, wo[p], preferred_element_type=f32)
            total[u] = value if p == 0 else total[u] + value

    last = pairs - 1
    thin = few // n_tp

    def swap(k, u):
        return remote(
            snd.at[k - 1, u], rcv.at[k - 1, u], swap_s.at[k - 1, u], swap_r.at[k - 1, u],
            (s, lax.rem(t + k, n_tp)),
        )

    def share_of(owner):
        if thin % 8 == 0:
            return mix[:, pl.ds(pl.multiple_of(owner * thin, thin), thin), :].astype(bf16)
        value = mix[:, 0:thin, :]
        for o in range(1, n_tp):
            value = jnp.where(owner == o, mix[:, o * thin:(o + 1) * thin, :], value)
        return value.astype(bf16)

    def close(u):
        for k in masks:
            back(last, k, u).wait_recv()
        rows_in = att_in[last, pl.ds(4 * u, 4)].reshape(4 * few, group * LANES)
        value = jnp.dot(rows_in, wo[last], preferred_element_type=f32)
        if last > 0:
            value = value + total[u]
        mix[...] = value.reshape(4, few, value.shape[1])
        for k in range(1, n_tp):
            snd[k - 1, u] = share_of(lax.rem(t + k, n_tp))
        keep[u] = share_of(t)
        for k in range(1, n_tp):
            swap(k, u).start()

    def settle(u):
        value = keep[u].astype(f32)
        for k in range(1, n_tp):
            swap(k, u).wait_recv()
            value = value + rcv[k - 1, u].astype(f32)
        scale = lax.rsqrt(jnp.mean(value * value, axis=-1, keepdims=True) + EPS)
        value = value * scale * post_ref[...]
        for j in range(4):
            for i in range(depth // LANES):
                final[i, pl.ds(u + 4 * j, thin, stride=WIDE), :] = value[j, :, i * LANES:(i + 1) * LANES]

    def tiles_of(p):
        qn, kw, vw, qr, kx, vx = (ref.at[p] for ref in (qn_all, kw_all, vw_all, qr_all, kx_all, vx_all))
        acc1, m1, l1 = (ref.at[p] for ref in (acc1_all, m1_all, l1_all))
        acc4, m4, l4 = (ref.at[p] for ref in (acc4_all, m4_all, l4_all))

        def step16(slot, _):
            r = 4 * (slot % 4) + slot // 4
            keys = pl.ds(skip16, steps + SPAN)
            o16, m16, l16 = tile(qr[slot], kx[slot, keys, :], vx[slot, keys, :], b16[...])
            apart = pl.ds(r, steps, stride=WIDE)
            here = pl.ds(pl.multiple_of(slot * steps, steps), steps)
            m_1, m_4 = m1[apart, :], m4[here, :]
            top = jnp.maximum(m16, jnp.maximum(m_1, m_4))
            e1, e4, e16 = jnp.exp(m_1 - top), jnp.exp(m_4 - top), jnp.exp(m16 - top)
            whole = l1[apart, :] * e1 + l4[here, :] * e4 + l16 * e16
            mixed = acc1[apart, :] * e1 + acc4[here, :] * e4 + o16 * e16
            att[p, slot] = (mixed / whole).astype(bf16)
            wide[apart, :] = top + jnp.log(whole)
            return 0

        def step4(r, i):
            at = i * 32
            low = at + behind * steps - 32
            if not isinstance(i, int):
                at = pl.multiple_of(at, 32)
                low = pl.multiple_of(low, 32)
            keys = pl.ds(low, 64)
            got = tile(
                jnp.concatenate([qr[4 * r + j, pl.ds(at, 32), :] for j in range(4)], axis=0),
                jnp.concatenate([kx[4 * r + j, keys, :] for j in range(4)], axis=0),
                jnp.concatenate([vx[4 * r + j, keys, :] for j in range(4)], axis=0),
                b4[0 if isinstance(i, int) else 1],
            )
            for ref, value in zip((acc4, m4, l4), got):
                for j in range(4):
                    ref[pl.ds(pl.multiple_of((4 * r + j) * steps + at, 32), 32), :] = value[j * 32:(j + 1) * 32]
            return 0

        def step1(i, _):
            at = pl.multiple_of(i * SPAN, SPAN)
            here = pl.ds(at, SPAN)
            keys = pl.ds(at, 2 * SPAN)
            got = tile(qn[here, :], kw[keys, :], vw[keys, :], b1[jnp.minimum(i, 1)])
            for ref, value in zip((acc1, m1, l1), got):
                ref[here, :] = value
            return 0

        def rest4():
            if blocks4 > 1:
                lax.fori_loop(
                    0, 4 * (blocks4 - 1),
                    lambda idx, _: step4(idx // (blocks4 - 1), idx % (blocks4 - 1) + 1), 0, unroll=4,
                )

        def rest1():
            plains = all_rows // SPAN - 1
            lax.fori_loop(1, plains + 1, step1, 0, unroll=max(x for x in range(1, 6) if plains % x == 0))

        return rest4, rest1, step4, step1, step16

    work = [tiles_of(p) for p in range(pairs)]

    def ext_first():
        for k, q in firsts:
            ext_direct(k, q).wait_recv()
            ext_across(k - 1).start()
            ext_twin(k, q).start()

    def ext_second():
        for k, q in seconds:
            ext_direct(k, q).wait_recv()
            ext_twin(k, q).start()

    def ext_third():
        for k, q in thirds:
            ext_across(q).wait_recv()
            ext_twin(k, q).start()
        ext_twin(0, 0).wait_recv()
        for k in masks:
            for q in range(2):
                ext_twin(k, q).wait_recv()
        for j in (1, 2):
            project_ext(j)

    stages = []
    if mixed:
        stages = [ext_first, ext_second, ext_third]
    for p in range(pairs):
        for part_work in work[p][:2]:
            part_work()
            if stages:
                pl.when(g >= 1)(stages.pop(0))
    for stage in stages:
        pl.when(g >= 1)(stage)
    for p in range(pairs):
        rest4, rest1, step4, step1, step16 = work[p]
        if not mixed:
            for j in range(2):
                @pl.when(g >= 1)
                def _(j=j):
                    early(p, j).wait_recv()
        step1(0, 0)
        if p == last:
            fetched(last)
        if p == 0:
            for j in range(2):
                for b in range(1, behind + 1):
                    for k in everything:
                        @pl.when((g >= b) & needed(k))
                        def _(j=j, b=b, k=k):
                            late(0, j, k, b).wait_recv()
        for u in range(4):
            if p > 0:
                for j in range(2):
                    for b in range(1, behind + 1):
                        @pl.when(g >= b)
                        def _(j=j, b=b, u=u):
                            part_of(p, j, u, b).wait_recv()
            step4(u, 0)
            lax.fori_loop(0, 4, lambda n, _, u=u: step16(4 * u + n, 0), 0, unroll=4)
            send_back(p, u)
            if p > 0 and u == 0:
                mix_out(p - 1)
            if p == last and u >= 1:
                close(u - 1)
            if p == last and u >= 2:
                settle(u - 2)
        levels(p)
        send_levels(p)

    close(3)
    settle(2)
    heads = 2 * pairs
    for p in range(pairs):
        for k in masks:
            level(p, k).wait_recv()
    for i in range(group):
        for p in range(pairs):
            for h in range(2):
                row = i * heads + p * 2 + h
                lw_ref[row:row + 1, :] = lw_in[i, p, h:h + 1, :]
    settle(3)
    for i in range(depth // LANES):
        out_ref[:, i * LANES:(i + 1) * LANES] = final[i].astype(bf16)

    for k in range(1, n_tp):
        for u in range(4):
            swap(k, u).wait_send()
    for p in range(pairs):
        for k in masks:
            level(p, k).wait_send()
            for u in range(4):
                back(p, k, u).wait_send()
    for j in range(2):
        for k in masks:
            near(k, j).wait_send()
        for d in range(min(count - 1, 4)):
            passed(j, d)
        if count > 5:
            lax.fori_loop(4, count - 1, lambda d, _, j=j: (passed(j, d), 0)[1], 0)
    for k, q in firsts + seconds:
        direct(k, q).wait_send()
        twin(k, q).wait_send()
    if group == 4:
        for i in range(2):
            across(i).wait_send()
            twin(3, i).wait_send()
    if mixed:
        @pl.when(g + 1 < count)
        def _():
            rise().wait_send()

        @pl.when(g >= 1)
        def _():
            ext_twin(0, 0).wait_send()
            for k, q in firsts + seconds:
                ext_direct(k, q).wait_send()
                ext_twin(k, q).wait_send()
            for i in range(2):
                ext_across(i).wait_send()
                ext_twin(3, i).wait_send()
    for pair in range(pairs):
        for j in range(2):
            if not mixed:
                @pl.when(g + 1 < count)
                def _(pair=pair, j=j):
                    early(pair, j).wait_send()

            for b in range(1, behind + 1):
                if pair == 0:
                    for k in everything:
                        @pl.when((g + b < count) & needed(k))
                        def _(j=j, b=b, k=k):
                            late(0, j, k, b).wait_send()
                else:
                    @pl.when(g + b < count)
                    def _(pair=pair, j=j, b=b):
                        for u in range(4):
                            part_of(pair, j, u, b).wait_send()


def layer(mesh, group, behind, hidden, gain, freq, wq, wk, wv, wo, post):
    n_sp = mesh.shape["sp"]
    n_tp = mesh.shape["tp"]
    rows, depth = hidden.shape
    w_rows, width = wk.shape
    part = width // group
    pairs = part // LANES
    all_rows = rows * group
    steps = all_rows // WIDE
    few = rows // WIDE
    thin = few // n_tp
    count = n_sp // group
    share = rows // n_tp
    f32, bf16 = jnp.float32, jnp.bfloat16
    dma = pltpu.SemaphoreType.DMA
    mixed = behind == 1 and group == 4
    extra = pltpu.VMEM((rows, depth) if mixed else (16, LANES), bf16)
    small = pltpu.VMEM((rows, LANES) if mixed else (8, LANES), f32)
    state = pltpu.VMEM((pairs, all_rows, LANES), f32)
    weight = pltpu.VMEM((depth, part), bf16)
    table = pltpu.VMEM((all_rows, LANES), f32)
    ring = pltpu.VMEM((pairs, SPAN + all_rows, LANES), bf16)
    woven = pltpu.VMEM((pairs, WIDE, (behind + 1) * steps, LANES), bf16)
    pieces = pltpu.VMEM((n_tp - 1, 4, 4, thin, depth), bf16)
    vmem = pl.BlockSpec(memory_space=pltpu.VMEM)
    near = max(group - 1, 1)
    return pl.pallas_call(
        functools.partial(layer_kernel, n_sp, n_tp, group, behind),
        out_shape=(
            jax.ShapeDtypeStruct((share, depth), bf16),
            jax.ShapeDtypeStruct((width // HEAD_DIM, rows), f32),
        ),
        in_specs=[ANY, vmem, vmem, ANY, ANY, ANY, ANY, vmem],
        out_specs=(vmem, vmem),
        scratch_shapes=[
            pltpu.VMEM((rows, depth), bf16), pltpu.VMEM((all_rows, depth), bf16), extra,
            weight, weight, weight, pltpu.VMEM((pairs, group * LANES, depth), bf16), table, table, small, small,
            pltpu.VMEM((pairs, rows, LANES), f32),
            pltpu.VMEM((pairs, all_rows, LANES), bf16), ring, ring,
            pltpu.VMEM((pairs, WIDE, steps, LANES), bf16), woven, woven,
            state, state, state, state, state, state, table,
            pltpu.VMEM((2, SPAN, 2 * SPAN), f32),
            pltpu.VMEM((2, SPAN, 2 * SPAN), f32),
            pltpu.VMEM((steps, steps + SPAN), f32),
            pltpu.VMEM((pairs, WIDE, steps, LANES), bf16), pltpu.VMEM((pairs, WIDE, few, group * LANES), bf16),
            pltpu.VMEM((pairs, 2, all_rows), f32), pltpu.VMEM((group, pairs, 2, rows), f32),
            pltpu.VMEM((4, 4 * few, depth), f32), pltpu.VMEM((4, few, depth), f32),
            pltpu.VMEM((4, 4, thin, depth), bf16), pieces, pieces,
            pltpu.VMEM((depth // LANES, share, LANES), f32),
            dma((4 + pairs * group,)),
            dma((2, near)), dma((2, near)), dma((2, 2, count)), dma((2, 2, count)),
            dma((2, 2)), dma((2, 2)), dma((2,)), dma((2,)), dma((3, 2)), dma((3, 2)),
            dma((1,)), dma((1,)), dma((2, 2)), dma((2, 2)), dma((2,)), dma((2,)), dma((4, 2)), dma((4, 2)),
            dma((pairs, 2)), dma((pairs, 2)),
            dma((pairs, 2, behind, 4)), dma((pairs, 2, behind, 4)),
            dma((pairs, near, 4)), dma((pairs, near, 4)), dma((pairs, near)), dma((pairs, near)),
            dma((n_tp - 1, 4)), dma((n_tp - 1, 4)),
        ],
        compiler_params=pltpu.CompilerParams(
            vmem_limit_bytes=63 * 1024 * 1024, collective_id=0, has_side_effects=True
        ),
        name="layer_core",
    )(hidden, gain, freq, wq, wk, wv, wo, post)


def body(mesh, hidden_in, pre_gain, query_proj, key_proj, value_proj, out_proj, post_gain):
    rows, depth = hidden_in.shape
    width = query_proj.shape[1]
    group = group_of(mesh, width)
    all_rows = rows * group
    behind = -(-(WIDE * SPAN) // all_rows)
    half_dim = HEAD_DIM // 2
    frequency = ROPE_BASE ** (-(jnp.arange(half_dim, dtype=jnp.float32) * 2.0 / HEAD_DIM))
    freq = jnp.concatenate([frequency] * (LANES // half_dim))[None, :]
    return layer(
        mesh, group, behind, hidden_in, pre_gain[None, :], freq,
        query_proj, key_proj, value_proj, out_proj, post_gain[None, :],
    )


def solution(mesh):
    placed = (P("sp", None), P(), P(None, "tp"), P("sp", "tp"), P("sp", "tp"), P("tp", None), P())
    return jax.shard_map(
        functools.partial(body, mesh),
        mesh=mesh,
        in_specs=placed,
        out_specs=(P(("sp", "tp"), None), P("tp", "sp")),
        check_vma=False,
    )
```

```python
import functools

import jax
import jax.numpy as jnp
import numpy as np
from jax import lax
from jax.experimental import pallas as pl
from jax.experimental.pallas import tpu as pltpu
from jax.sharding import PartitionSpec as P

HEAD_DIM = 64
SPAN = 128
EPS = 1e-06
ROPE_BASE = 10000.0
WIDE = 16
LANES = 128
MESH = pl.DeviceIdType.MESH
ANY = pl.BlockSpec(memory_space=pl.ANY)
NEG = -1e30


def remote(src, dst, send, recv, peer):
    return pltpu.make_async_remote_copy(
        src_ref=src, dst_ref=dst, send_sem=send, recv_sem=recv, device_id=peer, device_id_type=MESH
    )


def group_of(mesh, width):
    for size in (4, 2):
        if mesh.shape["sp"] % size == 0 and width % (size * LANES) == 0:
            return size
    return 1


def flip(c, mask):
    out = c
    if mask & 1:
        out = out + 1 - 2 * lax.rem(c, 2)
    if mask & 2:
        out = out + 2 - 4 * lax.rem(lax.div(c, 2), 2)
    return out


def layer_kernel(
    n_sp, n_tp, group, behind,
    hid_ref, gain_ref, freq_ref, wq_ref, wk_ref, wv_ref, wo_ref, post_ref,
    out_ref, lw_ref,
    raw, nrm, ext, wq, wk, wv, wo, cos_t, sin_t, cos_e, sin_e, scr,
    qn_all, kw_all, vw_all, qr_all, kx_all, vx_all,
    acc1_all, m1_all, l1_all, acc4_all, m4_all, l4_all, wide, b1, b4, b16,
    att, att_in, lw, lw_in, total, mix, keep, snd, rcv, final,
    local, own_s, own_r, near_s, near_r, line_s, line_r, dir_s, dir_r, across_s, across_r, twin_s, twin_r,
    rise_s, rise_r, edir_s, edir_r, eacross_s, eacross_r, etwin_s, etwin_r,
    early_s, early_r, late_s, late_r, back_s, back_r, level_s, level_r, swap_s, swap_r,
):
    f32, bf16 = jnp.float32, jnp.bfloat16
    s = lax.axis_index("sp")
    t = lax.axis_index("tp")
    rows, depth = hid_ref.shape
    all_rows = rows * group
    w_rows = wk_ref.shape[0]
    part = wq.shape[1]
    pairs = part // LANES
    steps = all_rows // WIDE
    few = rows // WIDE
    quarter = rows // 4
    count = n_sp // group
    c = lax.rem(s, group)
    base = s - c
    g = lax.div(s, group)
    half = lax.rem(t, 2)
    sibling = (s, t + 1 - 2 * half)
    masks = list(range(1, group))
    peer = {k: base + flip(c, k) for k in masks}
    up = lax.rem(s + group, n_sp)
    down = lax.rem(s + n_sp - group, n_sp)
    after = [lax.rem(s + b * group, n_sp) for b in range(1, behind + 1)]
    before = [lax.rem(s + n_sp - b * group, n_sp) for b in range(1, behind + 1)]
    start_row = pl.multiple_of(c * rows, rows)
    mixed = behind == 1 and group == 4
    end_steps = steps - few if mixed else steps

    kept = [pltpu.make_async_copy(hid_ref, raw, local.at[0])]
    own_cols = pl.ds(pl.multiple_of(c * part, LANES), part)
    own_rows = pl.ds(pl.multiple_of(s * w_rows, w_rows), w_rows)
    kept.append(pltpu.make_async_copy(wq_ref.at[:, own_cols], wq, local.at[1]))
    for j, (src, dst) in enumerate(((wk_ref, wk), (wv_ref, wv))):
        kept.append(pltpu.make_async_copy(src.at[:, own_cols], dst.at[own_rows], local.at[2 + j]))
    for p in range(pairs):
        for i in range(group):
            kept.append(pltpu.make_async_copy(
                wo_ref.at[pl.ds(i * part + p * LANES, LANES)], wo.at[p, pl.ds(i * LANES, LANES)],
                local.at[4 + p * group + i],
            ))
    for copy in kept:
        copy.start()

    known = [(peer[k], t) for k in masks] + [(x, t) for x in after + before]
    known += [(s, lax.rem(t + k, n_tp)) for k in range(1, n_tp)]
    barrier = pltpu.get_barrier_semaphore()
    for other in known:
        pl.semaphore_signal(barrier, inc=1, device_id=other, device_id_type=MESH)

    half_dim = HEAD_DIM // 2
    lo = lax.broadcasted_iota(jnp.int32, (LANES, LANES), 0).astype(f32) * freq_ref[...]
    cos_lo, sin_lo = jnp.cos(lo), jnp.sin(lo)
    lane = lax.rem(lax.broadcasted_iota(jnp.int32, (1, LANES), 1), HEAD_DIM)
    sign = jnp.where(lane < half_dim, -1.0, 1.0)

    def fill(i, _):
        hi = (base * rows + i * LANES).astype(f32) * freq_ref[...]
        cos_hi, sin_hi = jnp.cos(hi), jnp.sin(hi)
        at = pl.ds(pl.multiple_of(i * LANES, LANES), LANES)
        cos_t[at, :] = cos_lo * cos_hi - sin_lo * sin_hi
        sin_t[at, :] = (sin_lo * cos_hi + cos_lo * sin_hi) * sign
        return 0

    lax.fori_loop(0, all_rows // LANES, fill, 0)

    def fill_ext(i, _):
        hi = (base * rows - rows + i * LANES).astype(f32) * freq_ref[...]
        cos_hi, sin_hi = jnp.cos(hi), jnp.sin(hi)
        at = pl.ds(pl.multiple_of(i * LANES, LANES), LANES)
        cos_e[at, :] = cos_lo * cos_hi - sin_lo * sin_hi
        sin_e[at, :] = (sin_lo * cos_hi + cos_lo * sin_hi) * sign
        return 0

    if mixed:
        lax.fori_loop(0, rows // LANES, fill_ext, 0)

    @pl.when(g < behind)
    def _():
        for pair in range(pairs):
            for ref in (kw_all, vw_all):
                @pl.when(g < 1)
                def _(ref=ref, pair=pair):
                    ref[pair, pl.ds(0, SPAN), :] = jnp.zeros((SPAN, LANES), bf16)
            for ref in (kx_all, vx_all):
                for b in range(1, behind + 1):
                    @pl.when(g < b)
                    def _(ref=ref, pair=pair, b=b):
                        ref[pair, :, pl.ds((behind - b) * steps, steps), :] = jnp.zeros((WIDE, steps, LANES), bf16)

    pl.semaphore_wait(barrier, len(known))

    def near(k, j):
        src, dst = ((wk_ref, wk), (wv_ref, wv))[j]
        cols = pl.ds(pl.multiple_of(flip(c, k) * part, LANES), part)
        return remote(src.at[:, cols], dst.at[own_rows], near_s.at[j, k - 1], near_r.at[j, k - 1], (peer[k], t))

    def line(way, j, d):
        ref = (wk, wv)[j]
        to, off = ((up, g - d), (down, g + d))[way]
        off = jnp.clip(off, 0, count - 1)
        slot = ref.at[pl.ds(pl.multiple_of(off * group * w_rows, group * w_rows), group * w_rows)]
        return remote(slot, slot, line_s.at[way, j, d], line_r.at[way, j, d + 1], (to, t))

    def line_in(way, j, d):
        ref = (wk, wv)[j]
        off = jnp.clip((g - d, g + d)[way], 0, count - 1)
        slot = ref.at[pl.ds(pl.multiple_of(off * group * w_rows, group * w_rows), group * w_rows)]
        return remote(slot, slot, line_s.at[way, j, d - 1], line_r.at[way, j, d], ((up, down)[way], t))

    def line_own(way, j, k):
        at = pl.multiple_of((base + flip(c, k)) * w_rows, w_rows)
        slot = (wk, wv)[j].at[pl.ds(at, w_rows)]
        return remote(slot, slot, own_s.at[way, j, k], own_r.at[way, j, k], ((up, down)[way], t))

    def has_in(way, d):
        return g >= d if way == 0 else g + d < count

    def has_out(way, d):
        if way == 0:
            return (g >= d) & (g + 1 < count)
        return (g + d < count) & (g >= 1)

    def own_on(j, k):
        for way in range(2):
            @pl.when(has_out(way, 0))
            def _(way=way):
                line_own(way, j, k).start()

    def pass_on(j, d):
        for way in range(2):
            @pl.when(has_in(way, d))
            def _(way=way):
                if isinstance(d, int) and d == 1:
                    for k in [0] + masks:
                        line_own(way, j, k).wait_recv()
                else:
                    line_in(way, j, d).wait_recv()

            if not (isinstance(d, int) and d == count - 1):
                @pl.when(has_out(way, d))
                def _(way=way):
                    line(way, j, d).start()

    def passed(j, d):
        for way in range(2):
            @pl.when(has_out(way, d))
            def _(way=way):
                if isinstance(d, int) and d == 0:
                    for k in [0] + masks:
                        line_own(way, j, k).wait_send()
                else:
                    line(way, j, d).wait_send()

    def piece(block, side, q):
        return nrm.at[pl.ds(pl.multiple_of(block * rows + side * (2 * quarter) + q * quarter, quarter), quarter)]

    def direct(k, q):
        slot = piece(c, half, q)
        return remote(slot, slot, dir_s.at[k - 1, q], dir_r.at[k - 1, q], (peer[k], t))

    def across(i):
        k, other = ((1, 2), (2, 1))[i]
        slot = piece(flip(c, k), half, i)
        return remote(slot, slot, across_s.at[i], across_r.at[i], (peer[other], t))

    def twin(k, q):
        slot = piece(flip(c, k), half, q)
        return remote(slot, slot, twin_s.at[k - 1, q], twin_r.at[k - 1, q], sibling)

    bit = rows // 16

    def rise():
        at = pl.multiple_of(c * 4 * bit + half * 2 * bit, 2 * bit)
        src = nrm.at[pl.ds(pl.multiple_of(all_rows - rows + at, 2 * bit), 2 * bit)]
        return remote(src, ext.at[pl.ds(at, 2 * bit)], rise_s.at[0], rise_r.at[0], (up, t))

    def crumb(block, side, q, n=1):
        return ext.at[pl.ds(pl.multiple_of(block * 4 * bit + side * 2 * bit + q * bit, bit), n * bit)]

    def ext_direct(k, q):
        slot = crumb(c, half, q)
        return remote(slot, slot, edir_s.at[k - 1, q], edir_r.at[k - 1, q], (peer[k], t))

    def ext_across(i):
        k, other = ((1, 2), (2, 1))[i]
        slot = crumb(flip(c, k), half, i)
        return remote(slot, slot, eacross_s.at[i], eacross_r.at[i], (peer[other], t))

    def ext_twin(k, q):
        slot = crumb(flip(c, k), half, q, 2 if k == 0 else 1)
        return remote(slot, slot, etwin_s.at[k, q], etwin_r.at[k, q], sibling)

    def share_rise():
        rise().wait_recv()
        for k, q in firsts + seconds:
            ext_direct(k, q).start()
        ext_twin(0, 0).start()

    for j in range(2):
        for k in masks:
            near(k, j).start()
    kept[2].wait()
    own_on(0, 0)
    kept[3].wait()
    own_on(1, 0)
    firsts = {4: [(1, 0), (2, 1)], 2: [(1, 0)], 1: []}[group]
    seconds = {4: [(1, 1), (2, 0)], 2: [(1, 1)], 1: []}[group]
    thirds = {4: [(3, 0), (3, 1)], 2: [], 1: []}[group]
    def block_of(k):
        return flip(c, k) * rows

    kept[0].wait()

    def norm(i, _):
        x = raw[pl.ds(pl.multiple_of(i * quarter, quarter), quarter), :].astype(f32)
        scale = lax.rsqrt(jnp.mean(x * x, axis=-1, keepdims=True) + EPS)
        at = pl.ds(pl.multiple_of(start_row + i * quarter, quarter), quarter)
        nrm[at, :] = (x * scale * gain_ref[...]).astype(bf16)
        return 0

    lax.fori_loop(0, 4, norm, 0)

    def put_bias(ref, near_by, first_of):
        shape = ref.shape[1:]
        a = lax.broadcasted_iota(jnp.int32, shape, 0)
        b = lax.broadcasted_iota(jnp.int32, shape, 1)
        distance, place = near_by(a, b)
        band = (distance >= 0) & (distance <= SPAN)
        ref[0] = jnp.where(band & (place + first_of >= 0), 0.0, NEG).astype(f32)
        ref[1] = jnp.where(band, 0.0, NEG).astype(f32)

    def plain(a, b):
        return a + SPAN - b, b - SPAN

    def woven(a, b):
        return 4 * (a % 32 + 32 - b % 64) + a // 32 - b // 64, b % 64 - 32

    put_bias(b1, plain, g * all_rows)
    a16 = lax.broadcasted_iota(jnp.int32, b16.shape, 0)
    k16 = lax.broadcasted_iota(jnp.int32, b16.shape, 1)
    seen = (a16 + SPAN >= k16) & (a16 <= k16) & (g * steps + k16 >= SPAN)
    b16[...] = jnp.where(seen, 0.0, NEG).astype(f32)
    put_bias(b4, woven, g * steps)

    for k, q in firsts + seconds[:1]:
        direct(k, q).start()

    front = lax.rem(lax.broadcasted_iota(jnp.int32, (rows, LANES), 1), HEAD_DIM) < HEAD_DIM // 2

    def project(k, j):
        row = pl.multiple_of(block_of(k), rows)
        here = pl.ds(row, rows)
        out = jnp.dot(nrm[here, :], (wq, wk, wv)[j][...], preferred_element_type=f32)
        nat = (qn_all, kw_all, vw_all)[j]
        res = (qr_all, kx_all, vx_all)[j]
        skip = 0 if j == 0 else SPAN
        skip_res = 0 if j == 0 else behind * steps
        step = pl.multiple_of(lax.div(row, WIDE), few)
        for i in range(pairs):
            u = out[:, i * LANES:(i + 1) * LANES]
            if j < 2:
                swapped = jnp.where(
                    front,
                    pltpu.roll(u, LANES - HEAD_DIM // 2, 1),
                    pltpu.roll(u, HEAD_DIM // 2, 1),
                )
                u = u * cos_t[here, :] + swapped * sin_t[here, :]
            if j == 0:
                u = u * HEAD_DIM ** (-0.5)
            nat[i, pl.ds(row + skip, rows), :] = u.astype(bf16)
            scr[i] = u
        for i in range(pairs):
            for r in range(WIDE):
                res[i, 4 * (r % 4) + r // 4, pl.ds(step + skip_res, few), :] = scr[i, pl.ds(r, few, stride=WIDE), :].astype(bf16)

    def project_ext(j):
        out = jnp.dot(ext[...], (wq, wk, wv)[j][...], preferred_element_type=f32)
        nat = (qn_all, kw_all, vw_all)[j]
        res = (qr_all, kx_all, vx_all)[j]
        for i in range(pairs):
            u = out[:, i * LANES:(i + 1) * LANES]
            if j == 1:
                swapped = jnp.where(
                    front,
                    pltpu.roll(u, LANES - HEAD_DIM // 2, 1),
                    pltpu.roll(u, HEAD_DIM // 2, 1),
                )
                u = u * cos_e[...] + swapped * sin_e[...]
            nat[i, pl.ds(0, SPAN), :] = u[rows - SPAN:].astype(bf16)
            scr[i] = u
        for i in range(pairs):
            for r in range(WIDE):
                slot = 4 * (r % 4) + r // 4
                res[i, slot, pl.ds(end_steps, few), :] = scr[i, pl.ds(r, few, stride=WIDE), :].astype(bf16)

    for j in range(2):
        for k in masks:
            near(k, j).wait_recv()
            own_on(j, k)

    kept[1].wait()
    project(0, 0)
    if count > 1:
        for j in range(2):
            pass_on(j, 1)

    for k, q in firsts:
        direct(k, q).wait_recv()
        if group == 4:
            across(k - 1).start()
            if k == 1:
                direct(2, 0).start()
        twin(k, q).start()
    if count > 2:
        for j in range(2):
            pass_on(j, 2)
    for k, q in seconds[:1]:
        direct(k, q).wait_recv()
        twin(k, q).start()
    for k in masks[:1]:
        for q in range(2):
            twin(k, q).wait_recv()
        project(k, 0)
    if group == 4:
        twin(2, 1).wait_recv()
        if mixed:
            @pl.when((c != 0) & (g + 1 < count))
            def _():
                rise().start()
        across(0).wait_recv()
        twin(3, 0).start()

    def far(j):
        if count > 3:
            pass_on(j, 3)
        if count > 4:
            lax.fori_loop(4, count, lambda d, _: (pass_on(j, d), 0)[1], 0)

    def early(pair, j):
        ref = (kw_all, vw_all)[j]
        return remote(
            ref.at[pair, pl.ds(all_rows, SPAN)], ref.at[pair, pl.ds(0, SPAN)],
            early_s.at[pair, j], early_r.at[pair, j], (after[0], t),
        )

    def late(pair, j, k, b):
        ref = (kx_all, vx_all)[j]
        at = pl.multiple_of(flip(c, k) * few, few)
        return remote(
            ref.at[pair, :, pl.ds(behind * steps + at, few)],
            ref.at[pair, :, pl.ds((behind - b) * steps + at, few)],
            late_s.at[pair, j, b - 1, k], late_r.at[pair, j, b - 1, k], (after[b - 1], t),
        )

    everything = [0] + masks

    def needed(k):
        return flip(c, k) != group - 1 if mixed else flip(c, k) >= 0

    def send_late(pair, j, k):
        for b in range(1, behind + 1):
            @pl.when((g + b < count) & needed(k))
            def _(b=b):
                late(pair, j, k, b).start()

    def send_early(pair, j):
        @pl.when(g + 1 < count)
        def _():
            early(pair, j).start()

    for j in range(2):
        far(j)
        if group == 4 and j == 0:
            twin(3, 0).wait_recv()
            if mixed:
                @pl.when((c == 0) & (g + 1 < count))
                def _():
                    rise().start()
        for i, k in enumerate(everything[:2]):
            project(k, 1 + j)
            if i > 0:
                send_late(0, j, k - 1)
            elif j == 1:
                send_late(0, 0, everything[:2][-1])
    skip16 = behind * steps - SPAN

    def tile(q, k, v, bias):
        n = q.shape[0]
        low = lax.broadcasted_iota(jnp.int32, (n, LANES), 1) < HEAD_DIM
        low_q = low.astype(f32).astype(bf16)
        both = jnp.concatenate([q * low_q, q * (1 - low_q)], axis=0)
        sc = lax.dot_general(both, k, (((1,), (1,)), ((), ())), preferred_element_type=f32)
        sc = sc + jnp.concatenate([bias, bias], axis=0)
        m = jnp.max(sc, axis=-1, keepdims=True)
        e = jnp.exp(sc - m).astype(bf16)
        o = jnp.dot(e, jnp.concatenate([v, jnp.ones_like(v)], axis=1), preferred_element_type=f32)
        wide_m = jnp.broadcast_to(m, (2 * n, LANES))
        return (
            jnp.where(low, o[:n, :LANES], o[n:, :LANES]),
            jnp.where(low, wide_m[:n], wide_m[n:]),
            jnp.where(low, o[:n, LANES:], o[n:, LANES:]),
        )

    blocks4 = steps // 32
    def tiles_of(p):
        qn, kw, vw, qr, kx, vx = (ref.at[p] for ref in (qn_all, kw_all, vw_all, qr_all, kx_all, vx_all))
        acc1, m1, l1 = (ref.at[p] for ref in (acc1_all, m1_all, l1_all))
        acc4, m4, l4 = (ref.at[p] for ref in (acc4_all, m4_all, l4_all))

        def step16(slot, _):
            r = 4 * (slot % 4) + slot // 4
            keys = pl.ds(skip16, steps + SPAN)
            o16, m16, l16 = tile(qr[slot], kx[slot, keys, :], vx[slot, keys, :], b16[...])
            apart = pl.ds(r, steps, stride=WIDE)
            here = pl.ds(pl.multiple_of(slot * steps, steps), steps)
            m_1, m_4 = m1[apart, :], m4[here, :]
            top = jnp.maximum(m16, jnp.maximum(m_1, m_4))
            e1, e4, e16 = jnp.exp(m_1 - top), jnp.exp(m_4 - top), jnp.exp(m16 - top)
            whole = l1[apart, :] * e1 + l4[here, :] * e4 + l16 * e16
            mixed = acc1[apart, :] * e1 + acc4[here, :] * e4 + o16 * e16
            att[p, slot] = (mixed / whole).astype(bf16)
            wide[apart, :] = top + jnp.log(whole)
            return 0

        def step4(r, i):
            at = i * 32
            low = at + behind * steps - 32
            if not isinstance(i, int):
                at = pl.multiple_of(at, 32)
                low = pl.multiple_of(low, 32)
            keys = pl.ds(low, 64)
            got = tile(
                jnp.concatenate([qr[4 * r + j, pl.ds(at, 32), :] for j in range(4)], axis=0),
                jnp.concatenate([kx[4 * r + j, keys, :] for j in range(4)], axis=0),
                jnp.concatenate([vx[4 * r + j, keys, :] for j in range(4)], axis=0),
                b4[0 if isinstance(i, int) else 1],
            )
            for ref, value in zip((acc4, m4, l4), got):
                for j in range(4):
                    ref[pl.ds(pl.multiple_of((4 * r + j) * steps + at, 32), 32), :] = value[j * 32:(j + 1) * 32]
            return 0

        def step1(i, _):
            at = pl.multiple_of(i * SPAN, SPAN)
            here = pl.ds(at, SPAN)
            keys = pl.ds(at, 2 * SPAN)
            got = tile(qn[here, :], kw[keys, :], vw[keys, :], b1[jnp.minimum(i, 1)])
            for ref, value in zip((acc1, m1, l1), got):
                ref[here, :] = value
            return 0

        def rest4():
            if blocks4 > 1:
                lax.fori_loop(
                    0, 4 * (blocks4 - 1),
                    lambda idx, _: step4(idx // (blocks4 - 1), idx % (blocks4 - 1) + 1), 0, unroll=4,
                )

        halves = all_rows // SPAN // 2

        def part1(side):
            first = side * halves + 1
            lax.fori_loop(0, halves - 1, lambda n, _: step1(first + n, 0), 0, unroll=halves - 1)

        def soon1():
            part1(lax.div(2 * c, group))

        def rest1():
            part1(1 - lax.div(2 * c, group))
            step1(halves, 0)

        return rest4, rest1, step4, step1, step16, soon1

    work = [tiles_of(p) for p in range(pairs)]

    for p in range(pairs):
        work[p][5]()
    if group == 4:
        direct(2, 0).wait_recv()
        twin(2, 0).start()
        across(1).wait_recv()
        twin(3, 1).start()
        send_late(0, 1, 1)
        twin(2, 0).wait_recv()
        project(2, 1)
        project(2, 2)
        if mixed:
            pl.when(g >= 1)(share_rise)
        send_late(0, 0, 2)
        twin(3, 1).wait_recv()
        project(3, 1)
        send_late(0, 1, 2)
        project(3, 2)
        send_late(0, 0, 3)
        project(2, 0)
        project(3, 0)
        send_late(0, 1, 3)
    else:
        send_late(0, 1, everything[-1])
    if not mixed:
        for j in range(2):
            send_early(0, j)

    def part_of(pair, j, u, b):
        ref = (kx_all, vx_all)[j]
        return remote(
            ref.at[pair, pl.ds(4 * u, 4), pl.ds(behind * steps, end_steps)],
            ref.at[pair, pl.ds(4 * u, 4), pl.ds((behind - b) * steps, end_steps)],
            late_s.at[pair, j, b - 1, u], late_r.at[pair, j, b - 1, u], (after[b - 1], t),
        )

    for pair in range(1, pairs):
        if not mixed:
            for j in range(2):
                send_early(pair, j)
        for u in range(4):
            for j in range(2):
                for b in range(1, behind + 1):
                    @pl.when(g + b < count)
                    def _(pair=pair, j=j, u=u, b=b):
                        part_of(pair, j, u, b).start()


    mine = pl.ds(pl.multiple_of(c * LANES, LANES), LANES)
    own_steps = pl.ds(pl.multiple_of(c * few, few), few)

    def back(p, k, u):
        slots = pl.ds(4 * u, 4)
        span = pl.ds(pl.multiple_of(flip(c, k) * few, few), few)
        return remote(
            att.at[p, slots, span], att_in.at[p, slots, :, mine],
            back_s.at[p, k - 1, u], back_r.at[p, k - 1, u], (peer[k], t),
        )

    def level(p, k):
        span = pl.ds(pl.multiple_of(flip(c, k) * rows, rows), rows)
        return remote(lw.at[p, :, span], lw_in.at[c, p], level_s.at[p, k - 1], level_r.at[p, k - 1], (peer[k], t))

    def send_back(p, u):
        for k in masks[::-1]:
            back(p, k, u).start()
        slots = pl.ds(4 * u, 4)
        att_in[p, slots, :, mine] = att[p, slots, own_steps, :]

    def levels(p):
        def turn(i, _):
            here = pl.ds(pl.multiple_of(i * SPAN, SPAN), SPAN)
            turned = jnp.transpose(wide[here, :])
            lw[p, 0:1, here] = turned[0:1]
            lw[p, 1:2, here] = turned[HEAD_DIM:HEAD_DIM + 1]
            return 0

        lax.fori_loop(0, all_rows // SPAN, turn, 0, unroll=4)

    def send_levels(p):
        for k in masks:
            level(p, k).start()
        lw_in[c, p] = lw[p, :, pl.ds(start_row, rows)]

    def fetched(p):
        for copy in kept[4 + p * group:4 + (p + 1) * group]:
            copy.wait()

    def mix_out(p):
        fetched(p)
        for k in masks:
            for u in range(4):
                back(p, k, u).wait_recv()
        rows_in = att_in[p].reshape(WIDE * few, group * LANES)
        value = jnp.dot(rows_in, wo[p], preferred_element_type=f32).reshape(total.shape)
        total[...] = value if p == 0 else total[...] + value

    last = pairs - 1
    thin = few // n_tp

    def swap(k, u):
        return remote(
            snd.at[k - 1, u], rcv.at[k - 1, u], swap_s.at[k - 1, u], swap_r.at[k - 1, u],
            (s, lax.rem(t + k, n_tp)),
        )

    def share_of(owner):
        if thin % 8 == 0:
            return mix[:, pl.ds(pl.multiple_of(owner * thin, thin), thin), :].astype(bf16)
        value = mix[:, 0:thin, :]
        for o in range(1, n_tp):
            value = jnp.where(owner == o, mix[:, o * thin:(o + 1) * thin, :], value)
        return value.astype(bf16)

    def close(v):
        for u in (2 * v, 2 * v + 1):
            for k in masks:
                back(last, k, u).wait_recv()
        rows_in = att_in[last, pl.ds(8 * v, 8)].reshape(8 * few, group * LANES)
        value = jnp.dot(rows_in, wo[last], preferred_element_type=f32)
        if last > 0:
            value = value + total[pl.ds(2 * v, 2)].reshape(value.shape)
        mix[...] = value.reshape(8, few, value.shape[1])
        for k in range(1, n_tp):
            snd[k - 1, pl.ds(2 * v, 2)] = share_of(lax.rem(t + k, n_tp)).reshape(2, 4, thin, depth)
        keep[pl.ds(2 * v, 2)] = share_of(t).reshape(2, 4, thin, depth)
        for u in (2 * v, 2 * v + 1):
            for k in range(1, n_tp):
                swap(k, u).start()

    def settle(u):
        value = keep[u].astype(f32)
        for k in range(1, n_tp):
            swap(k, u).wait_recv()
            value = value + rcv[k - 1, u].astype(f32)
        scale = lax.rsqrt(jnp.mean(value * value, axis=-1, keepdims=True) + EPS)
        value = value * scale * post_ref[...]
        for j in range(4):
            for i in range(depth // LANES):
                final[i, pl.ds(u + 4 * j, thin, stride=WIDE), :] = value[j, :, i * LANES:(i + 1) * LANES]

    def ext_first():
        for k, q in firsts:
            ext_direct(k, q).wait_recv()
            ext_across(k - 1).start()
            ext_twin(k, q).start()

    def ext_second():
        for k, q in seconds:
            ext_direct(k, q).wait_recv()
            ext_twin(k, q).start()

    def ext_third():
        for k, q in thirds:
            ext_across(q).wait_recv()
            ext_twin(k, q).start()
        ext_twin(0, 0).wait_recv()
        for k in masks:
            for q in range(2):
                ext_twin(k, q).wait_recv()
        for j in (1, 2):
            project_ext(j)

    stages = []
    if mixed:
        stages = [ext_first, ext_second, ext_third]
    for p in range(pairs):
        for part_work in work[p][:2]:
            part_work()
            if stages:
                pl.when(g >= 1)(stages.pop(0))
    for stage in stages:
        pl.when(g >= 1)(stage)
    for p in range(pairs):
        rest4, rest1, step4, step1, step16, _ = work[p]
        if not mixed:
            for j in range(2):
                @pl.when(g >= 1)
                def _(j=j):
                    early(p, j).wait_recv()
        step1(0, 0)
        if p == last:
            fetched(last)
        if p == 0:
            for j in range(2):
                for b in range(1, behind + 1):
                    for k in everything:
                        @pl.when((g >= b) & needed(k))
                        def _(j=j, b=b, k=k):
                            late(0, j, k, b).wait_recv()
        for u in range(4):
            if p > 0:
                for j in range(2):
                    for b in range(1, behind + 1):
                        @pl.when(g >= b)
                        def _(j=j, b=b, u=u):
                            part_of(p, j, u, b).wait_recv()
            step4(u, 0)
            lax.fori_loop(0, 4, lambda n, _, u=u: step16(4 * u + n, 0), 0, unroll=4)
            send_back(p, u)
            if p > 0 and u == 0:
                mix_out(p - 1)
            if p == last and u == 2:
                close(0)
            if p == last and u == 3:
                settle(0)
                settle(1)
        levels(p)
        send_levels(p)

    close(1)
    settle(2)
    heads = 2 * pairs
    for p in range(pairs):
        for k in masks:
            level(p, k).wait_recv()
    for i in range(group):
        for p in range(pairs):
            for h in range(2):
                row = i * heads + p * 2 + h
                lw_ref[row:row + 1, :] = lw_in[i, p, h:h + 1, :]
    settle(3)
    for i in range(depth // LANES):
        out_ref[:, i * LANES:(i + 1) * LANES] = final[i].astype(bf16)

    for k in range(1, n_tp):
        for u in range(4):
            swap(k, u).wait_send()
    for p in range(pairs):
        for k in masks:
            level(p, k).wait_send()
            for u in range(4):
                back(p, k, u).wait_send()
    for j in range(2):
        for k in masks:
            near(k, j).wait_send()
        for d in range(min(count - 1, 4)):
            passed(j, d)
        if count > 5:
            lax.fori_loop(4, count - 1, lambda d, _, j=j: (passed(j, d), 0)[1], 0)
    for k, q in firsts + seconds:
        direct(k, q).wait_send()
        twin(k, q).wait_send()
    if group == 4:
        for i in range(2):
            across(i).wait_send()
            twin(3, i).wait_send()
    if mixed:
        @pl.when(g + 1 < count)
        def _():
            rise().wait_send()

        @pl.when(g >= 1)
        def _():
            ext_twin(0, 0).wait_send()
            for k, q in firsts + seconds:
                ext_direct(k, q).wait_send()
                ext_twin(k, q).wait_send()
            for i in range(2):
                ext_across(i).wait_send()
                ext_twin(3, i).wait_send()
    for pair in range(pairs):
        for j in range(2):
            if not mixed:
                @pl.when(g + 1 < count)
                def _(pair=pair, j=j):
                    early(pair, j).wait_send()

            for b in range(1, behind + 1):
                if pair == 0:
                    for k in everything:
                        @pl.when((g + b < count) & needed(k))
                        def _(j=j, b=b, k=k):
                            late(0, j, k, b).wait_send()
                else:
                    @pl.when(g + b < count)
                    def _(pair=pair, j=j, b=b):
                        for u in range(4):
                            part_of(pair, j, u, b).wait_send()


def layer(mesh, group, behind, hidden, gain, freq, wq, wk, wv, wo, post):
    n_sp = mesh.shape["sp"]
    n_tp = mesh.shape["tp"]
    rows, depth = hidden.shape
    w_rows, width = wk.shape
    part = width // group
    pairs = part // LANES
    all_rows = rows * group
    steps = all_rows // WIDE
    few = rows // WIDE
    thin = few // n_tp
    count = n_sp // group
    share = rows // n_tp
    f32, bf16 = jnp.float32, jnp.bfloat16
    dma = pltpu.SemaphoreType.DMA
    mixed = behind == 1 and group == 4
    extra = pltpu.VMEM((rows, depth) if mixed else (16, LANES), bf16)
    small = pltpu.VMEM((rows, LANES) if mixed else (8, LANES), f32)
    state = pltpu.VMEM((pairs, all_rows, LANES), f32)
    weight = pltpu.VMEM((depth, part), bf16)
    table = pltpu.VMEM((all_rows, LANES), f32)
    ring = pltpu.VMEM((pairs, SPAN + all_rows, LANES), bf16)
    woven = pltpu.VMEM((pairs, WIDE, (behind + 1) * steps, LANES), bf16)
    pieces = pltpu.VMEM((n_tp - 1, 4, 4, thin, depth), bf16)
    vmem = pl.BlockSpec(memory_space=pltpu.VMEM)
    near = max(group - 1, 1)
    return pl.pallas_call(
        functools.partial(layer_kernel, n_sp, n_tp, group, behind),
        out_shape=(
            jax.ShapeDtypeStruct((share, depth), bf16),
            jax.ShapeDtypeStruct((width // HEAD_DIM, rows), f32),
        ),
        in_specs=[ANY, vmem, vmem, ANY, ANY, ANY, ANY, vmem],
        out_specs=(vmem, vmem),
        scratch_shapes=[
            pltpu.VMEM((rows, depth), bf16), pltpu.VMEM((all_rows, depth), bf16), extra,
            weight, weight, weight, pltpu.VMEM((pairs, group * LANES, depth), bf16), table, table, small, small,
            pltpu.VMEM((pairs, rows, LANES), f32),
            pltpu.VMEM((pairs, all_rows, LANES), bf16), ring, ring,
            pltpu.VMEM((pairs, WIDE, steps, LANES), bf16), woven, woven,
            state, state, state, state, state, state, table,
            pltpu.VMEM((2, SPAN, 2 * SPAN), f32),
            pltpu.VMEM((2, SPAN, 2 * SPAN), f32),
            pltpu.VMEM((steps, steps + SPAN), f32),
            pltpu.VMEM((pairs, WIDE, steps, LANES), bf16), pltpu.VMEM((pairs, WIDE, few, group * LANES), bf16),
            pltpu.VMEM((pairs, 2, all_rows), f32), pltpu.VMEM((group, pairs, 2, rows), f32),
            pltpu.VMEM((4, 4 * few, depth), f32), pltpu.VMEM((8, few, depth), f32),
            pltpu.VMEM((4, 4, thin, depth), bf16), pieces, pieces,
            pltpu.VMEM((depth // LANES, share, LANES), f32),
            dma((4 + pairs * group,)), dma((2, 2, group)), dma((2, 2, group)),
            dma((2, near)), dma((2, near)), dma((2, 2, count)), dma((2, 2, count)),
            dma((2, 2)), dma((2, 2)), dma((2,)), dma((2,)), dma((3, 2)), dma((3, 2)),
            dma((1,)), dma((1,)), dma((2, 2)), dma((2, 2)), dma((2,)), dma((2,)), dma((4, 2)), dma((4, 2)),
            dma((pairs, 2)), dma((pairs, 2)),
            dma((pairs, 2, behind, 4)), dma((pairs, 2, behind, 4)),
            dma((pairs, near, 4)), dma((pairs, near, 4)), dma((pairs, near)), dma((pairs, near)),
            dma((n_tp - 1, 4)), dma((n_tp - 1, 4)),
        ],
        compiler_params=pltpu.CompilerParams(
            vmem_limit_bytes=63 * 1024 * 1024, collective_id=0, has_side_effects=True
        ),
        name="layer_core",
    )(hidden, gain, freq, wq, wk, wv, wo, post)


def place_kernel(out_ref, lw_ref, out_to, lw_to, held, held_lw, into, away):
    count = into.shape[0] - 1
    size = out_ref.shape[0] // count
    spans = [pl.ds(i * size, size) for i in range(count)]
    reads = [pltpu.make_async_copy(lw_ref, held_lw, into.at[count])]
    reads += [pltpu.make_async_copy(out_ref.at[x], held.at[x], into.at[i]) for i, x in enumerate(spans)]
    writes = [pltpu.make_async_copy(held_lw, lw_to, away.at[count])]
    writes += [pltpu.make_async_copy(held.at[x], out_to.at[x], away.at[i]) for i, x in enumerate(spans)]
    for copy in reads:
        copy.start()
    for read, write in zip(reads, writes):
        read.wait()
        write.start()
    for write in writes:
        write.wait()


def place(out, levels):
    parts = 4 if out.shape[0] % 64 == 0 else 1
    return pl.pallas_call(
        place_kernel,
        out_shape=(jax.ShapeDtypeStruct(out.shape, out.dtype), jax.ShapeDtypeStruct(levels.shape, levels.dtype)),
        in_specs=[ANY, ANY],
        out_specs=(ANY, ANY),
        scratch_shapes=[
            pltpu.VMEM(out.shape, out.dtype), pltpu.VMEM(levels.shape, levels.dtype),
            pltpu.SemaphoreType.DMA((parts + 1,)), pltpu.SemaphoreType.DMA((parts + 1,)),
        ],
        compiler_params=pltpu.CompilerParams(vmem_limit_bytes=62 * 1024 * 1024),
        name="place_outputs",
    )(out, levels)


def body(mesh, hidden_in, pre_gain, query_proj, key_proj, value_proj, out_proj, post_gain):
    rows, depth = hidden_in.shape
    width = query_proj.shape[1]
    group = group_of(mesh, width)
    all_rows = rows * group
    behind = -(-(WIDE * SPAN) // all_rows)
    half_dim = HEAD_DIM // 2
    frequency = ROPE_BASE ** (-(np.arange(half_dim) * 2.0 / HEAD_DIM))
    freq = jnp.asarray(np.tile(frequency, LANES // half_dim)[None, :], jnp.float32)
    out, levels = layer(
        mesh, group, behind, hidden_in, pre_gain[None, :], freq,
        query_proj, key_proj, value_proj, out_proj, post_gain[None, :],
    )
    return place(out, levels)


def solution(mesh):
    placed = (P("sp", None), P(), P(None, "tp"), P("sp", "tp"), P("sp", "tp"), P("tp", None), P())
    return jax.shard_map(
        functools.partial(body, mesh),
        mesh=mesh,
        in_specs=placed,
        out_specs=(P(("sp", "tp"), None), P("tp", "sp")),
        check_vma=False,
    )
```

```python
import functools

import jax
import jax.numpy as jnp
import numpy as np
from jax import lax
from jax.experimental import pallas as pl
from jax.experimental.pallas import tpu as pltpu
from jax.sharding import PartitionSpec as P

HEAD_DIM = 64
SPAN = 128
EPS = 1e-06
ROPE_BASE = 10000.0
WIDE = 16
LANES = 128
MESH = pl.DeviceIdType.MESH
ANY = pl.BlockSpec(memory_space=pl.ANY)
NEG = -1e30


def remote(src, dst, send, recv, peer):
    return pltpu.make_async_remote_copy(
        src_ref=src, dst_ref=dst, send_sem=send, recv_sem=recv, device_id=peer, device_id_type=MESH
    )


def group_of(mesh, width):
    for size in (4, 2):
        if mesh.shape["sp"] % size == 0 and width % (size * LANES) == 0:
            return size
    return 1


def flip(c, mask):
    out = c
    if mask & 1:
        out = out + 1 - 2 * lax.rem(c, 2)
    if mask & 2:
        out = out + 2 - 4 * lax.rem(lax.div(c, 2), 2)
    return out


def layer_kernel(
    n_sp, n_tp, group, behind,
    hid_ref, gain_ref, freq_ref, wq_ref, wk_ref, wv_ref, wo_ref, post_ref,
    out_ref, lw_ref,
    raw, nrm, ext, wq, wk, wv, wo, cos_t, sin_t, cos_e, sin_e, scr,
    qn_all, kw_all, vw_all, qr_all, kx_all, vx_all,
    acc1_all, m1_all, l1_all, acc4_all, m4_all, l4_all, wide, b1, b4, b16,
    att, att_in, lw, lw_in, total, mix, keep, snd, rcv, final,
    local, own_s, own_r, near_s, near_r, line_s, line_r, dir_s, dir_r, across_s, across_r, twin_s, twin_r,
    rise_s, rise_r, edir_s, edir_r, eacross_s, eacross_r, etwin_s, etwin_r,
    early_s, early_r, late_s, late_r, back_s, back_r, level_s, level_r, swap_s, swap_r,
):
    f32, bf16 = jnp.float32, jnp.bfloat16
    s = lax.axis_index("sp")
    t = lax.axis_index("tp")
    rows, depth = hid_ref.shape
    all_rows = rows * group
    w_rows = wk_ref.shape[0]
    part = wq.shape[1]
    pairs = part // LANES
    steps = all_rows // WIDE
    few = rows // WIDE
    quarter = rows // 4
    count = n_sp // group
    c = lax.rem(s, group)
    base = s - c
    g = lax.div(s, group)
    half = lax.rem(t, 2)
    sibling = (s, t + 1 - 2 * half)
    masks = list(range(1, group))
    peer = {k: base + flip(c, k) for k in masks}
    up = lax.rem(s + group, n_sp)
    down = lax.rem(s + n_sp - group, n_sp)
    after = [lax.rem(s + b * group, n_sp) for b in range(1, behind + 1)]
    before = [lax.rem(s + n_sp - b * group, n_sp) for b in range(1, behind + 1)]
    start_row = pl.multiple_of(c * rows, rows)
    mixed = behind == 1 and group == 4
    end_steps = steps - few if mixed else steps

    kept = [pltpu.make_async_copy(hid_ref, raw, local.at[0])]
    own_cols = pl.ds(pl.multiple_of(c * part, LANES), part)
    own_rows = pl.ds(pl.multiple_of(s * w_rows, w_rows), w_rows)
    kept.append(pltpu.make_async_copy(wq_ref.at[:, own_cols], wq, local.at[1]))
    for j, (src, dst) in enumerate(((wk_ref, wk), (wv_ref, wv))):
        kept.append(pltpu.make_async_copy(src.at[:, own_cols], dst.at[own_rows], local.at[2 + j]))
    for p in range(pairs):
        for i in range(group):
            kept.append(pltpu.make_async_copy(
                wo_ref.at[pl.ds(i * part + p * LANES, LANES)], wo.at[p, pl.ds(i * LANES, LANES)],
                local.at[4 + p * group + i],
            ))
    for copy in kept:
        copy.start()

    known = [(peer[k], t) for k in masks] + [(x, t) for x in after + before]
    known += [(s, lax.rem(t + k, n_tp)) for k in range(1, n_tp)]
    barrier = pltpu.get_barrier_semaphore()
    for other in known:
        pl.semaphore_signal(barrier, inc=1, device_id=other, device_id_type=MESH)

    half_dim = HEAD_DIM // 2
    lo = lax.broadcasted_iota(jnp.int32, (LANES, LANES), 0).astype(f32) * freq_ref[...]
    cos_lo, sin_lo = jnp.cos(lo), jnp.sin(lo)
    lane = lax.rem(lax.broadcasted_iota(jnp.int32, (1, LANES), 1), HEAD_DIM)
    sign = jnp.where(lane < half_dim, -1.0, 1.0)

    def fill(i, _):
        hi = (base * rows + i * LANES).astype(f32) * freq_ref[...]
        cos_hi, sin_hi = jnp.cos(hi), jnp.sin(hi)
        at = pl.ds(pl.multiple_of(i * LANES, LANES), LANES)
        cos_t[at, :] = cos_lo * cos_hi - sin_lo * sin_hi
        sin_t[at, :] = (sin_lo * cos_hi + cos_lo * sin_hi) * sign
        return 0

    lax.fori_loop(0, all_rows // LANES, fill, 0)

    def fill_ext(i, _):
        hi = (base * rows - rows + i * LANES).astype(f32) * freq_ref[...]
        cos_hi, sin_hi = jnp.cos(hi), jnp.sin(hi)
        at = pl.ds(pl.multiple_of(i * LANES, LANES), LANES)
        cos_e[at, :] = cos_lo * cos_hi - sin_lo * sin_hi
        sin_e[at, :] = (sin_lo * cos_hi + cos_lo * sin_hi) * sign
        return 0

    if mixed:
        lax.fori_loop(0, rows // LANES, fill_ext, 0)

    @pl.when(g < behind)
    def _():
        for pair in range(pairs):
            for ref in (kw_all, vw_all):
                @pl.when(g < 1)
                def _(ref=ref, pair=pair):
                    ref[pair, pl.ds(0, SPAN), :] = jnp.zeros((SPAN, LANES), bf16)
            for ref in (kx_all, vx_all):
                for b in range(1, behind + 1):
                    @pl.when(g < b)
                    def _(ref=ref, pair=pair, b=b):
                        ref[pair, :, pl.ds((behind - b) * steps, steps), :] = jnp.zeros((WIDE, steps, LANES), bf16)

    pl.semaphore_wait(barrier, len(known))

    def near(k, j):
        src, dst = ((wk_ref, wk), (wv_ref, wv))[j]
        cols = pl.ds(pl.multiple_of(flip(c, k) * part, LANES), part)
        return remote(src.at[:, cols], dst.at[own_rows], near_s.at[j, k - 1], near_r.at[j, k - 1], (peer[k], t))

    def line(way, j, d):
        ref = (wk, wv)[j]
        to, off = ((up, g - d), (down, g + d))[way]
        off = jnp.clip(off, 0, count - 1)
        slot = ref.at[pl.ds(pl.multiple_of(off * group * w_rows, group * w_rows), group * w_rows)]
        return remote(slot, slot, line_s.at[way, j, d], line_r.at[way, j, d + 1], (to, t))

    def line_in(way, j, d):
        ref = (wk, wv)[j]
        off = jnp.clip((g - d, g + d)[way], 0, count - 1)
        slot = ref.at[pl.ds(pl.multiple_of(off * group * w_rows, group * w_rows), group * w_rows)]
        return remote(slot, slot, line_s.at[way, j, d - 1], line_r.at[way, j, d], ((up, down)[way], t))

    def line_own(way, j, k):
        at = pl.multiple_of((base + flip(c, k)) * w_rows, w_rows)
        slot = (wk, wv)[j].at[pl.ds(at, w_rows)]
        return remote(slot, slot, own_s.at[way, j, k], own_r.at[way, j, k], ((up, down)[way], t))

    def has_in(way, d):
        return g >= d if way == 0 else g + d < count

    def has_out(way, d):
        if way == 0:
            return (g >= d) & (g + 1 < count)
        return (g + d < count) & (g >= 1)

    def own_on(j, k):
        for way in range(2):
            @pl.when(has_out(way, 0))
            def _(way=way):
                line_own(way, j, k).start()

    def pass_on(j, d):
        for way in range(2):
            @pl.when(has_in(way, d))
            def _(way=way):
                if isinstance(d, int) and d == 1:
                    for k in [0] + masks:
                        line_own(way, j, k).wait_recv()
                else:
                    line_in(way, j, d).wait_recv()

            if not (isinstance(d, int) and d == count - 1):
                @pl.when(has_out(way, d))
                def _(way=way):
                    line(way, j, d).start()

    def passed(j, d):
        for way in range(2):
            @pl.when(has_out(way, d))
            def _(way=way):
                if isinstance(d, int) and d == 0:
                    for k in [0] + masks:
                        line_own(way, j, k).wait_send()
                else:
                    line(way, j, d).wait_send()

    def piece(block, side, q):
        return nrm.at[pl.ds(pl.multiple_of(block * rows + side * (2 * quarter) + q * quarter, quarter), quarter)]

    def direct(k, q):
        slot = piece(c, half, q)
        return remote(slot, slot, dir_s.at[k - 1, q], dir_r.at[k - 1, q], (peer[k], t))

    def across(i):
        k, other = ((1, 2), (2, 1))[i]
        slot = piece(flip(c, k), half, i)
        return remote(slot, slot, across_s.at[i], across_r.at[i], (peer[other], t))

    def twin(k, q):
        slot = piece(flip(c, k), half, q)
        return remote(slot, slot, twin_s.at[k - 1, q], twin_r.at[k - 1, q], sibling)

    bit = rows // 16

    def rise():
        at = pl.multiple_of(c * 4 * bit + half * 2 * bit, 2 * bit)
        src = nrm.at[pl.ds(pl.multiple_of(all_rows - rows + at, 2 * bit), 2 * bit)]
        return remote(src, ext.at[pl.ds(at, 2 * bit)], rise_s.at[0], rise_r.at[0], (up, t))

    def crumb(block, side, q, n=1):
        return ext.at[pl.ds(pl.multiple_of(block * 4 * bit + side * 2 * bit + q * bit, bit), n * bit)]

    def ext_direct(k, q):
        slot = crumb(c, half, q)
        return remote(slot, slot, edir_s.at[k - 1, q], edir_r.at[k - 1, q], (peer[k], t))

    def ext_across(i):
        k, other = ((1, 2), (2, 1))[i]
        slot = crumb(flip(c, k), half, i)
        return remote(slot, slot, eacross_s.at[i], eacross_r.at[i], (peer[other], t))

    def ext_twin(k, q):
        slot = crumb(flip(c, k), half, q, 2 if k == 0 else 1)
        return remote(slot, slot, etwin_s.at[k, q], etwin_r.at[k, q], sibling)

    def share_rise():
        rise().wait_recv()
        for k, q in firsts + seconds:
            ext_direct(k, q).start()
        ext_twin(0, 0).start()

    for j in range(2):
        for k in masks:
            near(k, j).start()
    kept[2].wait()
    own_on(0, 0)
    kept[3].wait()
    own_on(1, 0)
    firsts = {4: [(1, 0), (2, 1)], 2: [(1, 0)], 1: []}[group]
    seconds = {4: [(1, 1), (2, 0)], 2: [(1, 1)], 1: []}[group]
    thirds = {4: [(3, 0), (3, 1)], 2: [], 1: []}[group]
    def block_of(k):
        return flip(c, k) * rows

    kept[0].wait()

    def norm(i, _):
        x = raw[pl.ds(pl.multiple_of(i * quarter, quarter), quarter), :].astype(f32)
        scale = lax.rsqrt(jnp.mean(x * x, axis=-1, keepdims=True) + EPS)
        at = pl.ds(pl.multiple_of(start_row + i * quarter, quarter), quarter)
        nrm[at, :] = (x * scale * gain_ref[...]).astype(bf16)
        return 0

    lax.fori_loop(0, 4, norm, 0)

    def put_bias(ref, near_by, first_of):
        shape = ref.shape[1:]
        a = lax.broadcasted_iota(jnp.int32, shape, 0)
        b = lax.broadcasted_iota(jnp.int32, shape, 1)
        distance, place = near_by(a, b)
        band = (distance >= 0) & (distance <= SPAN)
        ref[0] = jnp.where(band & (place + first_of >= 0), 0.0, NEG).astype(f32)
        ref[1] = jnp.where(band, 0.0, NEG).astype(f32)

    def plain(a, b):
        return a + SPAN - b, b - SPAN

    def woven(a, b):
        return 4 * (a % 32 + 32 - b % 64) + a // 32 - b // 64, b % 64 - 32

    put_bias(b1, plain, g * all_rows)
    a16 = lax.broadcasted_iota(jnp.int32, b16.shape, 0)
    k16 = lax.broadcasted_iota(jnp.int32, b16.shape, 1)
    seen = (a16 + SPAN >= k16) & (a16 <= k16) & (g * steps + k16 >= SPAN)
    b16[...] = jnp.where(seen, 0.0, NEG).astype(f32)
    put_bias(b4, woven, g * steps)

    for k, q in firsts + seconds[:1]:
        direct(k, q).start()

    front = lax.rem(lax.broadcasted_iota(jnp.int32, (rows, LANES), 1), HEAD_DIM) < HEAD_DIM // 2

    def project(*items):
        outs = [
            jnp.dot(nrm[pl.ds(pl.multiple_of(block_of(k), rows), rows), :], (wq, wk, wv)[j][...],
                    preferred_element_type=f32)
            for k, j in items
        ]
        for n, (k, j) in enumerate(items):
            place_rows(k, j, outs[n], scr.at[n])

    def place_rows(k, j, out, scr):
        row = pl.multiple_of(block_of(k), rows)
        here = pl.ds(row, rows)
        nat = (qn_all, kw_all, vw_all)[j]
        res = (qr_all, kx_all, vx_all)[j]
        skip = 0 if j == 0 else SPAN
        skip_res = 0 if j == 0 else behind * steps
        step = pl.multiple_of(lax.div(row, WIDE), few)
        for i in range(pairs):
            u = out[:, i * LANES:(i + 1) * LANES]
            if j < 2:
                swapped = jnp.where(
                    front,
                    pltpu.roll(u, LANES - HEAD_DIM // 2, 1),
                    pltpu.roll(u, HEAD_DIM // 2, 1),
                )
                u = u * cos_t[here, :] + swapped * sin_t[here, :]
            if j == 0:
                u = u * HEAD_DIM ** (-0.5)
            nat[i, pl.ds(row + skip, rows), :] = u.astype(bf16)
            scr[i] = u
        for i in range(pairs):
            for r in range(WIDE):
                res[i, 4 * (r % 4) + r // 4, pl.ds(step + skip_res, few), :] = scr[i, pl.ds(r, few, stride=WIDE), :].astype(bf16)

    def project_ext(j):
        out = jnp.dot(ext[...], (wq, wk, wv)[j][...], preferred_element_type=f32)
        nat = (qn_all, kw_all, vw_all)[j]
        res = (qr_all, kx_all, vx_all)[j]
        for i in range(pairs):
            u = out[:, i * LANES:(i + 1) * LANES]
            if j == 1:
                swapped = jnp.where(
                    front,
                    pltpu.roll(u, LANES - HEAD_DIM // 2, 1),
                    pltpu.roll(u, HEAD_DIM // 2, 1),
                )
                u = u * cos_e[...] + swapped * sin_e[...]
            nat[i, pl.ds(0, SPAN), :] = u[rows - SPAN:].astype(bf16)
            scr[0, i] = u
        for i in range(pairs):
            for r in range(WIDE):
                slot = 4 * (r % 4) + r // 4
                res[i, slot, pl.ds(end_steps, few), :] = scr[0, i, pl.ds(r, few, stride=WIDE), :].astype(bf16)

    for j in range(2):
        for k in masks:
            near(k, j).wait_recv()
            own_on(j, k)

    kept[1].wait()
    project((0, 0))
    if count > 1:
        for j in range(2):
            pass_on(j, 1)

    for k, q in firsts:
        direct(k, q).wait_recv()
        if group == 4:
            across(k - 1).start()
            if k == 1:
                direct(2, 0).start()
        twin(k, q).start()
    if count > 2:
        for j in range(2):
            pass_on(j, 2)
    for k, q in seconds[:1]:
        direct(k, q).wait_recv()
        twin(k, q).start()
    for k in masks[:1]:
        for q in range(2):
            twin(k, q).wait_recv()
        project((k, 0))
    if group == 4:
        twin(2, 1).wait_recv()
        if mixed:
            @pl.when((c != 0) & (g + 1 < count))
            def _():
                rise().start()
        across(0).wait_recv()
        twin(3, 0).start()

    def far(j):
        if count > 3:
            pass_on(j, 3)
        if count > 4:
            lax.fori_loop(4, count, lambda d, _: (pass_on(j, d), 0)[1], 0)

    def early(pair, j):
        ref = (kw_all, vw_all)[j]
        return remote(
            ref.at[pair, pl.ds(all_rows, SPAN)], ref.at[pair, pl.ds(0, SPAN)],
            early_s.at[pair, j], early_r.at[pair, j], (after[0], t),
        )

    def late(pair, j, k, b):
        ref = (kx_all, vx_all)[j]
        at = pl.multiple_of(flip(c, k) * few, few)
        return remote(
            ref.at[pair, :, pl.ds(behind * steps + at, few)],
            ref.at[pair, :, pl.ds((behind - b) * steps + at, few)],
            late_s.at[pair, j, b - 1, k], late_r.at[pair, j, b - 1, k], (after[b - 1], t),
        )

    everything = [0] + masks

    def needed(k):
        return flip(c, k) != group - 1 if mixed else flip(c, k) >= 0

    def send_late(pair, j, k):
        for b in range(1, behind + 1):
            @pl.when((g + b < count) & needed(k))
            def _(b=b):
                late(pair, j, k, b).start()

    def send_early(pair, j):
        @pl.when(g + 1 < count)
        def _():
            early(pair, j).start()

    far(0)
    if group == 4:
        twin(3, 0).wait_recv()
        if mixed:
            @pl.when((c == 0) & (g + 1 < count))
            def _():
                rise().start()
    ready = everything[:2]
    for k in ready:
        project((k, 1))
        if k > 0:
            send_late(0, 0, k - 1)
    far(1)
    project(*[(k, 2) for k in ready])
    send_late(0, 0, ready[-1])

    skip16 = behind * steps - SPAN

    def tile(q, k, v, bias):
        n = q.shape[0]
        low = lax.broadcasted_iota(jnp.int32, (n, LANES), 1) < HEAD_DIM
        low_q = low.astype(f32).astype(bf16)
        both = jnp.concatenate([q * low_q, q * (1 - low_q)], axis=0)
        sc = lax.dot_general(both, k, (((1,), (1,)), ((), ())), preferred_element_type=f32)
        sc = sc + jnp.concatenate([bias, bias], axis=0)
        m = jnp.max(sc, axis=-1, keepdims=True)
        e = jnp.exp(sc - m).astype(bf16)
        o = jnp.dot(e, jnp.concatenate([v, jnp.ones_like(v)], axis=1), preferred_element_type=f32)
        wide_m = jnp.broadcast_to(m, (2 * n, LANES))
        return (
            jnp.where(low, o[:n, :LANES], o[n:, :LANES]),
            jnp.where(low, wide_m[:n], wide_m[n:]),
            jnp.where(low, o[:n, LANES:], o[n:, LANES:]),
        )

    blocks4 = steps // 32
    def tiles_of(p):
        qn, kw, vw, qr, kx, vx = (ref.at[p] for ref in (qn_all, kw_all, vw_all, qr_all, kx_all, vx_all))
        acc1, m1, l1 = (ref.at[p] for ref in (acc1_all, m1_all, l1_all))
        acc4, m4, l4 = (ref.at[p] for ref in (acc4_all, m4_all, l4_all))

        def step16(slot, _):
            r = 4 * (slot % 4) + slot // 4
            keys = pl.ds(skip16, steps + SPAN)
            o16, m16, l16 = tile(qr[slot], kx[slot, keys, :], vx[slot, keys, :], b16[...])
            apart = pl.ds(r, steps, stride=WIDE)
            here = pl.ds(pl.multiple_of(slot * steps, steps), steps)
            m_1, m_4 = m1[apart, :], m4[here, :]
            top = jnp.maximum(m16, jnp.maximum(m_1, m_4))
            e1, e4, e16 = jnp.exp(m_1 - top), jnp.exp(m_4 - top), jnp.exp(m16 - top)
            whole = l1[apart, :] * e1 + l4[here, :] * e4 + l16 * e16
            mixed = acc1[apart, :] * e1 + acc4[here, :] * e4 + o16 * e16
            att[p, slot] = (mixed / whole).astype(bf16)
            wide[apart, :] = top + jnp.log(whole)
            return 0

        def step4(r, i):
            at = i * 32
            low = at + behind * steps - 32
            if not isinstance(i, int):
                at = pl.multiple_of(at, 32)
                low = pl.multiple_of(low, 32)
            keys = pl.ds(low, 64)
            got = tile(
                jnp.concatenate([qr[4 * r + j, pl.ds(at, 32), :] for j in range(4)], axis=0),
                jnp.concatenate([kx[4 * r + j, keys, :] for j in range(4)], axis=0),
                jnp.concatenate([vx[4 * r + j, keys, :] for j in range(4)], axis=0),
                b4[0 if isinstance(i, int) else 1],
            )
            for ref, value in zip((acc4, m4, l4), got):
                for j in range(4):
                    ref[pl.ds(pl.multiple_of((4 * r + j) * steps + at, 32), 32), :] = value[j * 32:(j + 1) * 32]
            return 0

        def step1(i, _):
            at = pl.multiple_of(i * SPAN, SPAN)
            here = pl.ds(at, SPAN)
            keys = pl.ds(at, 2 * SPAN)
            got = tile(qn[here, :], kw[keys, :], vw[keys, :], b1[jnp.minimum(i, 1)])
            for ref, value in zip((acc1, m1, l1), got):
                ref[here, :] = value
            return 0

        def rest4():
            if blocks4 > 1:
                lax.fori_loop(
                    0, 4 * (blocks4 - 1),
                    lambda idx, _: step4(idx // (blocks4 - 1), idx % (blocks4 - 1) + 1), 0, unroll=4,
                )

        halves = all_rows // SPAN // 2

        def part1(side):
            first = side * halves + 1
            lax.fori_loop(0, halves - 1, lambda n, _: step1(first + n, 0), 0, unroll=halves - 1)

        def soon1():
            part1(lax.div(2 * c, group))

        def rest1():
            part1(1 - lax.div(2 * c, group))
            step1(halves, 0)

        return rest4, rest1, step4, step1, step16, soon1

    work = [tiles_of(p) for p in range(pairs)]

    for p in range(pairs):
        work[p][5]()
    for k in ready:
        send_late(0, 1, k)
    if group == 4:
        direct(2, 0).wait_recv()
        twin(2, 0).start()
        across(1).wait_recv()
        twin(3, 1).start()
        twin(2, 0).wait_recv()
        project((2, 1), (2, 2))
        if mixed:
            pl.when(g >= 1)(share_rise)
        twin(3, 1).wait_recv()
        project((3, 1), (3, 2))
        send_late(0, 0, 2)
        send_late(0, 1, 2)
        project((2, 0), (3, 0))
        send_late(0, 0, 3)
        send_late(0, 1, 3)
    if not mixed:
        for j in range(2):
            send_early(0, j)

    def part_of(pair, j, u, b):
        ref = (kx_all, vx_all)[j]
        return remote(
            ref.at[pair, pl.ds(4 * u, 4), pl.ds(behind * steps, end_steps)],
            ref.at[pair, pl.ds(4 * u, 4), pl.ds((behind - b) * steps, end_steps)],
            late_s.at[pair, j, b - 1, u], late_r.at[pair, j, b - 1, u], (after[b - 1], t),
        )

    for pair in range(1, pairs):
        if not mixed:
            for j in range(2):
                send_early(pair, j)
        for u in range(4):
            for j in range(2):
                for b in range(1, behind + 1):
                    @pl.when(g + b < count)
                    def _(pair=pair, j=j, u=u, b=b):
                        part_of(pair, j, u, b).start()


    mine = pl.ds(pl.multiple_of(c * LANES, LANES), LANES)
    own_steps = pl.ds(pl.multiple_of(c * few, few), few)

    def back(p, k, u):
        slots = pl.ds(4 * u, 4)
        span = pl.ds(pl.multiple_of(flip(c, k) * few, few), few)
        return remote(
            att.at[p, slots, span], att_in.at[p, slots, :, mine],
            back_s.at[p, k - 1, u], back_r.at[p, k - 1, u], (peer[k], t),
        )

    def level(p, k):
        span = pl.ds(pl.multiple_of(flip(c, k) * rows, rows), rows)
        return remote(lw.at[p, :, span], lw_in.at[c, p], level_s.at[p, k - 1], level_r.at[p, k - 1], (peer[k], t))

    def send_back(p, u):
        for k in masks[::-1]:
            back(p, k, u).start()
        slots = pl.ds(4 * u, 4)
        att_in[p, slots, :, mine] = att[p, slots, own_steps, :]

    def levels(p):
        def turn(i, _):
            here = pl.ds(pl.multiple_of(i * SPAN, SPAN), SPAN)
            turned = jnp.transpose(wide[here, :])
            lw[p, 0:1, here] = turned[0:1]
            lw[p, 1:2, here] = turned[HEAD_DIM:HEAD_DIM + 1]
            return 0

        lax.fori_loop(0, all_rows // SPAN, turn, 0, unroll=4)

    def send_levels(p):
        for k in masks:
            level(p, k).start()
        lw_in[c, p] = lw[p, :, pl.ds(start_row, rows)]

    def fetched(p):
        for copy in kept[4 + p * group:4 + (p + 1) * group]:
            copy.wait()

    def mix_out(p):
        fetched(p)
        for k in masks:
            for u in range(4):
                back(p, k, u).wait_recv()
        rows_in = att_in[p].reshape(WIDE * few, group * LANES)
        value = jnp.dot(rows_in, wo[p], preferred_element_type=f32).reshape(total.shape)
        total[...] = value if p == 0 else total[...] + value

    last = pairs - 1
    thin = few // n_tp

    def swap(k, u):
        return remote(
            snd.at[k - 1, u], rcv.at[k - 1, u], swap_s.at[k - 1, u], swap_r.at[k - 1, u],
            (s, lax.rem(t + k, n_tp)),
        )

    def share_of(owner):
        if thin % 8 == 0:
            return mix[:, pl.ds(pl.multiple_of(owner * thin, thin), thin), :].astype(bf16)
        value = mix[:, 0:thin, :]
        for o in range(1, n_tp):
            value = jnp.where(owner == o, mix[:, o * thin:(o + 1) * thin, :], value)
        return value.astype(bf16)

    def close(v):
        for u in (2 * v, 2 * v + 1):
            for k in masks:
                back(last, k, u).wait_recv()
        rows_in = att_in[last, pl.ds(8 * v, 8)].reshape(8 * few, group * LANES)
        value = jnp.dot(rows_in, wo[last], preferred_element_type=f32)
        if last > 0:
            value = value + total[pl.ds(2 * v, 2)].reshape(value.shape)
        mix[...] = value.reshape(8, few, value.shape[1])
        for k in range(1, n_tp):
            snd[k - 1, pl.ds(2 * v, 2)] = share_of(lax.rem(t + k, n_tp)).reshape(2, 4, thin, depth)
        keep[pl.ds(2 * v, 2)] = share_of(t).reshape(2, 4, thin, depth)
        for u in (2 * v, 2 * v + 1):
            for k in range(1, n_tp):
                swap(k, u).start()

    def settle(u):
        value = keep[u].astype(f32)
        for k in range(1, n_tp):
            swap(k, u).wait_recv()
            value = value + rcv[k - 1, u].astype(f32)
        scale = lax.rsqrt(jnp.mean(value * value, axis=-1, keepdims=True) + EPS)
        value = value * scale * post_ref[...]
        for j in range(4):
            for i in range(depth // LANES):
                final[i, pl.ds(u + 4 * j, thin, stride=WIDE), :] = value[j, :, i * LANES:(i + 1) * LANES]

    def ext_first():
        for k, q in firsts:
            ext_direct(k, q).wait_recv()
            ext_across(k - 1).start()
            ext_twin(k, q).start()

    def ext_second():
        for k, q in seconds:
            ext_direct(k, q).wait_recv()
            ext_twin(k, q).start()

    def ext_third():
        for k, q in thirds:
            ext_across(q).wait_recv()
            ext_twin(k, q).start()

    def ext_last():
        ext_twin(0, 0).wait_recv()
        for k in masks:
            for q in range(2):
                ext_twin(k, q).wait_recv()
        for j in (1, 2):
            project_ext(j)

    stages = []
    if mixed:
        stages = [ext_first, ext_second, ext_third, ext_last]
    for p in range(pairs):
        for part_work in work[p][:2]:
            part_work()
            if stages:
                pl.when(g >= 1)(stages.pop(0))
    for stage in stages:
        pl.when(g >= 1)(stage)
    for p in range(pairs):
        rest4, rest1, step4, step1, step16, _ = work[p]
        if not mixed:
            for j in range(2):
                @pl.when(g >= 1)
                def _(j=j):
                    early(p, j).wait_recv()
        step1(0, 0)
        if p == last:
            fetched(last)
        if p == 0:
            for j in range(2):
                for b in range(1, behind + 1):
                    for k in everything:
                        @pl.when((g >= b) & needed(k))
                        def _(j=j, b=b, k=k):
                            late(0, j, k, b).wait_recv()
        for u in range(4):
            if p > 0:
                for j in range(2):
                    for b in range(1, behind + 1):
                        @pl.when(g >= b)
                        def _(j=j, b=b, u=u):
                            part_of(p, j, u, b).wait_recv()
            step4(u, 0)
            lax.fori_loop(0, 4, lambda n, _, u=u: step16(4 * u + n, 0), 0, unroll=4)
            send_back(p, u)
            if p > 0 and u == 0:
                mix_out(p - 1)
            if p == last and u == 2:
                close(0)
            if p == last and u == 3:
                settle(0)
                settle(1)
        levels(p)
        send_levels(p)

    close(1)
    settle(2)
    heads = 2 * pairs
    for p in range(pairs):
        for k in masks:
            level(p, k).wait_recv()
    for i in range(group):
        for p in range(pairs):
            for h in range(2):
                row = i * heads + p * 2 + h
                lw_ref[row:row + 1, :] = lw_in[i, p, h:h + 1, :]
    settle(3)
    for i in range(depth // LANES):
        out_ref[:, i * LANES:(i + 1) * LANES] = final[i].astype(bf16)

    for k in range(1, n_tp):
        for u in range(4):
            swap(k, u).wait_send()
    for p in range(pairs):
        for k in masks:
            level(p, k).wait_send()
            for u in range(4):
                back(p, k, u).wait_send()
    for j in range(2):
        for k in masks:
            near(k, j).wait_send()
        for d in range(min(count - 1, 4)):
            passed(j, d)
        if count > 5:
            lax.fori_loop(4, count - 1, lambda d, _, j=j: (passed(j, d), 0)[1], 0)
    for k, q in firsts + seconds:
        direct(k, q).wait_send()
        twin(k, q).wait_send()
    if group == 4:
        for i in range(2):
            across(i).wait_send()
            twin(3, i).wait_send()
    if mixed:
        @pl.when(g + 1 < count)
        def _():
            rise().wait_send()

        @pl.when(g >= 1)
        def _():
            ext_twin(0, 0).wait_send()
            for k, q in firsts + seconds:
                ext_direct(k, q).wait_send()
                ext_twin(k, q).wait_send()
            for i in range(2):
                ext_across(i).wait_send()
                ext_twin(3, i).wait_send()
    for pair in range(pairs):
        for j in range(2):
            if not mixed:
                @pl.when(g + 1 < count)
                def _(pair=pair, j=j):
                    early(pair, j).wait_send()

            for b in range(1, behind + 1):
                if pair == 0:
                    for k in everything:
                        @pl.when((g + b < count) & needed(k))
                        def _(j=j, b=b, k=k):
                            late(0, j, k, b).wait_send()
                else:
                    @pl.when(g + b < count)
                    def _(pair=pair, j=j, b=b):
                        for u in range(4):
                            part_of(pair, j, u, b).wait_send()


def layer(mesh, group, behind, hidden, gain, freq, wq, wk, wv, wo, post):
    n_sp = mesh.shape["sp"]
    n_tp = mesh.shape["tp"]
    rows, depth = hidden.shape
    w_rows, width = wk.shape
    part = width // group
    pairs = part // LANES
    all_rows = rows * group
    steps = all_rows // WIDE
    few = rows // WIDE
    thin = few // n_tp
    count = n_sp // group
    share = rows // n_tp
    f32, bf16 = jnp.float32, jnp.bfloat16
    dma = pltpu.SemaphoreType.DMA
    mixed = behind == 1 and group == 4
    extra = pltpu.VMEM((rows, depth) if mixed else (16, LANES), bf16)
    small = pltpu.VMEM((rows, LANES) if mixed else (8, LANES), f32)
    state = pltpu.VMEM((pairs, all_rows, LANES), f32)
    weight = pltpu.VMEM((depth, part), bf16)
    table = pltpu.VMEM((all_rows, LANES), f32)
    ring = pltpu.VMEM((pairs, SPAN + all_rows, LANES), bf16)
    woven = pltpu.VMEM((pairs, WIDE, (behind + 1) * steps, LANES), bf16)
    pieces = pltpu.VMEM((n_tp - 1, 4, 4, thin, depth), bf16)
    vmem = pl.BlockSpec(memory_space=pltpu.VMEM)
    near = max(group - 1, 1)
    return pl.pallas_call(
        functools.partial(layer_kernel, n_sp, n_tp, group, behind),
        out_shape=(
            jax.ShapeDtypeStruct((share, depth), bf16),
            jax.ShapeDtypeStruct((width // HEAD_DIM, rows), f32),
        ),
        in_specs=[ANY, vmem, vmem, ANY, ANY, ANY, ANY, vmem],
        out_specs=(vmem, vmem),
        scratch_shapes=[
            pltpu.VMEM((rows, depth), bf16), pltpu.VMEM((all_rows, depth), bf16), extra,
            weight, weight, weight, pltpu.VMEM((pairs, group * LANES, depth), bf16), table, table, small, small,
            pltpu.VMEM((2, pairs, rows, LANES), f32),
            pltpu.VMEM((pairs, all_rows, LANES), bf16), ring, ring,
            pltpu.VMEM((pairs, WIDE, steps, LANES), bf16), woven, woven,
            state, state, state, state, state, state, table,
            pltpu.VMEM((2, SPAN, 2 * SPAN), f32),
            pltpu.VMEM((2, SPAN, 2 * SPAN), f32),
            pltpu.VMEM((steps, steps + SPAN), f32),
            pltpu.VMEM((pairs, WIDE, steps, LANES), bf16), pltpu.VMEM((pairs, WIDE, few, group * LANES), bf16),
            pltpu.VMEM((pairs, 2, all_rows), f32), pltpu.VMEM((group, pairs, 2, rows), f32),
            pltpu.VMEM((4, 4 * few, depth), f32), pltpu.VMEM((8, few, depth), f32),
            pltpu.VMEM((4, 4, thin, depth), bf16), pieces, pieces,
            pltpu.VMEM((depth // LANES, share, LANES), f32),
            dma((4 + pairs * group,)), dma((2, 2, group)), dma((2, 2, group)),
            dma((2, near)), dma((2, near)), dma((2, 2, count)), dma((2, 2, count)),
            dma((2, 2)), dma((2, 2)), dma((2,)), dma((2,)), dma((3, 2)), dma((3, 2)),
            dma((1,)), dma((1,)), dma((2, 2)), dma((2, 2)), dma((2,)), dma((2,)), dma((4, 2)), dma((4, 2)),
            dma((pairs, 2)), dma((pairs, 2)),
            dma((pairs, 2, behind, 4)), dma((pairs, 2, behind, 4)),
            dma((pairs, near, 4)), dma((pairs, near, 4)), dma((pairs, near)), dma((pairs, near)),
            dma((n_tp - 1, 4)), dma((n_tp - 1, 4)),
        ],
        compiler_params=pltpu.CompilerParams(
            vmem_limit_bytes=63 * 1024 * 1024, collective_id=0, has_side_effects=True
        ),
        name="layer_core",
    )(hidden, gain, freq, wq, wk, wv, wo, post)


def place_kernel(out_ref, lw_ref, out_to, lw_to, held, held_lw, into, away):
    count = into.shape[0] - 1
    size = out_ref.shape[0] // count
    spans = [pl.ds(i * size, size) for i in range(count)]
    reads = [pltpu.make_async_copy(lw_ref, held_lw, into.at[count])]
    reads += [pltpu.make_async_copy(out_ref.at[x], held.at[x], into.at[i]) for i, x in enumerate(spans)]
    writes = [pltpu.make_async_copy(held_lw, lw_to, away.at[count])]
    writes += [pltpu.make_async_copy(held.at[x], out_to.at[x], away.at[i]) for i, x in enumerate(spans)]
    for copy in reads:
        copy.start()
    for read, write in zip(reads, writes):
        read.wait()
        write.start()
    for write in writes:
        write.wait()


def place(out, levels):
    parts = 4 if out.shape[0] % 64 == 0 else 1
    return pl.pallas_call(
        place_kernel,
        out_shape=(jax.ShapeDtypeStruct(out.shape, out.dtype), jax.ShapeDtypeStruct(levels.shape, levels.dtype)),
        in_specs=[ANY, ANY],
        out_specs=(ANY, ANY),
        scratch_shapes=[
            pltpu.VMEM(out.shape, out.dtype), pltpu.VMEM(levels.shape, levels.dtype),
            pltpu.SemaphoreType.DMA((parts + 1,)), pltpu.SemaphoreType.DMA((parts + 1,)),
        ],
        compiler_params=pltpu.CompilerParams(vmem_limit_bytes=62 * 1024 * 1024),
        name="place_outputs",
    )(out, levels)


def body(mesh, hidden_in, pre_gain, query_proj, key_proj, value_proj, out_proj, post_gain):
    rows, depth = hidden_in.shape
    width = query_proj.shape[1]
    group = group_of(mesh, width)
    all_rows = rows * group
    behind = -(-(WIDE * SPAN) // all_rows)
    half_dim = HEAD_DIM // 2
    frequency = ROPE_BASE ** (-(np.arange(half_dim) * 2.0 / HEAD_DIM))
    freq = jnp.asarray(np.tile(frequency, LANES // half_dim)[None, :], jnp.float32)
    out, levels = layer(
        mesh, group, behind, hidden_in, pre_gain[None, :], freq,
        query_proj, key_proj, value_proj, out_proj, post_gain[None, :],
    )
    return place(out, levels)


def solution(mesh):
    placed = (P("sp", None), P(), P(None, "tp"), P("sp", "tp"), P("sp", "tp"), P("tp", None), P())
    return jax.shard_map(
        functools.partial(body, mesh),
        mesh=mesh,
        in_specs=placed,
        out_specs=(P(("sp", "tp"), None), P("tp", "sp")),
        check_vma=False,
    )
```
